32 devices in a mesh: sp: 8 (over z, y), tp: 4 (over x, core).
Axes of the slice: x: 2, y: 2, z: 4, core: 2. Of those that a mesh axis runs over, the one named last changes fastest.
Arguments:
- resid: bfloat16 [6144, 2048], P(('sp', 'tp')), may hold values from -6 to 6
- query: bfloat16 [6144, 1024], P('sp', 'tp'), may hold values from -6 to 6
- keys: bfloat16 [6144, 1024], P('sp', 'tp'), may hold values from -6 to 6
- values: bfloat16 [6144, 1024], P('sp', 'tp'), may hold values from -6 to 6
- out_gate: bfloat16 [6144, 1024], P(('sp', 'tp')), may hold values from -6 to 6
- forget_pre: float32 [4, 6144], P('tp', 'sp'), may hold values from 0 to 16
- input_pre: float32 [4, 6144], P('tp', 'sp'), may hold values from -4 to 130
- head_gain: float32 [1024], replicated, may hold values from 0.1 to 1.9
- out_proj: bfloat16 [1024, 2048], replicated, may hold values from -0.1875 to 0.1875
- ffn_gain: float32 [2048], replicated, may hold values from 0.1 to 1.9
- routes: int32 [6144, 2], P(('sp', 'tp')), may hold values from 0 to 7, all different within a row; in each aligned block of 96 rows (0 to 95, 96 to 191, ...) at most 48 rows name the same one
- route_scores: float32 [6144, 2], P(('sp', 'tp')), may hold values from 0.1 to 1
- w_gate: bfloat16 [8, 2048, 512], P('sp'), may hold values from -0.125 to 0.125
- w_up: bfloat16 [8, 2048, 512], P('sp'), may hold values from -0.125 to 0.125
- w_down: bfloat16 [8, 512, 2048], P('sp'), may hold values from -0.25 to 0.25
Outputs:
- layer_out: bfloat16 [6144, 2048], P(('sp', 'tp'))
The draws below stay inside these ranges and needn't reach their ends.
Inputs may be any that keep to these rules, and one draw needn't show every extreme that they name: `routes`: each row names 2 different experts; in each aligned block of 96 rows no expert is named by more than 48 rows, a bound that some block reaches.
All inputs are finite; a program needn't handle non-finite values.
Results may differ from the reference program's by a relative error of at most 0.0095.
Values may be sent and summed in bfloat16 or wider, within the bound.
A program may use at most 128 MiB of HBM per device.

```python
import math
import jax
import jax.numpy as jnp
import numpy as np
from jax import lax

D = 2048
CELL_HEADS = 4
HEAD_DIM = 256
MDIM = 1024
FF = 512
EXPERTS = 8
TOPK = 2
BLOCK = 64
TOK_DEV = 768
SEQUENCE_TOKENS = 6144
HALF = 96
CAP = 48


def draw_forget_pre(key, part):
    split_random_keys = jax.random.split(jax.random.fold_in(key, 17), 5)
    head_order = jax.random.permutation(split_random_keys[0], CELL_HEADS)
    fast_heads = head_order < CELL_HEADS // 2
    jitter = jnp.clip(jax.random.normal(split_random_keys[1], (CELL_HEADS, SEQUENCE_TOKENS), jnp.float32) * 0.7, -2.4, 2.4)
    base_level = jnp.where(fast_heads, jnp.log(100.0), jnp.log(1.0 * SEQUENCE_TOKENS) + 1.5).astype(jnp.float32)
    factor = jax.random.uniform(split_random_keys[2], (SEQUENCE_TOKENS // TOK_DEV,), jnp.float32, 0.0, jnp.log(4.0))
    slow_part = jnp.repeat(factor, TOK_DEV, total_repeat_length=SEQUENCE_TOKENS)
    output_values = base_level[:, None] - slow_part[None, :] + jitter
    outlier_position = jax.random.randint(split_random_keys[3], (3,), 0, SEQUENCE_TOKENS)
    outlier_mask = jnp.any(jnp.arange(SEQUENCE_TOKENS)[:, None] == outlier_position[None, :], axis=1)
    outlier_value = jax.random.uniform(split_random_keys[4], (CELL_HEADS, SEQUENCE_TOKENS), jnp.float32, 0.0, 1.39)
    return jnp.where(outlier_mask[None, :], outlier_value, output_values)


def draw_input_pre(key, part):
    split_random_keys = jax.random.split(jax.random.fold_in(key, 29), 1)
    return jnp.clip(jax.random.normal(split_random_keys[0], (CELL_HEADS, SEQUENCE_TOKENS), jnp.float32), -4.0, 4.0)


def block_levels(stream_key, dims, pieces, least, largest):
    factor_of = 1.0
    for position, parts in pieces:
        steps = jax.random.uniform(jax.random.fold_in(jax.random.fold_in(stream_key, 6), position), (parts,), jnp.float32, least / len(pieces), largest / len(pieces))
        factor_of = factor_of * jnp.repeat(jnp.exp(steps), dims[position] // parts).reshape((-1,) + (1,) * (len(dims) - 1 - position))
    return factor_of


def shared_out(rng, own, number, rows, count, top, reach, skew):
    sequence = jax.random.permutation(rng, count)
    packed, ordinary = shares(count, rows * top, reach, skew, True), shares(count, rows * top, reach, skew, False)
    places = jnp.arange(count)

    def named(sizes, rotation):
        used = int((sizes > 0).sum())
        fixed = max(1, used // 4)
        moved = fixed + (places - fixed + rotation * (used - fixed)) % max(1, count - fixed)
        return jnp.zeros((count,), jnp.int32).at[sequence[jnp.where(places < fixed, places, moved)]].set(jnp.asarray(sizes, jnp.int32))

    sizes = jnp.where(number % 4 == 0, named(packed, number // 4), named(ordinary, number - number // 4 - 1))
    mixed = jax.random.permutation(jax.random.fold_in(own, 3), count)
    donor, sink = mixed[0:count // 2 * 2:2], mixed[1:count // 2 * 2:2]
    margin = jnp.minimum(sizes[donor] - 1, reach - sizes[sink]) // 2
    margin = jnp.where((donor == sequence[0]) | (sink == sequence[0]) | (sizes[sink] == 0), 0, jnp.maximum(margin, 0))
    moved = jax.random.randint(jax.random.fold_in(own, 4), (count // 2,), 0, 1 << 20) % (margin + 1)
    sizes = sizes.at[donor].add(-moved).at[sink].add(moved)
    labels = jnp.searchsorted(jnp.cumsum(sizes), jnp.arange(rows * top), side="right").astype(jnp.int32)
    grid = labels.reshape(top, rows).T
    grid = grid[jax.random.permutation(jax.random.fold_in(own, 1), rows)]
    rotation = jax.random.randint(jax.random.fold_in(own, 2), (rows, 1), 0, top)
    return jnp.take_along_axis(grid, (jnp.arange(top)[None, :] + rotation) % top, axis=1)


def shares(count, total, limit, skew, full):
    loads = [(1 << 20) // math.isqrt(rank ** skew) + 1 for rank in range(1, count + 1)]
    largest = limit if full else min(limit, max(-(-total // count), total * loads[0] // sum(loads)))
    least = 1 if total - largest >= count - 1 else 0
    counts, spare = [largest] + [least] * (count - 1), total - largest - least * (count - 1)
    while spare > 0:
        movable = [i for i in range(1, count) if counts[i] < largest] or [i for i in range(1, count) if counts[i] < limit]
        pool, left = sum([loads[i] for i in movable]), spare
        for i in movable:
            addition = min(limit - counts[i], max(1, left * loads[i] // pool), spare)
            counts[i] = counts[i] + addition
            spare = spare - addition
    return np.array(counts)


def centred(key, extent, spread, limit, shards=(), held_as=jnp.bfloat16):
    values = spread * jax.random.normal(key, extent, jnp.float32)
    if shards:
        values = values * block_levels(key, extent, shards, -0.22, 0.18)
    return jnp.clip(values, -limit, limit).astype(held_as)


def setup_inputs(seed: int = 0) -> dict:
    key_list = jax.random.split(jax.random.key(seed), 16)
    resid = centred(key_list[0], (SEQUENCE_TOKENS, D), 1.0, 6.0, ((0, 32),))
    query = centred(key_list[1], (SEQUENCE_TOKENS, MDIM), 1.0, 6.0, ((0, 8), (1, 4)))
    keys = centred(key_list[2], (SEQUENCE_TOKENS, MDIM), 1.0, 6.0, ((0, 8), (1, 4)))
    values = centred(key_list[3], (SEQUENCE_TOKENS, MDIM), 1.0, 6.0, ((0, 8), (1, 4)))
    out_gate = centred(key_list[4], (SEQUENCE_TOKENS, MDIM), 1.0, 6.0, ((0, 32),))
    forget_pre = draw_forget_pre(jax.random.fold_in(key_list[15], 71), 0)
    input_pre = draw_input_pre(jax.random.fold_in(key_list[15], 71), 0)
    head_gain = jnp.clip(1.0 + 0.18 * jax.random.normal(key_list[7], (MDIM,), jnp.float32), 0.1, 1.9)
    out_proj = centred(key_list[8], (MDIM, D), MDIM ** -0.5, 0.1875)
    ffn_gain = jnp.clip(1.0 + 0.18 * jax.random.normal(key_list[9], (D,), jnp.float32), 0.1, 1.9)
    routes_keys = jax.random.split(jax.random.fold_in(key_list[10], 1), SEQUENCE_TOKENS // HALF)
    routes_turns = jax.random.permutation(jax.random.fold_in(key_list[10], 3), SEQUENCE_TOKENS // HALF)
    routes = jax.vmap(lambda own, number: shared_out(jax.random.fold_in(key_list[10], 2), own, number, HALF, EXPERTS, TOPK, CAP, 1))(routes_keys, routes_turns).reshape((SEQUENCE_TOKENS, TOPK))
    route_scores = jnp.clip(0.1 + 0.9 * jax.random.uniform(key_list[11], (SEQUENCE_TOKENS, TOPK), jnp.float32) ** block_levels(key_list[11], (SEQUENCE_TOKENS, TOPK), ((0, 32),), -0.2, 0.2), 0.1, 1.0)
    w_gate = centred(key_list[12], (EXPERTS, D, FF), D ** -0.5, 0.125, ((0, 8),))
    w_up = centred(key_list[13], (EXPERTS, D, FF), D ** -0.5, 0.125, ((0, 8),))
    w_down = centred(key_list[14], (EXPERTS, FF, D), FF ** -0.5, 0.25, ((0, 8),))
    return {"resid": resid, "query": query, "keys": keys, "values": values, "out_gate": out_gate, "forget_pre": forget_pre, "input_pre": input_pre, "head_gain": head_gain, "out_proj": out_proj, "ffn_gain": ffn_gain, "routes": routes, "route_scores": route_scores, "w_gate": w_gate, "w_up": w_up, "w_down": w_down}


EPS = 1e-06
HIGHEST = lax.Precision.HIGHEST

def block_pass(query, keys, values, log_forget, log_input, state):
    seq_len, head_width = query.shape
    blocks = seq_len // BLOCK
    key_scale = head_width ** (-0.5)
    causal = jnp.tril(jnp.ones((BLOCK, BLOCK), dtype=bool))

    def block_step(state_in, inputs):
        state_mat, state_vec, max_log = state_in
        q_block, k_block, v_block, forget_blk, input_blk = inputs
        cum_log = jnp.cumsum(forget_blk)
        block_total = cum_log[-1]
        log_mat = jnp.where(causal, cum_log[:, None] - cum_log[None, :] + input_blk[None, :], -jnp.inf)
        inter_log = cum_log + max_log
        row_max = jnp.maximum(inter_log, lax.optimization_barrier(jnp.max(log_mat, axis=1)))
        weight_mat = jnp.exp(log_mat - row_max[:, None])
        carry_weight = jnp.exp(inter_log - row_max)
        scores = jnp.dot(q_block, k_block.T, preferred_element_type=jnp.float32) * key_scale
        weights_blk = (scores * weight_mat).astype(jnp.bfloat16)
        q_float = q_block.astype(jnp.float32)
        numerator = carry_weight[:, None] * jnp.dot(q_float, state_mat, precision=HIGHEST) + jnp.dot(weights_blk, v_block, preferred_element_type=jnp.float32)
        denominator = carry_weight * jnp.dot(q_float, state_vec, precision=HIGHEST) + lax.optimization_barrier(jnp.sum(weights_blk.astype(jnp.float32), axis=1))
        log_keep = block_total - cum_log + input_blk
        new_max = jnp.maximum(block_total + max_log, jnp.max(log_keep))
        keep_weight = jnp.exp(log_keep - new_max)
        decay_now = jnp.exp(block_total + max_log - new_max)
        k_float = k_block.astype(jnp.float32) * key_scale
        state_mat = decay_now * state_mat + jnp.dot((k_float * keep_weight[:, None]).T, v_block.astype(jnp.float32), precision=HIGHEST)
        state_vec = decay_now * state_vec + jnp.dot(keep_weight, k_float, precision=HIGHEST)
        return ((state_mat, state_vec, new_max), (numerator, denominator, row_max))

    def to_blocks(array_in):
        return array_in.reshape((blocks, BLOCK) + array_in.shape[1:])
    ignored, outputs = lax.scan(block_step, state, (to_blocks(query), to_blocks(keys), to_blocks(values), to_blocks(log_forget), to_blocks(log_input)))
    numerator, denominator, row_max = outputs
    return (numerator.reshape(seq_len, head_width), denominator.reshape(seq_len), row_max.reshape(seq_len))

def reference(resid, query, keys, values, out_gate, forget_pre, input_pre, head_gain, out_proj, ffn_gain, routes, route_scores, w_gate, w_up, w_down):
    log_forget = jax.nn.log_sigmoid(forget_pre)
    start_state = (jnp.zeros((HEAD_DIM, HEAD_DIM), jnp.float32), jnp.zeros((HEAD_DIM,), jnp.float32), jnp.zeros((), jnp.float32))
    head_outs = []
    for head_idx in range(CELL_HEADS):
        col_start = head_idx * HEAD_DIM
        col_end = col_start + HEAD_DIM
        numerator, denominator, row_max = block_pass(query[:, col_start:col_end], keys[:, col_start:col_end], values[:, col_start:col_end], log_forget[head_idx], input_pre[head_idx], start_state)
        hidden = numerator / jnp.maximum(jnp.abs(denominator), jnp.exp(-row_max))[:, None]
        head_outs.append(hidden)
    cell_rows = lax.optimization_barrier(jnp.concatenate(head_outs, axis=1).astype(jnp.bfloat16))
    cell_float = cell_rows.astype(jnp.float32)
    headed = cell_float * lax.rsqrt(lax.optimization_barrier(jnp.mean(cell_float * cell_float, axis=1, keepdims=True)) + EPS) * head_gain[None, :]
    gated_out = (headed * jax.nn.sigmoid(out_gate.astype(jnp.float32))).astype(jnp.bfloat16)
    after_mix = resid.astype(jnp.float32) + jnp.dot(gated_out, out_proj, preferred_element_type=jnp.float32)
    normed_rows = (after_mix * lax.rsqrt(lax.optimization_barrier(jnp.mean(after_mix * after_mix, axis=1, keepdims=True)) + EPS) * ffn_gain[None, :]).astype(jnp.bfloat16)
    flat_ids = routes.reshape(-1).astype(jnp.int32)
    one_hot = (flat_ids[:, None] == jnp.arange(EXPERTS, dtype=jnp.int32)[None, :]).astype(jnp.int32)
    slot_rank = lax.optimization_barrier(jnp.sum((jnp.cumsum(one_hot, axis=0) - 1) * one_hot, axis=1)).astype(jnp.int32)
    most_rows = SEQUENCE_TOKENS // HALF * CAP
    index_table = jnp.zeros((EXPERTS, most_rows), jnp.int32).at[flat_ids, slot_rank].set(jnp.arange(flat_ids.shape[0], dtype=jnp.int32) // TOPK)

    def one_expert(operands):
        row_picks, gate_mat, up_mat, down_mat = operands
        tok_rows = normed_rows[row_picks]
        gate_pre = jnp.dot(tok_rows, gate_mat, preferred_element_type=jnp.float32)
        up_pre = jnp.dot(tok_rows, up_mat, preferred_element_type=jnp.float32)
        active = (jax.nn.silu(gate_pre) * up_pre).astype(jnp.bfloat16)
        return jnp.dot(active, down_mat, preferred_element_type=jnp.float32).astype(jnp.bfloat16)
    expert_out = lax.map(one_expert, (index_table, w_gate, w_up, w_down))
    assigned = expert_out[flat_ids, slot_rank].astype(jnp.float32).reshape(SEQUENCE_TOKENS, TOPK, D)
    route_weight = route_scores / lax.optimization_barrier(jnp.sum(route_scores, axis=1, keepdims=True))
    combined = lax.optimization_barrier(jnp.sum(assigned * route_weight[:, :, None], axis=1))
    return (after_mix + combined).astype(jnp.bfloat16)
```

```python
import functools

import jax
import jax.numpy as jnp
from jax import lax
from jax.experimental import pallas as pl
from jax.experimental.pallas import tpu as pltpu
from jax.sharding import PartitionSpec as P

BLOCK = 64


EPS = 1e-06
FLOOR_LOG = -1e30
HIGHEST = lax.Precision.HIGHEST


EXTRA = 8
VMEM_LIMIT = 56 * 1024 * 1024


def col_mask(first_row, rows, cols):
    row = lax.broadcasted_iota(jnp.int32, (rows, cols), 0) + first_row
    col = lax.broadcasted_iota(jnp.int32, (rows, cols), 1)
    return row, col


def split_two(a):
    high = a.astype(jnp.bfloat16)
    return high, (a - high.astype(jnp.float32)).astype(jnp.bfloat16)


def log_rows(forget_ref, input_ref):
    pre = forget_ref[...]
    log_forget = jnp.minimum(pre, 0.0) - jnp.log1p(jnp.exp(-jnp.abs(pre)))
    seq_len = pre.shape[1]
    row, col = col_mask(0, seq_len, seq_len)
    upper = jnp.where(row <= col, 1.0, 0.0).astype(jnp.bfloat16)
    one, rest = split_two(log_forget)
    two, three = split_two(log_forget - one.astype(jnp.float32))
    stacked = jnp.concatenate([one, two, three, jnp.zeros((13, seq_len), jnp.bfloat16)], axis=0)
    sums = jnp.dot(stacked, upper, preferred_element_type=jnp.float32)
    cum_row = sums[0:1] + sums[1:2] + sums[2:3]
    return log_forget, cum_row, input_ref[...] - cum_row


def cell_state_kernel(k_ref, v_ref, forget_ref, input_ref, state_ref):
    width = k_ref.shape[1]
    seq_len = k_ref.shape[0]
    log_forget, cum_row, gap_row = log_rows(forget_ref, input_ref)
    total = jnp.sum(log_forget, axis=1, keepdims=True)
    top = jnp.max(gap_row, axis=1, keepdims=True)
    keep_row = jnp.exp(gap_row - top) * width ** (-0.5)
    k_turned = k_ref[...].astype(jnp.float32).T
    weighted = k_turned * keep_row
    high, low = split_two(weighted)
    v = v_ref[...]
    state_ref[0:width, :] = jnp.dot(high, v, preferred_element_type=jnp.float32) + jnp.dot(
        low, v, preferred_element_type=jnp.float32
    )
    vector = jnp.dot(
        jnp.broadcast_to(keep_row, (8, seq_len)),
        k_ref[...].astype(jnp.float32),
        precision=HIGHEST,
        preferred_element_type=jnp.float32,
    )[0:1]
    lanes = jnp.zeros((1, width), jnp.float32)
    state_ref[width : width + EXTRA, :] = jnp.concatenate(
        [vector, lanes + total, lanes + total + top, jnp.zeros((EXTRA - 3, width), jnp.float32)],
        axis=0,
    )


def cell_local_kernel(q_ref, k_ref, v_ref, forget_ref, input_ref, num_ref, aux_ref, *, tile):
    seq_len, width = q_ref.shape
    log_forget, cum_row, gap_row = log_rows(forget_ref, input_ref)
    for first in range(0, seq_len, tile):
        span = first + tile
        row, col = col_mask(first, tile, span)
        causal = col <= row
        own = (col // BLOCK) == (row // BLOCK)
        gap = jnp.where(causal, gap_row[:, :span], -jnp.inf)
        top = jnp.max(gap, axis=1, keepdims=True)
        cum = jnp.sum(jnp.where(causal, log_forget[:, :span], 0.0), axis=1, keepdims=True)
        scores = lax.dot_general(
            q_ref[first:span, :],
            k_ref[0:span, :],
            (((1,), (1,)), ((), ())),
            preferred_element_type=jnp.float32,
        ) * width ** (-0.5)
        weights = scores * jnp.exp(gap - top)
        high = weights.astype(jnp.bfloat16)
        high_float = high.astype(jnp.float32)
        low_float = jnp.where(own, 0.0, weights - high_float)
        v = v_ref[0:span, :]
        num_ref[first:span, :] = jnp.dot(high, v, preferred_element_type=jnp.float32) + jnp.dot(
            low_float.astype(jnp.bfloat16), v, preferred_element_type=jnp.float32
        )
        den = jnp.sum(high_float + low_float, axis=1, keepdims=True)
        lane = lax.broadcasted_iota(jnp.int32, (tile, 128), 1)
        aux_ref[first:span, :] = jnp.where(lane == 0, den, jnp.where(lane == 1, top, cum))


def cell_join_kernel(q_ref, num_ref, aux_ref, states_ref, rows_ref, mat_ref, *, axis):
    width = q_ref.shape[1]
    place = lax.axis_index(axis)
    mat_ref[...] = jnp.zeros_like(mat_ref)

    def join(step, carry):
        vector, old_max = carry
        extra = states_ref[step, width : width + EXTRA, :]
        new_max, total = extra[2:3], extra[1:2]
        joined = jnp.maximum(total + old_max, new_max)
        keep_old = jnp.exp(total + old_max - joined)
        keep_new = jnp.exp(new_max - joined)
        mat_ref[...] = keep_old * mat_ref[...] + keep_new * states_ref[step, 0:width, :]
        return keep_old * vector + keep_new * extra[0:1], joined

    vector, far_max = lax.fori_loop(
        0,
        place,
        join,
        (jnp.zeros((1, width), jnp.float32), jnp.full((1, width), FLOOR_LOG, jnp.float32)),
    )
    aux = aux_ref[...]
    den, top, cum = aux[:, 0:1], aux[:, 1:2], aux[:, 2:3]
    far = far_max[:, 0:1]
    joined = jnp.maximum(top, far)
    keep_own = jnp.exp(top - joined)
    keep_far = jnp.exp(far - joined)
    q_float = q_ref[...].astype(jnp.float32)
    one, rest = split_two(mat_ref[...])
    two, three = split_two(mat_ref[...] - one.astype(jnp.float32))
    q = q_ref[...]
    far_num = (
        jnp.dot(q, one, preferred_element_type=jnp.float32)
        + jnp.dot(q, two, preferred_element_type=jnp.float32)
        + jnp.dot(q, three, preferred_element_type=jnp.float32)
    )
    far_den = jnp.sum(q_float * vector, axis=1, keepdims=True)
    numerator = keep_own * num_ref[...] + keep_far * far_num
    denominator = keep_own * den + keep_far * far_den
    divisor = jnp.maximum(jnp.abs(denominator), jnp.exp(-(cum + joined)))
    rows_ref[...] = (numerator / divisor).astype(rows_ref.dtype)


def run_cell(query, keys, values, forget_pre, input_pre):
    seq_len, width = query.shape
    params = pltpu.CompilerParams(vmem_limit_bytes=VMEM_LIMIT)
    state = pl.pallas_call(
        cell_state_kernel,
        out_shape=jax.ShapeDtypeStruct((width + EXTRA, width), jnp.float32),
        compiler_params=params,
        cost_estimate=pl.CostEstimate(flops=10**9, bytes_accessed=2**20, transcendentals=0),
        name="cell_state",
    )(keys, values, forget_pre, input_pre)
    cut = (width + EXTRA) // 3
    parts = [lax.all_gather(state[i * cut : (i + 1) * cut], "sp") for i in range(3)]
    gathered = jnp.concatenate(parts, axis=1)
    tile = 4 * BLOCK if seq_len % (4 * BLOCK) == 0 else BLOCK
    numerator, aux = pl.pallas_call(
        functools.partial(cell_local_kernel, tile=tile),
        out_shape=(
            jax.ShapeDtypeStruct((seq_len, width), jnp.float32),
            jax.ShapeDtypeStruct((seq_len, 128), jnp.float32),
        ),
        compiler_params=params,
        cost_estimate=pl.CostEstimate(flops=5 * 10**9, bytes_accessed=2**21, transcendentals=0),
        name="cell_local",
    )(query, keys, values, forget_pre, input_pre)
    rows = pl.pallas_call(
        functools.partial(cell_join_kernel, axis="sp"),
        out_shape=jax.ShapeDtypeStruct((seq_len, width), jnp.bfloat16),
        scratch_shapes=[pltpu.VMEM((width, width), jnp.float32)],
        compiler_params=params,
        name="cell_join",
    )(query, numerator, aux, gathered)
    return rows


def sp_tp_barrier(barrier, counts):
    total = 0
    for axis, count in counts.items():
        place = lax.axis_index(axis)
        for step in range(1, count):
            pl.semaphore_signal(
                barrier,
                inc=1,
                device_id={axis: lax.rem(place + step, count)},
                device_id_type=pl.DeviceIdType.MESH,
            )
        total += count - 1
    return total


def cell_kernel(
    q_ref,
    k_ref,
    v_ref,
    forget_ref,
    input_ref,
    out_ref,
    state_ref,
    piece_ref,
    extra_ref,
    prefix_ref,
    mat_ref,
    num_ref,
    aux_ref,
    rows_ref,
    send_sems,
    recv_sems,
    extra_send_sems,
    extra_recv_sems,
    back_send_sems,
    back_recv_sems,
    turn_send_sems,
    turn_recv_sems,
    own_sem,
    *,
    count,
    heads,
    tile,
):
    seq_len, width = q_ref.shape
    cut = width // count
    place = lax.axis_index("sp")
    head = lax.axis_index("tp")
    barrier = pltpu.get_barrier_semaphore()
    greeted = sp_tp_barrier(barrier, {"sp": count, "tp": heads})
    log_forget, cum_row, gap_row = log_rows(forget_ref, input_ref)
    total = jnp.sum(log_forget, axis=1, keepdims=True)
    best = jnp.max(gap_row, axis=1, keepdims=True)
    keep_row = jnp.exp(gap_row - best) * width ** (-0.5)
    weighted = k_ref[...].astype(jnp.float32).T * keep_row
    high, low = split_two(weighted)
    v_all = v_ref[...]
    state_ref[0:width, :] = jnp.dot(high, v_all, preferred_element_type=jnp.float32) + jnp.dot(
        low, v_all, preferred_element_type=jnp.float32
    )
    vector = jnp.dot(
        jnp.broadcast_to(keep_row, (8, seq_len)),
        k_ref[...].astype(jnp.float32),
        precision=HIGHEST,
        preferred_element_type=jnp.float32,
    )[0:1]
    lanes = jnp.zeros((1, width), jnp.float32)
    state_ref[width : width + EXTRA, :] = jnp.concatenate(
        [vector, lanes + total, lanes + total + best, jnp.zeros((EXTRA - 3, width), jnp.float32)],
        axis=0,
    )
    pl.semaphore_wait(barrier, greeted)
    sends = []
    for step in range(1, count):
        peer = lax.rem(place + step, count)
        extra_copy = pltpu.make_async_remote_copy(
            src_ref=state_ref.at[pl.ds(width, EXTRA)],
            dst_ref=extra_ref.at[place],
            send_sem=extra_send_sems.at[step - 1],
            recv_sem=extra_recv_sems.at[step - 1],
            device_id={"sp": peer},
            device_id_type=pl.DeviceIdType.MESH,
        )
        piece_copy = pltpu.make_async_remote_copy(
            src_ref=state_ref.at[pl.ds(pl.multiple_of(peer * cut, cut), cut)],
            dst_ref=piece_ref.at[place],
            send_sem=send_sems.at[step - 1],
            recv_sem=recv_sems.at[step - 1],
            device_id={"sp": peer},
            device_id_type=pl.DeviceIdType.MESH,
        )
        extra_copy.start()
        piece_copy.start()
        sends += [extra_copy, piece_copy]
    extra_ref[place] = state_ref[width : width + EXTRA, :]
    piece_ref[place] = state_ref[pl.ds(pl.multiple_of(place * cut, cut), cut), :]

    for first in range(0, seq_len, tile):
        span = first + tile
        row, col = col_mask(first, tile, span)
        causal = col <= row
        own = (col // BLOCK) == (row // BLOCK)
        gap = jnp.where(causal, gap_row[:, :span], -jnp.inf)
        top = jnp.max(gap, axis=1, keepdims=True)
        cum = jnp.sum(jnp.where(causal, log_forget[:, :span], 0.0), axis=1, keepdims=True)
        scores = lax.dot_general(
            q_ref[first:span, :],
            k_ref[0:span, :],
            (((1,), (1,)), ((), ())),
            preferred_element_type=jnp.float32,
        ) * width ** (-0.5)
        weights = scores * jnp.exp(gap - top)
        high = weights.astype(jnp.bfloat16)
        high_float = high.astype(jnp.float32)
        low_float = jnp.where(own, 0.0, weights - high_float)
        v = v_ref[0:span, :]
        num_ref[first:span, :] = jnp.dot(high, v, preferred_element_type=jnp.float32) + jnp.dot(
            low_float.astype(jnp.bfloat16), v, preferred_element_type=jnp.float32
        )
        den = jnp.sum(high_float + low_float, axis=1, keepdims=True)
        lane = lax.broadcasted_iota(jnp.int32, (tile, 128), 1)
        aux_ref[first:span, :] = jnp.where(lane == 0, den, jnp.where(lane == 1, top, cum))

    for copy in sends:
        copy.wait()

    running = jnp.zeros((cut, width), jnp.float32)
    vector = jnp.zeros((1, width), jnp.float32)
    far_max = jnp.full((1, width), FLOOR_LOG, jnp.float32)
    own_vector, own_max = vector, far_max
    for step in range(count):
        prefix_ref[step] = running
        own_vector = jnp.where(place == step, vector, own_vector)
        own_max = jnp.where(place == step, far_max, own_max)
        if step < count - 1:
            extra = extra_ref[step]
            new_max, step_total = extra[2:3], extra[1:2]
            joined = jnp.maximum(step_total + far_max, new_max)
            keep_old = jnp.exp(step_total + far_max - joined)
            keep_new = jnp.exp(new_max - joined)
            running = keep_old * running + keep_new * piece_ref[step]
            vector = keep_old * vector + keep_new * extra[0:1]
            far_max = joined
    backs = []
    for step in range(1, count):
        peer = lax.rem(place + step, count)
        back = pltpu.make_async_remote_copy(
            src_ref=prefix_ref.at[peer],
            dst_ref=mat_ref.at[pl.ds(pl.multiple_of(place * cut, cut), cut)],
            send_sem=back_send_sems.at[step - 1],
            recv_sem=back_recv_sems.at[step - 1],
            device_id={"sp": peer},
            device_id_type=pl.DeviceIdType.MESH,
        )
        back.start()
        backs.append(back)
    mat_ref[pl.ds(pl.multiple_of(place * cut, cut), cut), :] = prefix_ref[place]

    aux = aux_ref[...]
    den, top, cum = aux[:, 0:1], aux[:, 1:2], aux[:, 2:3]
    far = own_max[:, 0:1]
    joined = jnp.maximum(top, far)
    keep_own = jnp.exp(top - joined)
    keep_far = jnp.exp(far - joined)
    q_float = q_ref[...].astype(jnp.float32)
    far_den = jnp.sum(q_float * own_vector, axis=1, keepdims=True)
    denominator = keep_own * den + keep_far * far_den
    divisor = jnp.maximum(jnp.abs(denominator), jnp.exp(-(cum + joined)))
    for copy in backs:
        copy.wait()
    one, rest = split_two(mat_ref[...])
    two, three = split_two(mat_ref[...] - one.astype(jnp.float32))
    q = q_ref[...]
    far_num = (
        jnp.dot(q, one, preferred_element_type=jnp.float32)
        + jnp.dot(q, two, preferred_element_type=jnp.float32)
        + jnp.dot(q, three, preferred_element_type=jnp.float32)
    )
    numerator = keep_own * num_ref[...] + keep_far * far_num
    rows_ref[...] = (numerator / divisor).astype(rows_ref.dtype)

    share = seq_len // heads
    columns = pl.ds(pl.multiple_of(head * width, width), width)
    turns = []
    for step in range(1, heads):
        peer = lax.rem(head + step, heads)
        turn = pltpu.make_async_remote_copy(
            src_ref=rows_ref.at[pl.ds(pl.multiple_of(peer * share, share), share)],
            dst_ref=out_ref.at[:, columns],
            send_sem=turn_send_sems.at[step - 1],
            recv_sem=turn_recv_sems.at[step - 1],
            device_id={"tp": peer},
            device_id_type=pl.DeviceIdType.MESH,
        )
        turn.start()
        turns.append(turn)
    own_copy = pltpu.make_async_copy(
        rows_ref.at[pl.ds(pl.multiple_of(head * share, share), share)],
        out_ref.at[:, columns],
        own_sem,
    )
    own_copy.start()
    own_copy.wait()
    for turn in turns:
        turn.wait()


def run_cell_scan(query, keys, values, forget_pre, input_pre):
    seq_len, width = query.shape
    count, heads = lax.axis_size("sp"), lax.axis_size("tp")
    tile = 4 * BLOCK if seq_len % (4 * BLOCK) == 0 else BLOCK
    cut = width // count
    vmem = pl.BlockSpec(memory_space=pltpu.VMEM)
    dma = pltpu.SemaphoreType.DMA
    return pl.pallas_call(
        functools.partial(cell_kernel, count=count, heads=heads, tile=tile),
        out_shape=jax.ShapeDtypeStruct((seq_len // heads, heads * width), jnp.bfloat16),
        in_specs=[vmem] * 5,
        out_specs=vmem,
        scratch_shapes=[
            pltpu.VMEM((width + EXTRA, width), jnp.float32),
            pltpu.VMEM((count, cut, width), jnp.float32),
            pltpu.VMEM((count, EXTRA, width), jnp.float32),
            pltpu.VMEM((count, cut, width), jnp.float32),
            pltpu.VMEM((width, width), jnp.float32),
            pltpu.VMEM((seq_len, width), jnp.float32),
            pltpu.VMEM((seq_len, 128), jnp.float32),
            pltpu.VMEM((seq_len, width), jnp.bfloat16),
            dma((count - 1,)),
            dma((count - 1,)),
            dma((count - 1,)),
            dma((count - 1,)),
            dma((count - 1,)),
            dma((count - 1,)),
            dma((heads - 1,)),
            dma((heads - 1,)),
            dma(()),
        ],
        compiler_params=pltpu.CompilerParams(
            vmem_limit_bytes=VMEM_LIMIT, collective_id=3, has_side_effects=True
        ),
        cost_estimate=pl.CostEstimate(flops=10**10, bytes_accessed=2**21, transcendentals=0),
        name="cell",
    )(query, keys, values, forget_pre, input_pre)


def token_cell(query, keys, values, forget_pre, input_pre):
    if query.shape[1] % (8 * lax.axis_size("sp")) == 0:
        return run_cell_scan(query, keys, values, forget_pre, input_pre)
    rows = run_cell(query, keys, values, forget_pre, input_pre)
    return lax.all_to_all(rows, "tp", split_axis=0, concat_axis=1, tiled=True)


def slot_select(expert_ids, expert_count, capacity):
    flat_ids = expert_ids.reshape(-1)
    one_hot = (flat_ids[:, None] == jnp.arange(expert_count, dtype=jnp.int32)[None, :]).astype(
        jnp.int32
    )
    slot_rank = jnp.sum((jnp.cumsum(one_hot, axis=0) - 1) * one_hot, axis=1)
    target = flat_ids * capacity + slot_rank
    return (
        jnp.arange(expert_count * capacity, dtype=jnp.int32)[:, None] == target[None, :]
    ).astype(jnp.bfloat16)


def exchange_kernel(send_ref, recv_ref, send_sems, recv_sems, own_sem, *, axis, count):
    place = lax.axis_index(axis)
    barrier = pltpu.get_barrier_semaphore()
    for step in range(1, count):
        peer = lax.rem(place + step, count)
        pl.semaphore_signal(
            barrier, inc=1, device_id={axis: peer}, device_id_type=pl.DeviceIdType.MESH
        )
    own = pltpu.make_async_copy(send_ref.at[place], recv_ref.at[place], own_sem)
    own.start()
    pl.semaphore_wait(barrier, count - 1)
    copies = []
    for step in range(1, count):
        peer = lax.rem(place + step, count)
        copy = pltpu.make_async_remote_copy(
            src_ref=send_ref.at[peer],
            dst_ref=recv_ref.at[place],
            send_sem=send_sems.at[step - 1],
            recv_sem=recv_sems.at[step - 1],
            device_id={axis: peer},
            device_id_type=pl.DeviceIdType.MESH,
        )
        copy.start()
        copies.append(copy)
    own.wait()
    for copy in copies:
        copy.wait()


def exchange(blocks, axis, collective_id):
    count = lax.axis_size(axis)
    grouped = blocks.reshape((count, -1) + blocks.shape[2:])
    out = pl.pallas_call(
        functools.partial(exchange_kernel, axis=axis, count=count),
        out_shape=jax.ShapeDtypeStruct(grouped.shape, grouped.dtype),
        in_specs=[pl.BlockSpec(memory_space=pl.ANY)],
        out_specs=pl.BlockSpec(memory_space=pl.ANY),
        scratch_shapes=[
            pltpu.SemaphoreType.DMA((count - 1,)),
            pltpu.SemaphoreType.DMA((count - 1,)),
            pltpu.SemaphoreType.DMA(()),
        ],
        compiler_params=pltpu.CompilerParams(collective_id=collective_id, has_side_effects=True),
        name="exchange",
    )(grouped)
    return out.reshape(blocks.shape)


def run_experts(arrived, w_gate, w_up, w_down, sources):
    local_count = w_gate.shape[0]
    grouped = arrived.reshape(sources, local_count, arrived.shape[1], arrived.shape[2])
    gate_pre = jnp.einsum("pesd,edf->pesf", grouped, w_gate, preferred_element_type=jnp.float32)
    up_pre = jnp.einsum("pesd,edf->pesf", grouped, w_up, preferred_element_type=jnp.float32)
    active = (jax.nn.silu(gate_pre) * up_pre).astype(jnp.bfloat16)
    result = jnp.einsum(
        "pesf,efd->pesd", active, w_down, preferred_element_type=jnp.float32
    ).astype(jnp.bfloat16)
    return result.reshape(arrived.shape)


def shards(
    resid,
    query,
    keys,
    values,
    out_gate,
    forget_pre,
    input_pre,
    head_gain,
    out_proj,
    ffn_gain,
    routes,
    route_scores,
    w_gate,
    w_up,
    w_down,
):
    head_width = query.shape[1]
    row_count, route_count = routes.shape
    sources = lax.axis_size("sp")
    local_experts = w_gate.shape[0]
    expert_count = local_experts * sources
    half_rows = row_count // 2
    capacity = max(2, 2 * half_rows * route_count // expert_count)
    route_weight = route_scores / jnp.sum(route_scores, axis=1, keepdims=True)
    token_rows = token_cell(query, keys, values, forget_pre, input_pre)
    cell_float = token_rows.astype(jnp.float32)
    headed = (
        cell_float
        * lax.rsqrt(jnp.mean(cell_float * cell_float, axis=1, keepdims=True) + EPS)
        * head_gain[None, :]
    )
    gated_out = (headed * jax.nn.sigmoid(out_gate.astype(jnp.float32))).astype(jnp.bfloat16)
    after_mix = resid.astype(jnp.float32) + jnp.dot(
        gated_out, out_proj, preferred_element_type=jnp.float32
    )
    normed_rows = (
        after_mix
        * lax.rsqrt(jnp.mean(after_mix * after_mix, axis=1, keepdims=True) + EPS)
        * ffn_gain[None, :]
    ).astype(jnp.bfloat16)
    selects = [
        slot_select(
            routes[half_idx * half_rows : (half_idx + 1) * half_rows], expert_count, capacity
        )
        for half_idx in range(2)
    ]

    def pack_rows(half_idx):
        selection = (
            selects[half_idx].reshape(expert_count * capacity, half_rows, route_count).sum(axis=2)
        )
        packed = jnp.dot(
            selection,
            normed_rows[half_idx * half_rows : (half_idx + 1) * half_rows],
            preferred_element_type=jnp.float32,
        )
        return packed.astype(jnp.bfloat16).reshape(expert_count, capacity, normed_rows.shape[1])

    send_rows = jnp.concatenate([pack_rows(0), pack_rows(1)], axis=1)
    finished = run_experts(
        exchange(send_rows, "sp", 1),
        w_gate,
        w_up,
        w_down,
        sources,
    )
    returned = exchange(finished, "sp", 2)
    answers = [returned[:, :capacity], returned[:, capacity:]]
    pieces = []
    for half_idx in range(2):
        gathered = lax.dot_general(
            selects[half_idx],
            answers[half_idx].reshape(expert_count * capacity, -1),
            (((0,), (0,)), ((), ())),
            preferred_element_type=jnp.float32,
        )
        weights_half = route_weight[half_idx * half_rows : (half_idx + 1) * half_rows]
        pieces.append(
            jnp.sum(gathered.reshape(half_rows, route_count, -1) * weights_half[:, :, None], axis=1)
        )
    return (after_mix + jnp.concatenate(pieces, axis=0)).astype(jnp.bfloat16)


def solution(mesh):
    placed = (
        P(("sp", "tp"), None),
        P("sp", "tp"),
        P("sp", "tp"),
        P("sp", "tp"),
        P(("sp", "tp"), None),
        P("tp", "sp"),
        P("tp", "sp"),
        P(),
        P(),
        P(),
        P(("sp", "tp"), None),
        P(("sp", "tp"), None),
        P("sp", None, None),
        P("sp", None, None),
        P("sp", None, None),
    )
    return jax.shard_map(
        shards, mesh=mesh, in_specs=placed, out_specs=P(("sp", "tp"), None), check_vma=False
    )
```

```python
import functools

import jax
import jax.numpy as jnp
from jax import lax
from jax.experimental import pallas as pl
from jax.experimental.pallas import tpu as pltpu
from jax.sharding import PartitionSpec as P

BLOCK = 64


EPS = 1e-06
FLOOR_LOG = -1e30
HIGHEST = lax.Precision.HIGHEST


EXTRA = 8
VMEM_LIMIT = 56 * 1024 * 1024


def col_mask(first_row, rows, cols):
    row = lax.broadcasted_iota(jnp.int32, (rows, cols), 0) + first_row
    col = lax.broadcasted_iota(jnp.int32, (rows, cols), 1)
    return row, col


def split_two(a):
    high = a.astype(jnp.bfloat16)
    return high, (a - high.astype(jnp.float32)).astype(jnp.bfloat16)


def log_rows(forget_ref, input_ref):
    pre = forget_ref[...]
    log_forget = jnp.minimum(pre, 0.0) - jnp.log1p(jnp.exp(-jnp.abs(pre)))
    seq_len = pre.shape[1]
    row, col = col_mask(0, seq_len, seq_len)
    upper = jnp.where(row <= col, 1.0, 0.0).astype(jnp.bfloat16)
    one, rest = split_two(log_forget)
    two, three = split_two(log_forget - one.astype(jnp.float32))
    stacked = jnp.concatenate([one, two, three, jnp.zeros((13, seq_len), jnp.bfloat16)], axis=0)
    sums = jnp.dot(stacked, upper, preferred_element_type=jnp.float32)
    cum_row = sums[0:1] + sums[1:2] + sums[2:3]
    return log_forget, cum_row, input_ref[...] - cum_row


def cell_state_kernel(k_ref, v_ref, forget_ref, input_ref, state_ref):
    width = k_ref.shape[1]
    seq_len = k_ref.shape[0]
    log_forget, cum_row, gap_row = log_rows(forget_ref, input_ref)
    total = jnp.sum(log_forget, axis=1, keepdims=True)
    top = jnp.max(gap_row, axis=1, keepdims=True)
    keep_row = jnp.exp(gap_row - top) * width ** (-0.5)
    k_turned = k_ref[...].astype(jnp.float32).T
    weighted = k_turned * keep_row
    high, low = split_two(weighted)
    v = v_ref[...]
    state_ref[0:width, :] = jnp.dot(high, v, preferred_element_type=jnp.float32) + jnp.dot(
        low, v, preferred_element_type=jnp.float32
    )
    vector = jnp.dot(
        jnp.broadcast_to(keep_row, (8, seq_len)),
        k_ref[...].astype(jnp.float32),
        precision=HIGHEST,
        preferred_element_type=jnp.float32,
    )[0:1]
    lanes = jnp.zeros((1, width), jnp.float32)
    state_ref[width : width + EXTRA, :] = jnp.concatenate(
        [vector, lanes + total, lanes + total + top, jnp.zeros((EXTRA - 3, width), jnp.float32)],
        axis=0,
    )


def cell_local_kernel(q_ref, k_ref, v_ref, forget_ref, input_ref, num_ref, aux_ref, *, tile):
    seq_len, width = q_ref.shape
    log_forget, cum_row, gap_row = log_rows(forget_ref, input_ref)
    for first in range(0, seq_len, tile):
        span = first + tile
        row, col = col_mask(first, tile, span)
        causal = col <= row
        own = (col // BLOCK) == (row // BLOCK)
        gap = jnp.where(causal, gap_row[:, :span], -jnp.inf)
        top = jnp.max(gap, axis=1, keepdims=True)
        cum = jnp.sum(jnp.where(causal, log_forget[:, :span], 0.0), axis=1, keepdims=True)
        scores = lax.dot_general(
            q_ref[first:span, :],
            k_ref[0:span, :],
            (((1,), (1,)), ((), ())),
            preferred_element_type=jnp.float32,
        ) * width ** (-0.5)
        weights = scores * jnp.exp(gap - top)
        high = weights.astype(jnp.bfloat16)
        high_float = high.astype(jnp.float32)
        low_float = jnp.where(own, 0.0, weights - high_float)
        v = v_ref[0:span, :]
        num_ref[first:span, :] = jnp.dot(high, v, preferred_element_type=jnp.float32) + jnp.dot(
            low_float.astype(jnp.bfloat16), v, preferred_element_type=jnp.float32
        )
        den = jnp.sum(high_float + low_float, axis=1, keepdims=True)
        lane = lax.broadcasted_iota(jnp.int32, (tile, 128), 1)
        aux_ref[first:span, :] = jnp.where(lane == 0, den, jnp.where(lane == 1, top, cum))


def cell_join_kernel(q_ref, num_ref, aux_ref, states_ref, rows_ref, mat_ref, *, axis):
    width = q_ref.shape[1]
    place = lax.axis_index(axis)
    mat_ref[...] = jnp.zeros_like(mat_ref)

    def join(step, carry):
        vector, old_max = carry
        extra = states_ref[step, width : width + EXTRA, :]
        new_max, total = extra[2:3], extra[1:2]
        joined = jnp.maximum(total + old_max, new_max)
        keep_old = jnp.exp(total + old_max - joined)
        keep_new = jnp.exp(new_max - joined)
        mat_ref[...] = keep_old * mat_ref[...] + keep_new * states_ref[step, 0:width, :]
        return keep_old * vector + keep_new * extra[0:1], joined

    vector, far_max = lax.fori_loop(
        0,
        place,
        join,
        (jnp.zeros((1, width), jnp.float32), jnp.full((1, width), FLOOR_LOG, jnp.float32)),
    )
    aux = aux_ref[...]
    den, top, cum = aux[:, 0:1], aux[:, 1:2], aux[:, 2:3]
    far = far_max[:, 0:1]
    joined = jnp.maximum(top, far)
    keep_own = jnp.exp(top - joined)
    keep_far = jnp.exp(far - joined)
    q_float = q_ref[...].astype(jnp.float32)
    one, rest = split_two(mat_ref[...])
    two, three = split_two(mat_ref[...] - one.astype(jnp.float32))
    q = q_ref[...]
    far_num = (
        jnp.dot(q, one, preferred_element_type=jnp.float32)
        + jnp.dot(q, two, preferred_element_type=jnp.float32)
        + jnp.dot(q, three, preferred_element_type=jnp.float32)
    )
    far_den = jnp.sum(q_float * vector, axis=1, keepdims=True)
    numerator = keep_own * num_ref[...] + keep_far * far_num
    denominator = keep_own * den + keep_far * far_den
    divisor = jnp.maximum(jnp.abs(denominator), jnp.exp(-(cum + joined)))
    rows_ref[...] = (numerator / divisor).astype(rows_ref.dtype)


def run_cell(query, keys, values, forget_pre, input_pre):
    seq_len, width = query.shape
    params = pltpu.CompilerParams(vmem_limit_bytes=VMEM_LIMIT)
    state = pl.pallas_call(
        cell_state_kernel,
        out_shape=jax.ShapeDtypeStruct((width + EXTRA, width), jnp.float32),
        compiler_params=params,
        cost_estimate=pl.CostEstimate(flops=10**9, bytes_accessed=2**20, transcendentals=0),
        name="cell_state",
    )(keys, values, forget_pre, input_pre)
    cut = (width + EXTRA) // 3
    parts = [lax.all_gather(state[i * cut : (i + 1) * cut], "sp") for i in range(3)]
    gathered = jnp.concatenate(parts, axis=1)
    tile = 4 * BLOCK if seq_len % (4 * BLOCK) == 0 else BLOCK
    numerator, aux = pl.pallas_call(
        functools.partial(cell_local_kernel, tile=tile),
        out_shape=(
            jax.ShapeDtypeStruct((seq_len, width), jnp.float32),
            jax.ShapeDtypeStruct((seq_len, 128), jnp.float32),
        ),
        compiler_params=params,
        cost_estimate=pl.CostEstimate(flops=5 * 10**9, bytes_accessed=2**21, transcendentals=0),
        name="cell_local",
    )(query, keys, values, forget_pre, input_pre)
    rows = pl.pallas_call(
        functools.partial(cell_join_kernel, axis="sp"),
        out_shape=jax.ShapeDtypeStruct((seq_len, width), jnp.bfloat16),
        scratch_shapes=[pltpu.VMEM((width, width), jnp.float32)],
        compiler_params=params,
        name="cell_join",
    )(query, numerator, aux, gathered)
    return rows


def sp_tp_barrier(barrier, counts):
    total = 0
    for axis, count in counts.items():
        place = lax.axis_index(axis)
        for step in range(1, count):
            pl.semaphore_signal(
                barrier,
                inc=1,
                device_id={axis: lax.rem(place + step, count)},
                device_id_type=pl.DeviceIdType.MESH,
            )
        total += count - 1
    return total


def cell_kernel(
    q_ref,
    k_ref,
    v_ref,
    forget_ref,
    input_ref,
    out_ref,
    state_ref,
    piece_ref,
    extra_ref,
    prefix_ref,
    mat_ref,
    num_ref,
    aux_ref,
    rows_ref,
    send_sems,
    recv_sems,
    extra_send_sems,
    extra_recv_sems,
    back_send_sems,
    back_recv_sems,
    turn_send_sems,
    turn_recv_sems,
    own_sem,
    *,
    count,
    heads,
    tile,
):
    seq_len, width = q_ref.shape
    cut = width // count
    place = lax.axis_index("sp")
    head = lax.axis_index("tp")
    barrier = pltpu.get_barrier_semaphore()
    greeted = sp_tp_barrier(barrier, {"sp": count, "tp": heads})
    log_forget, cum_row, gap_row = log_rows(forget_ref, input_ref)
    total = jnp.sum(log_forget, axis=1, keepdims=True)
    best = jnp.max(gap_row, axis=1, keepdims=True)
    keep_row = jnp.exp(gap_row - best) * width ** (-0.5)
    weighted = k_ref[...].astype(jnp.float32).T * keep_row
    high, low = split_two(weighted)
    v_all = v_ref[...]
    state_ref[0:width, :] = jnp.dot(high, v_all, preferred_element_type=jnp.float32) + jnp.dot(
        low, v_all, preferred_element_type=jnp.float32
    )
    vector = jnp.dot(
        jnp.broadcast_to(keep_row, (8, seq_len)),
        k_ref[...].astype(jnp.float32),
        precision=HIGHEST,
        preferred_element_type=jnp.float32,
    )[0:1]
    lanes = jnp.zeros((1, width), jnp.float32)
    state_ref[width : width + EXTRA, :] = jnp.concatenate(
        [vector, lanes + total, lanes + total + best, jnp.zeros((EXTRA - 3, width), jnp.float32)],
        axis=0,
    )
    pl.semaphore_wait(barrier, greeted)
    sends = []
    for step in range(1, count):
        peer = lax.rem(place + step, count)
        extra_copy = pltpu.make_async_remote_copy(
            src_ref=state_ref.at[pl.ds(width, EXTRA)],
            dst_ref=extra_ref.at[place],
            send_sem=extra_send_sems.at[step - 1],
            recv_sem=extra_recv_sems.at[step - 1],
            device_id={"sp": peer},
            device_id_type=pl.DeviceIdType.MESH,
        )
        piece_copy = pltpu.make_async_remote_copy(
            src_ref=state_ref.at[pl.ds(pl.multiple_of(peer * cut, cut), cut)],
            dst_ref=piece_ref.at[place],
            send_sem=send_sems.at[step - 1],
            recv_sem=recv_sems.at[step - 1],
            device_id={"sp": peer},
            device_id_type=pl.DeviceIdType.MESH,
        )
        extra_copy.start()
        piece_copy.start()
        sends += [extra_copy, piece_copy]
    extra_ref[place] = state_ref[width : width + EXTRA, :]
    piece_ref[place] = state_ref[pl.ds(pl.multiple_of(place * cut, cut), cut), :]

    for first in range(0, seq_len, tile):
        span = first + tile
        row, col = col_mask(first, tile, span)
        causal = col <= row
        own = (col // BLOCK) == (row // BLOCK)
        gap = jnp.where(causal, gap_row[:, :span], -jnp.inf)
        top = jnp.max(gap, axis=1, keepdims=True)
        cum = jnp.sum(jnp.where(causal, log_forget[:, :span], 0.0), axis=1, keepdims=True)
        scores = lax.dot_general(
            q_ref[first:span, :],
            k_ref[0:span, :],
            (((1,), (1,)), ((), ())),
            preferred_element_type=jnp.float32,
        ) * width ** (-0.5)
        weights = scores * jnp.exp(gap - top)
        high = weights.astype(jnp.bfloat16)
        high_float = high.astype(jnp.float32)
        low_float = jnp.where(own, 0.0, weights - high_float)
        v = v_ref[0:span, :]
        num_ref[first:span, :] = jnp.dot(high, v, preferred_element_type=jnp.float32) + jnp.dot(
            low_float.astype(jnp.bfloat16), v, preferred_element_type=jnp.float32
        )
        den = jnp.sum(high_float + low_float, axis=1, keepdims=True)
        lane = lax.broadcasted_iota(jnp.int32, (tile, 128), 1)
        aux_ref[first:span, :] = jnp.where(lane == 0, den, jnp.where(lane == 1, top, cum))

    for copy in sends:
        copy.wait()

    running = jnp.zeros((cut, width), jnp.float32)
    vector = jnp.zeros((1, width), jnp.float32)
    far_max = jnp.full((1, width), FLOOR_LOG, jnp.float32)
    own_vector, own_max = vector, far_max
    for step in range(count):
        prefix_ref[step] = running
        own_vector = jnp.where(place == step, vector, own_vector)
        own_max = jnp.where(place == step, far_max, own_max)
        if step < count - 1:
            extra = extra_ref[step]
            new_max, step_total = extra[2:3], extra[1:2]
            joined = jnp.maximum(step_total + far_max, new_max)
            keep_old = jnp.exp(step_total + far_max - joined)
            keep_new = jnp.exp(new_max - joined)
            running = keep_old * running + keep_new * piece_ref[step]
            vector = keep_old * vector + keep_new * extra[0:1]
            far_max = joined
    backs = []
    for step in range(1, count):
        peer = lax.rem(place + step, count)
        back = pltpu.make_async_remote_copy(
            src_ref=prefix_ref.at[peer],
            dst_ref=mat_ref.at[pl.ds(pl.multiple_of(place * cut, cut), cut)],
            send_sem=back_send_sems.at[step - 1],
            recv_sem=back_recv_sems.at[step - 1],
            device_id={"sp": peer},
            device_id_type=pl.DeviceIdType.MESH,
        )
        back.start()
        backs.append(back)
    mat_ref[pl.ds(pl.multiple_of(place * cut, cut), cut), :] = prefix_ref[place]

    aux = aux_ref[...]
    den, top, cum = aux[:, 0:1], aux[:, 1:2], aux[:, 2:3]
    far = own_max[:, 0:1]
    joined = jnp.maximum(top, far)
    keep_own = jnp.exp(top - joined)
    keep_far = jnp.exp(far - joined)
    q_float = q_ref[...].astype(jnp.float32)
    far_den = jnp.sum(q_float * own_vector, axis=1, keepdims=True)
    denominator = keep_own * den + keep_far * far_den
    divisor = jnp.maximum(jnp.abs(denominator), jnp.exp(-(cum + joined)))
    for copy in backs:
        copy.wait()
    one, rest = split_two(mat_ref[...])
    two, three = split_two(mat_ref[...] - one.astype(jnp.float32))
    q = q_ref[...]
    far_num = (
        jnp.dot(q, one, preferred_element_type=jnp.float32)
        + jnp.dot(q, two, preferred_element_type=jnp.float32)
        + jnp.dot(q, three, preferred_element_type=jnp.float32)
    )
    numerator = keep_own * num_ref[...] + keep_far * far_num
    rows_ref[...] = (numerator / divisor).astype(rows_ref.dtype)

    share = seq_len // heads
    columns = pl.ds(pl.multiple_of(head * width, width), width)
    turns = []
    for step in range(1, heads):
        peer = lax.rem(head + step, heads)
        turn = pltpu.make_async_remote_copy(
            src_ref=rows_ref.at[pl.ds(pl.multiple_of(peer * share, share), share)],
            dst_ref=out_ref.at[:, columns],
            send_sem=turn_send_sems.at[step - 1],
            recv_sem=turn_recv_sems.at[step - 1],
            device_id={"tp": peer},
            device_id_type=pl.DeviceIdType.MESH,
        )
        turn.start()
        turns.append(turn)
    own_copy = pltpu.make_async_copy(
        rows_ref.at[pl.ds(pl.multiple_of(head * share, share), share)],
        out_ref.at[:, columns],
        own_sem,
    )
    own_copy.start()
    own_copy.wait()
    for turn in turns:
        turn.wait()


def run_cell_scan(query, keys, values, forget_pre, input_pre):
    seq_len, width = query.shape
    count, heads = lax.axis_size("sp"), lax.axis_size("tp")
    tile = 4 * BLOCK if seq_len % (4 * BLOCK) == 0 else BLOCK
    cut = width // count
    vmem = pl.BlockSpec(memory_space=pltpu.VMEM)
    dma = pltpu.SemaphoreType.DMA
    return pl.pallas_call(
        functools.partial(cell_kernel, count=count, heads=heads, tile=tile),
        out_shape=jax.ShapeDtypeStruct((seq_len // heads, heads * width), jnp.bfloat16),
        in_specs=[vmem] * 5,
        out_specs=vmem,
        scratch_shapes=[
            pltpu.VMEM((width + EXTRA, width), jnp.float32),
            pltpu.VMEM((count, cut, width), jnp.float32),
            pltpu.VMEM((count, EXTRA, width), jnp.float32),
            pltpu.VMEM((count, cut, width), jnp.float32),
            pltpu.VMEM((width, width), jnp.float32),
            pltpu.VMEM((seq_len, width), jnp.float32),
            pltpu.VMEM((seq_len, 128), jnp.float32),
            pltpu.VMEM((seq_len, width), jnp.bfloat16),
            dma((count - 1,)),
            dma((count - 1,)),
            dma((count - 1,)),
            dma((count - 1,)),
            dma((count - 1,)),
            dma((count - 1,)),
            dma((heads - 1,)),
            dma((heads - 1,)),
            dma(()),
        ],
        compiler_params=pltpu.CompilerParams(
            vmem_limit_bytes=VMEM_LIMIT, collective_id=3, has_side_effects=True
        ),
        cost_estimate=pl.CostEstimate(flops=10**10, bytes_accessed=2**21, transcendentals=0),
        name="cell",
    )(query, keys, values, forget_pre, input_pre)


def token_cell(query, keys, values, forget_pre, input_pre):
    if query.shape[1] % (8 * lax.axis_size("sp")) == 0:
        return run_cell_scan(query, keys, values, forget_pre, input_pre)
    rows = run_cell(query, keys, values, forget_pre, input_pre)
    return lax.all_to_all(rows, "tp", split_axis=0, concat_axis=1, tiled=True)


def slot_select(expert_ids, expert_count, capacity):
    flat_ids = expert_ids.reshape(-1)
    one_hot = (flat_ids[:, None] == jnp.arange(expert_count, dtype=jnp.int32)[None, :]).astype(
        jnp.int32
    )
    slot_rank = jnp.sum((jnp.cumsum(one_hot, axis=0) - 1) * one_hot, axis=1)
    target = flat_ids * capacity + slot_rank
    return (
        jnp.arange(expert_count * capacity, dtype=jnp.int32)[:, None] == target[None, :]
    ).astype(jnp.bfloat16)


def exchange_kernel(send_ref, recv_ref, send_sems, recv_sems, own_sem, *, axis, count):
    place = lax.axis_index(axis)
    barrier = pltpu.get_barrier_semaphore()
    for step in range(1, count):
        peer = lax.rem(place + step, count)
        pl.semaphore_signal(
            barrier, inc=1, device_id={axis: peer}, device_id_type=pl.DeviceIdType.MESH
        )
    own = pltpu.make_async_copy(send_ref.at[place], recv_ref.at[place], own_sem)
    own.start()
    pl.semaphore_wait(barrier, count - 1)
    copies = []
    for step in range(1, count):
        peer = lax.rem(place + step, count)
        copy = pltpu.make_async_remote_copy(
            src_ref=send_ref.at[peer],
            dst_ref=recv_ref.at[place],
            send_sem=send_sems.at[step - 1],
            recv_sem=recv_sems.at[step - 1],
            device_id={axis: peer},
            device_id_type=pl.DeviceIdType.MESH,
        )
        copy.start()
        copies.append(copy)
    own.wait()
    for copy in copies:
        copy.wait()


def exchange(blocks, axis, collective_id):
    count = lax.axis_size(axis)
    grouped = blocks.reshape((count, -1) + blocks.shape[2:])
    out = pl.pallas_call(
        functools.partial(exchange_kernel, axis=axis, count=count),
        out_shape=jax.ShapeDtypeStruct(grouped.shape, grouped.dtype),
        in_specs=[pl.BlockSpec(memory_space=pl.ANY)],
        out_specs=pl.BlockSpec(memory_space=pl.ANY),
        scratch_shapes=[
            pltpu.SemaphoreType.DMA((count - 1,)),
            pltpu.SemaphoreType.DMA((count - 1,)),
            pltpu.SemaphoreType.DMA(()),
        ],
        compiler_params=pltpu.CompilerParams(collective_id=collective_id, has_side_effects=True),
        name="exchange",
    )(grouped)
    return out.reshape(blocks.shape)


def run_experts(arrived, w_gate, w_up, w_down, sources):
    local_count = w_gate.shape[0]
    grouped = arrived.reshape(sources, local_count, arrived.shape[1], arrived.shape[2])
    gate_pre = jnp.einsum("pesd,edf->pesf", grouped, w_gate, preferred_element_type=jnp.float32)
    up_pre = jnp.einsum("pesd,edf->pesf", grouped, w_up, preferred_element_type=jnp.float32)
    active = (jax.nn.silu(gate_pre) * up_pre).astype(jnp.bfloat16)
    result = jnp.einsum(
        "pesf,efd->pesd", active, w_down, preferred_element_type=jnp.float32
    ).astype(jnp.bfloat16)
    return result.reshape(arrived.shape)


def line_kernel(
    rows_ref,
    mix_ref,
    info_ref,
    gate_hbm,
    up_hbm,
    down_hbm,
    out_ref,
    gate_ref,
    up_ref,
    down_ref,
    infos_ref,
    held_ref,
    cross_ref,
    crossed_ref,
    answer_ref,
    done_ref,
    batch_ref,
    part_ref,
    own_ref,
    sum_ref,
    load_sems,
    info_send,
    info_recv,
    row_send,
    row_recv,
    cross_send,
    cross_recv,
    answer_send,
    answer_recv,
    sum_send,
    sum_recv,
    *,
    line,
    halves,
    slots,
):
    place = lax.axis_index("sp")
    here = place // 2
    side = lax.rem(place, 2)
    twin = place + 1 - 2 * side
    units = line * halves
    tokens = rows_ref.shape[1]
    last = line - 1

    def remote(src, dst, send, recv, peer):
        return pltpu.make_async_remote_copy(
            src_ref=src,
            dst_ref=dst,
            send_sem=send,
            recv_sem=recv,
            device_id={"sp": peer},
            device_id_type=pl.DeviceIdType.MESH,
        )

    loads = [
        pltpu.make_async_copy(src, dst, load_sems.at[i])
        for i, (src, dst) in enumerate(
            [(gate_hbm, gate_ref), (up_hbm, up_ref), (down_hbm, down_ref)]
        )
    ]
    for load in loads:
        load.start()

    barrier = pltpu.get_barrier_semaphore()
    for step in range(1, line):
        pl.semaphore_signal(
            barrier,
            inc=1,
            device_id={"sp": lax.rem(here + step, line) * 2 + side},
            device_id_type=pl.DeviceIdType.MESH,
        )
    pl.semaphore_signal(
        barrier, inc=1, device_id={"sp": twin}, device_id_type=pl.DeviceIdType.MESH
    )
    pl.semaphore_wait(barrier, line)

    def info_copy(step):
        peer = lax.rem(here + step, line)
        return remote(
            info_ref,
            infos_ref.at[here],
            info_send.at[step - 1],
            info_recv.at[step - 1],
            peer * 2 + side,
        )

    def row_copy(src, source, half, way):
        unit = source * halves + half
        return remote(
            src,
            held_ref.at[unit],
            row_send.at[way, unit],
            row_recv.at[unit],
            place + (4 * way - 2),
        )

    def cross_copy(unit):
        return remote(
            cross_ref.at[unit],
            crossed_ref.at[unit],
            cross_send.at[unit],
            cross_recv.at[unit],
            twin,
        )

    def answer_copy(unit):
        return remote(
            answer_ref.at[unit],
            done_ref.at[unit, pl.ds(slots, slots)],
            answer_send.at[unit],
            answer_recv.at[unit],
            twin,
        )

    def sum_copy(target, half, way):
        landing = (target + way) * halves + half
        return remote(
            part_ref.at[target * halves + half],
            sum_ref.at[landing],
            sum_send.at[target * halves + half],
            sum_recv.at[landing],
            place + (4 * way - 2),
        )

    for step in range(1, line):
        info_copy(step).start()
    for half in range(halves):
        for way in range(2):

            @pl.when((here < last) if way else (here > 0))
            def _():
                row_copy(rows_ref.at[half], here, half, way).start()

    infos_ref[here] = info_ref[...]
    for half in range(halves):
        held_ref[here * halves + half] = rows_ref[half]
    batch_ref[...] = jnp.zeros_like(batch_ref)
    for step in range(1, line):
        info_copy(step).wait()

    shorter = jnp.minimum(here, last - here)

    def source_of(k):
        i = k // halves
        paired = i <= 2 * shorter
        near = (i + 1) // 2
        near_source = here + near * (1 - 2 * lax.rem(i, 2))
        far = i - shorter
        far_source = jnp.where(here < last - here, here + far, here - far)
        return jnp.where(paired, near_source, far_source), lax.rem(k, halves)

    def matches(source, half, weighted):
        info = infos_ref[source, half]
        rank = lax.broadcasted_iota(jnp.int32, (slots, tokens), 0).astype(jnp.float32)
        tables = []
        for expert in (place, twin):
            name = expert.astype(jnp.float32)
            table = jnp.zeros((slots, tokens), jnp.float32)
            for route in range(2):
                hit = jnp.where(info[route : route + 1] == name, info[2 + route : 3 + route], -1.0)
                value = info[4 + route : 5 + route] if weighted else 1.0
                table += jnp.where(hit == rank, value, 0.0)
            tables.append(table)
        return jnp.concatenate(tables, axis=0)

    def step_body(k, carry):
        @pl.when(k < units)
        def _():
            source, half = source_of(k)
            unit = source * halves + half

            @pl.when(source != here)
            def _():
                remote(
                    held_ref.at[unit], held_ref.at[unit], row_send.at[0, unit], row_recv.at[unit], twin
                ).wait_recv()

            @pl.when((source < here) & (here < last))
            def _():
                row_copy(held_ref.at[unit], source, half, 1).start()

            @pl.when((source > here) & (here > 0))
            def _():
                row_copy(held_ref.at[unit], source, half, 0).start()

            packed = jnp.dot(
                matches(source, half, False).astype(jnp.bfloat16),
                held_ref[unit],
                preferred_element_type=jnp.float32,
            ).astype(jnp.bfloat16)
            cross_ref[unit] = packed[slots:]
            cross_copy(unit).start()
            batch_ref[0:slots, :] = packed[:slots]

        @pl.when(k == 0)
        def _():
            for load in loads:
                load.wait()

        @pl.when((k > 0) & (k <= units))
        def _():
            source, half = source_of(k - 1)
            unit = source * halves + half
            cross_copy(unit).wait_recv()
            batch_ref[slots : 2 * slots, :] = crossed_ref[unit]

        @pl.when(k <= units)
        def _():
            rows = batch_ref[...]
            gate = jnp.dot(rows, gate_ref[0], preferred_element_type=jnp.float32)
            up = jnp.dot(rows, up_ref[0], preferred_element_type=jnp.float32)
            active = (jax.nn.silu(gate) * up).astype(jnp.bfloat16)
            batch_ref[...] = jnp.dot(
                active, down_ref[0], preferred_element_type=jnp.float32
            ).astype(jnp.bfloat16)

        @pl.when(k < units)
        def _():
            source, half = source_of(k)
            done_ref[source * halves + half, 0:slots, :] = batch_ref[0:slots, :]

        @pl.when((k > 0) & (k <= units))
        def _():
            source, half = source_of(k - 1)
            unit = source * halves + half
            answer_ref[unit] = batch_ref[slots : 2 * slots, :]
            answer_copy(unit).start()

        @pl.when(k > 1)
        def _():
            source, half = source_of(k - 2)
            unit = source * halves + half
            answer_copy(unit).wait_recv()
            high, low = split_two(matches(source, half, True))
            answers = done_ref[unit]
            turned = (((0,), (0,)), ((), ()))
            part = lax.dot_general(
                high, answers, turned, preferred_element_type=jnp.float32
            ) + lax.dot_general(low, answers, turned, preferred_element_type=jnp.float32)

            @pl.when(source == here)
            def _():
                own_ref[half] = part

            @pl.when(source != here)
            def _():
                part_ref[unit] = part.astype(jnp.bfloat16)

            @pl.when((source < here) & (here == last))
            def _():
                sum_copy(source, half, 0).start()

            @pl.when((source > here) & (here == 0))
            def _():
                sum_copy(source, half, 1).start()

        return carry

    lax.fori_loop(0, units + 2, step_body, 0)

    def relay(way):
        for ahead in range(1, line):
            target = here + ahead * (2 * way - 1)
            for half in range(halves):

                @pl.when((target >= 0) & (target <= last) & (here > 0) & (here < last))
                def _():
                    unit = target * halves + half
                    landing = (target + way) * halves + half
                    remote(
                        part_ref.at[unit],
                        sum_ref.at[landing],
                        sum_send.at[unit],
                        sum_recv.at[landing],
                        twin,
                    ).wait_recv()
                    part_ref[unit] = (
                        part_ref[unit].astype(jnp.float32) + sum_ref[landing].astype(jnp.float32)
                    ).astype(jnp.bfloat16)
                    sum_copy(target, half, way).start()

    first_way = jnp.where(last - here <= here, 0, 1)
    relay(first_way)
    relay(1 - first_way)

    for half in range(halves):
        own_ref[half] = own_ref[half] + mix_ref[half]
        for way in range(2):

            @pl.when((here > 0) if way else (here < last))
            def _():
                landing = (here + way) * halves + half
                remote(
                    part_ref.at[0], sum_ref.at[landing], sum_send.at[0], sum_recv.at[landing], twin
                ).wait_recv()
                own_ref[half] = own_ref[half] + sum_ref[landing].astype(jnp.float32)

        out_ref[half] = own_ref[half].astype(out_ref.dtype)

    def drain(unit, carry):
        source = unit // halves
        half = lax.rem(unit, halves)
        cross_copy(unit).wait_send()
        answer_copy(unit).wait_send()

        @pl.when((source <= here) & (here < last))
        def _():
            row_copy(held_ref.at[unit], source, half, 1).wait_send()

        @pl.when((source >= here) & (here > 0))
        def _():
            row_copy(held_ref.at[unit], source, half, 0).wait_send()

        @pl.when(source != here)
        def _():
            sum_copy(source, half, 0).wait_send()

        return carry

    lax.fori_loop(0, units, drain, 0)


def run_line(normed_rows, after_mix, info, w_gate, w_up, w_down, slots):
    count = lax.axis_size("sp")
    line, halves = count // 2, info.shape[0]
    units = line * halves
    row_count, width = normed_rows.shape
    tokens = row_count // halves
    vmem = pl.BlockSpec(memory_space=pltpu.VMEM)
    whole = pl.BlockSpec(memory_space=pl.ANY)
    dma = pltpu.SemaphoreType.DMA
    out = pl.pallas_call(
        functools.partial(line_kernel, line=line, halves=halves, slots=slots),
        out_shape=jax.ShapeDtypeStruct((halves, tokens, width), jnp.bfloat16),
        in_specs=[vmem, vmem, vmem, whole, whole, whole],
        out_specs=vmem,
        scratch_shapes=[
            pltpu.VMEM(w_gate.shape, jnp.bfloat16),
            pltpu.VMEM(w_up.shape, jnp.bfloat16),
            pltpu.VMEM(w_down.shape, jnp.bfloat16),
            pltpu.VMEM((line,) + info.shape, jnp.float32),
            pltpu.VMEM((units, tokens, width), jnp.bfloat16),
            pltpu.VMEM((units, slots, width), jnp.bfloat16),
            pltpu.VMEM((units, slots, width), jnp.bfloat16),
            pltpu.VMEM((units, slots, width), jnp.bfloat16),
            pltpu.VMEM((units, 2 * slots, width), jnp.bfloat16),
            pltpu.VMEM((2 * slots, width), jnp.bfloat16),
            pltpu.VMEM((units, tokens, width), jnp.bfloat16),
            pltpu.VMEM((halves, tokens, width), jnp.float32),
            pltpu.VMEM((units + halves, tokens, width), jnp.bfloat16),
            dma((3,)),
            dma((line - 1,)),
            dma((line - 1,)),
            dma((2, units)),
            dma((units,)),
            dma((units,)),
            dma((units,)),
            dma((units,)),
            dma((units,)),
            dma((units,)),
            dma((units + halves,)),
        ],
        compiler_params=pltpu.CompilerParams(
            vmem_limit_bytes=VMEM_LIMIT, collective_id=4, has_side_effects=True
        ),
        cost_estimate=pl.CostEstimate(flops=10**10, bytes_accessed=2**23, transcendentals=0),
        name="experts",
    )(
        normed_rows.reshape(halves, tokens, width),
        after_mix.reshape(halves, tokens, width),
        info,
        w_gate,
        w_up,
        w_down,
    )
    return out.reshape(row_count, width)


def route_info(routes, route_weight, halves):
    tokens = routes.shape[0] // halves
    ids = routes.reshape(halves, -1)
    order = jnp.arange(ids.shape[1], dtype=jnp.int32)
    same = (ids[:, :, None] == ids[:, None, :]) & (order[None, None, :] < order[None, :, None])
    rank = jnp.sum(same.astype(jnp.float32), axis=2)

    def turned(a):
        return a.astype(jnp.float32).reshape(halves, tokens, -1).transpose(0, 2, 1)

    return jnp.concatenate(
        [turned(routes), turned(rank), turned(route_weight), jnp.zeros((halves, 2, tokens), jnp.float32)],
        axis=1,
    )


def shards(
    resid,
    query,
    keys,
    values,
    out_gate,
    forget_pre,
    input_pre,
    head_gain,
    out_proj,
    ffn_gain,
    routes,
    route_scores,
    w_gate,
    w_up,
    w_down,
):
    head_width = query.shape[1]
    row_count, route_count = routes.shape
    sources = lax.axis_size("sp")
    local_experts = w_gate.shape[0]
    expert_count = local_experts * sources
    half_rows = row_count // 2
    capacity = max(2, 2 * half_rows * route_count // expert_count)
    route_weight = route_scores / jnp.sum(route_scores, axis=1, keepdims=True)
    token_rows = token_cell(query, keys, values, forget_pre, input_pre)
    cell_float = token_rows.astype(jnp.float32)
    headed = (
        cell_float
        * lax.rsqrt(jnp.mean(cell_float * cell_float, axis=1, keepdims=True) + EPS)
        * head_gain[None, :]
    )
    gated_out = (headed * jax.nn.sigmoid(out_gate.astype(jnp.float32))).astype(jnp.bfloat16)
    after_mix = resid.astype(jnp.float32) + jnp.dot(
        gated_out, out_proj, preferred_element_type=jnp.float32
    )
    normed_rows = (
        after_mix
        * lax.rsqrt(jnp.mean(after_mix * after_mix, axis=1, keepdims=True) + EPS)
        * ffn_gain[None, :]
    ).astype(jnp.bfloat16)
    dense = local_experts == 1 and sources % 2 == 0 and route_count == 2
    if dense and 2 * capacity >= half_rows and capacity % 16 == 0:
        info = route_info(routes, route_weight, 2)
        return run_line(normed_rows, after_mix, info, w_gate, w_up, w_down, capacity)
    selects = [
        slot_select(
            routes[half_idx * half_rows : (half_idx + 1) * half_rows], expert_count, capacity
        )
        for half_idx in range(2)
    ]

    def pack_rows(half_idx):
        selection = (
            selects[half_idx].reshape(expert_count * capacity, half_rows, route_count).sum(axis=2)
        )
        packed = jnp.dot(
            selection,
            normed_rows[half_idx * half_rows : (half_idx + 1) * half_rows],
            preferred_element_type=jnp.float32,
        )
        return packed.astype(jnp.bfloat16).reshape(expert_count, capacity, normed_rows.shape[1])

    send_rows = jnp.concatenate([pack_rows(0), pack_rows(1)], axis=1)
    finished = run_experts(
        exchange(send_rows, "sp", 1),
        w_gate,
        w_up,
        w_down,
        sources,
    )
    returned = exchange(finished, "sp", 2)
    answers = [returned[:, :capacity], returned[:, capacity:]]
    pieces = []
    for half_idx in range(2):
        gathered = lax.dot_general(
            selects[half_idx],
            answers[half_idx].reshape(expert_count * capacity, -1),
            (((0,), (0,)), ((), ())),
            preferred_element_type=jnp.float32,
        )
        weights_half = route_weight[half_idx * half_rows : (half_idx + 1) * half_rows]
        pieces.append(
            jnp.sum(gathered.reshape(half_rows, route_count, -1) * weights_half[:, :, None], axis=1)
        )
    return (after_mix + jnp.concatenate(pieces, axis=0)).astype(jnp.bfloat16)


def solution(mesh):
    placed = (
        P(("sp", "tp"), None),
        P("sp", "tp"),
        P("sp", "tp"),
        P("sp", "tp"),
        P(("sp", "tp"), None),
        P("tp", "sp"),
        P("tp", "sp"),
        P(),
        P(),
        P(),
        P(("sp", "tp"), None),
        P(("sp", "tp"), None),
        P("sp", None, None),
        P("sp", None, None),
        P("sp", None, None),
    )
    return jax.shard_map(
        shards, mesh=mesh, in_specs=placed, out_specs=P(("sp", "tp"), None), check_vma=False
    )
```

```python
import functools

import jax
import jax.numpy as jnp
from jax import lax
from jax.experimental import pallas as pl
from jax.experimental.pallas import tpu as pltpu
from jax.sharding import PartitionSpec as P

BLOCK = 64


EPS = 1e-06
FLOOR_LOG = -1e30
HIGHEST = lax.Precision.HIGHEST


EXTRA = 8
VMEM_LIMIT = 56 * 1024 * 1024


def col_mask(first_row, rows, cols):
    row = lax.broadcasted_iota(jnp.int32, (rows, cols), 0) + first_row
    col = lax.broadcasted_iota(jnp.int32, (rows, cols), 1)
    return row, col


def split_two(a):
    high = a.astype(jnp.bfloat16)
    return high, (a - high.astype(jnp.float32)).astype(jnp.bfloat16)


def log_rows(forget_ref, input_ref):
    pre = forget_ref[...]
    log_forget = jnp.minimum(pre, 0.0) - jnp.log1p(jnp.exp(-jnp.abs(pre)))
    seq_len = pre.shape[1]
    row, col = col_mask(0, seq_len, seq_len)
    upper = jnp.where(row <= col, 1.0, 0.0).astype(jnp.bfloat16)
    one, rest = split_two(log_forget)
    two, three = split_two(log_forget - one.astype(jnp.float32))
    stacked = jnp.concatenate([one, two, three, jnp.zeros((13, seq_len), jnp.bfloat16)], axis=0)
    sums = jnp.dot(stacked, upper, preferred_element_type=jnp.float32)
    cum_row = sums[0:1] + sums[1:2] + sums[2:3]
    return log_forget, cum_row, input_ref[...] - cum_row


def cell_state_kernel(k_ref, v_ref, forget_ref, input_ref, state_ref):
    width = k_ref.shape[1]
    seq_len = k_ref.shape[0]
    log_forget, cum_row, gap_row = log_rows(forget_ref, input_ref)
    total = jnp.sum(log_forget, axis=1, keepdims=True)
    top = jnp.max(gap_row, axis=1, keepdims=True)
    keep_row = jnp.exp(gap_row - top) * width ** (-0.5)
    k_turned = k_ref[...].astype(jnp.float32).T
    weighted = k_turned * keep_row
    high, low = split_two(weighted)
    v = v_ref[...]
    state_ref[0:width, :] = jnp.dot(high, v, preferred_element_type=jnp.float32) + jnp.dot(
        low, v, preferred_element_type=jnp.float32
    )
    vector = jnp.dot(
        jnp.broadcast_to(keep_row, (8, seq_len)),
        k_ref[...].astype(jnp.float32),
        precision=HIGHEST,
        preferred_element_type=jnp.float32,
    )[0:1]
    lanes = jnp.zeros((1, width), jnp.float32)
    state_ref[width : width + EXTRA, :] = jnp.concatenate(
        [vector, lanes + total, lanes + total + top, jnp.zeros((EXTRA - 3, width), jnp.float32)],
        axis=0,
    )


def cell_local_kernel(q_ref, k_ref, v_ref, forget_ref, input_ref, num_ref, aux_ref, *, tile):
    seq_len, width = q_ref.shape
    log_forget, cum_row, gap_row = log_rows(forget_ref, input_ref)
    for first in range(0, seq_len, tile):
        span = first + tile
        row, col = col_mask(first, tile, span)
        causal = col <= row
        own = (col // BLOCK) == (row // BLOCK)
        gap = jnp.where(causal, gap_row[:, :span], -jnp.inf)
        top = jnp.max(gap, axis=1, keepdims=True)
        cum = jnp.sum(jnp.where(causal, log_forget[:, :span], 0.0), axis=1, keepdims=True)
        scores = lax.dot_general(
            q_ref[first:span, :],
            k_ref[0:span, :],
            (((1,), (1,)), ((), ())),
            preferred_element_type=jnp.float32,
        ) * width ** (-0.5)
        weights = scores * jnp.exp(gap - top)
        high = weights.astype(jnp.bfloat16)
        high_float = high.astype(jnp.float32)
        low_float = jnp.where(own, 0.0, weights - high_float)
        v = v_ref[0:span, :]
        num_ref[first:span, :] = jnp.dot(high, v, preferred_element_type=jnp.float32) + jnp.dot(
            low_float.astype(jnp.bfloat16), v, preferred_element_type=jnp.float32
        )
        den = jnp.sum(high_float + low_float, axis=1, keepdims=True)
        lane = lax.broadcasted_iota(jnp.int32, (tile, 128), 1)
        aux_ref[first:span, :] = jnp.where(lane == 0, den, jnp.where(lane == 1, top, cum))


def cell_join_kernel(q_ref, num_ref, aux_ref, states_ref, rows_ref, mat_ref, *, axis):
    width = q_ref.shape[1]
    place = lax.axis_index(axis)
    mat_ref[...] = jnp.zeros_like(mat_ref)

    def join(step, carry):
        vector, old_max = carry
        extra = states_ref[step, width : width + EXTRA, :]
        new_max, total = extra[2:3], extra[1:2]
        joined = jnp.maximum(total + old_max, new_max)
        keep_old = jnp.exp(total + old_max - joined)
        keep_new = jnp.exp(new_max - joined)
        mat_ref[...] = keep_old * mat_ref[...] + keep_new * states_ref[step, 0:width, :]
        return keep_old * vector + keep_new * extra[0:1], joined

    vector, far_max = lax.fori_loop(
        0,
        place,
        join,
        (jnp.zeros((1, width), jnp.float32), jnp.full((1, width), FLOOR_LOG, jnp.float32)),
    )
    aux = aux_ref[...]
    den, top, cum = aux[:, 0:1], aux[:, 1:2], aux[:, 2:3]
    far = far_max[:, 0:1]
    joined = jnp.maximum(top, far)
    keep_own = jnp.exp(top - joined)
    keep_far = jnp.exp(far - joined)
    q_float = q_ref[...].astype(jnp.float32)
    one, rest = split_two(mat_ref[...])
    two, three = split_two(mat_ref[...] - one.astype(jnp.float32))
    q = q_ref[...]
    far_num = (
        jnp.dot(q, one, preferred_element_type=jnp.float32)
        + jnp.dot(q, two, preferred_element_type=jnp.float32)
        + jnp.dot(q, three, preferred_element_type=jnp.float32)
    )
    far_den = jnp.sum(q_float * vector, axis=1, keepdims=True)
    numerator = keep_own * num_ref[...] + keep_far * far_num
    denominator = keep_own * den + keep_far * far_den
    divisor = jnp.maximum(jnp.abs(denominator), jnp.exp(-(cum + joined)))
    rows_ref[...] = (numerator / divisor).astype(rows_ref.dtype)


def run_cell(query, keys, values, forget_pre, input_pre):
    seq_len, width = query.shape
    params = pltpu.CompilerParams(vmem_limit_bytes=VMEM_LIMIT)
    state = pl.pallas_call(
        cell_state_kernel,
        out_shape=jax.ShapeDtypeStruct((width + EXTRA, width), jnp.float32),
        compiler_params=params,
        cost_estimate=pl.CostEstimate(flops=10**9, bytes_accessed=2**20, transcendentals=0),
        name="cell_state",
    )(keys, values, forget_pre, input_pre)
    cut = (width + EXTRA) // 3
    parts = [lax.all_gather(state[i * cut : (i + 1) * cut], "sp") for i in range(3)]
    gathered = jnp.concatenate(parts, axis=1)
    tile = 4 * BLOCK if seq_len % (4 * BLOCK) == 0 else BLOCK
    numerator, aux = pl.pallas_call(
        functools.partial(cell_local_kernel, tile=tile),
        out_shape=(
            jax.ShapeDtypeStruct((seq_len, width), jnp.float32),
            jax.ShapeDtypeStruct((seq_len, 128), jnp.float32),
        ),
        compiler_params=params,
        cost_estimate=pl.CostEstimate(flops=5 * 10**9, bytes_accessed=2**21, transcendentals=0),
        name="cell_local",
    )(query, keys, values, forget_pre, input_pre)
    rows = pl.pallas_call(
        functools.partial(cell_join_kernel, axis="sp"),
        out_shape=jax.ShapeDtypeStruct((seq_len, width), jnp.bfloat16),
        scratch_shapes=[pltpu.VMEM((width, width), jnp.float32)],
        compiler_params=params,
        name="cell_join",
    )(query, numerator, aux, gathered)
    return rows


def sp_tp_barrier(barrier, counts):
    total = 0
    for axis, count in counts.items():
        place = lax.axis_index(axis)
        for step in range(1, count):
            pl.semaphore_signal(
                barrier,
                inc=1,
                device_id={axis: lax.rem(place + step, count)},
                device_id_type=pl.DeviceIdType.MESH,
            )
        total += count - 1
    return total


def cell_kernel(
    q_ref,
    k_ref,
    v_ref,
    forget_ref,
    input_ref,
    out_ref,
    state_ref,
    piece_ref,
    extra_ref,
    prefix_ref,
    mat_ref,
    num_ref,
    aux_ref,
    rows_ref,
    send_sems,
    recv_sems,
    extra_send_sems,
    extra_recv_sems,
    back_send_sems,
    back_recv_sems,
    turn_send_sems,
    turn_recv_sems,
    own_sem,
    *,
    count,
    heads,
    tile,
):
    seq_len, width = q_ref.shape
    cut = width // count
    place = lax.axis_index("sp")
    head = lax.axis_index("tp")
    barrier = pltpu.get_barrier_semaphore()
    greeted = sp_tp_barrier(barrier, {"sp": count, "tp": heads})
    log_forget, cum_row, gap_row = log_rows(forget_ref, input_ref)
    total = jnp.sum(log_forget, axis=1, keepdims=True)
    best = jnp.max(gap_row, axis=1, keepdims=True)
    keep_row = jnp.exp(gap_row - best) * width ** (-0.5)
    weighted = k_ref[...].astype(jnp.float32).T * keep_row
    high, low = split_two(weighted)
    v_all = v_ref[...]
    state_ref[0:width, :] = jnp.dot(high, v_all, preferred_element_type=jnp.float32) + jnp.dot(
        low, v_all, preferred_element_type=jnp.float32
    )
    vector = jnp.dot(
        jnp.broadcast_to(keep_row, (8, seq_len)),
        k_ref[...].astype(jnp.float32),
        precision=HIGHEST,
        preferred_element_type=jnp.float32,
    )[0:1]
    lanes = jnp.zeros((1, width), jnp.float32)
    state_ref[width : width + EXTRA, :] = jnp.concatenate(
        [vector, lanes + total, lanes + total + best, jnp.zeros((EXTRA - 3, width), jnp.float32)],
        axis=0,
    )
    pl.semaphore_wait(barrier, greeted)
    sends = []
    for step in range(1, count):
        peer = lax.rem(place + step, count)
        extra_copy = pltpu.make_async_remote_copy(
            src_ref=state_ref.at[pl.ds(width, EXTRA)],
            dst_ref=extra_ref.at[place],
            send_sem=extra_send_sems.at[step - 1],
            recv_sem=extra_recv_sems.at[step - 1],
            device_id={"sp": peer},
            device_id_type=pl.DeviceIdType.MESH,
        )
        piece_copy = pltpu.make_async_remote_copy(
            src_ref=state_ref.at[pl.ds(pl.multiple_of(peer * cut, cut), cut)],
            dst_ref=piece_ref.at[place],
            send_sem=send_sems.at[step - 1],
            recv_sem=recv_sems.at[step - 1],
            device_id={"sp": peer},
            device_id_type=pl.DeviceIdType.MESH,
        )
        extra_copy.start()
        piece_copy.start()
        sends += [extra_copy, piece_copy]
    extra_ref[place] = state_ref[width : width + EXTRA, :]
    piece_ref[place] = state_ref[pl.ds(pl.multiple_of(place * cut, cut), cut), :]

    for first in range(0, seq_len, tile):
        span = first + tile
        row, col = col_mask(first, tile, span)
        causal = col <= row
        own = (col // BLOCK) == (row // BLOCK)
        gap = jnp.where(causal, gap_row[:, :span], -jnp.inf)
        top = jnp.max(gap, axis=1, keepdims=True)
        cum = jnp.sum(jnp.where(causal, log_forget[:, :span], 0.0), axis=1, keepdims=True)
        scores = lax.dot_general(
            q_ref[first:span, :],
            k_ref[0:span, :],
            (((1,), (1,)), ((), ())),
            preferred_element_type=jnp.float32,
        ) * width ** (-0.5)
        weights = scores * jnp.exp(gap - top)
        high = weights.astype(jnp.bfloat16)
        high_float = high.astype(jnp.float32)
        low_float = jnp.where(own, 0.0, weights - high_float)
        v = v_ref[0:span, :]
        num_ref[first:span, :] = jnp.dot(high, v, preferred_element_type=jnp.float32) + jnp.dot(
            low_float.astype(jnp.bfloat16), v, preferred_element_type=jnp.float32
        )
        den = jnp.sum(high_float + low_float, axis=1, keepdims=True)
        lane = lax.broadcasted_iota(jnp.int32, (tile, 128), 1)
        aux_ref[first:span, :] = jnp.where(lane == 0, den, jnp.where(lane == 1, top, cum))

    for copy in sends:
        copy.wait()

    running = jnp.zeros((cut, width), jnp.float32)
    vector = jnp.zeros((1, width), jnp.float32)
    far_max = jnp.full((1, width), FLOOR_LOG, jnp.float32)
    own_vector, own_max = vector, far_max
    for step in range(count):
        prefix_ref[step] = running
        own_vector = jnp.where(place == step, vector, own_vector)
        own_max = jnp.where(place == step, far_max, own_max)
        if step < count - 1:
            extra = extra_ref[step]
            new_max, step_total = extra[2:3], extra[1:2]
            joined = jnp.maximum(step_total + far_max, new_max)
            keep_old = jnp.exp(step_total + far_max - joined)
            keep_new = jnp.exp(new_max - joined)
            running = keep_old * running + keep_new * piece_ref[step]
            vector = keep_old * vector + keep_new * extra[0:1]
            far_max = joined
    backs = []
    for step in range(1, count):
        peer = lax.rem(place + step, count)
        back = pltpu.make_async_remote_copy(
            src_ref=prefix_ref.at[peer],
            dst_ref=mat_ref.at[pl.ds(pl.multiple_of(place * cut, cut), cut)],
            send_sem=back_send_sems.at[step - 1],
            recv_sem=back_recv_sems.at[step - 1],
            device_id={"sp": peer},
            device_id_type=pl.DeviceIdType.MESH,
        )
        back.start()
        backs.append(back)
    mat_ref[pl.ds(pl.multiple_of(place * cut, cut), cut), :] = prefix_ref[place]

    aux = aux_ref[...]
    den, top, cum = aux[:, 0:1], aux[:, 1:2], aux[:, 2:3]
    far = own_max[:, 0:1]
    joined = jnp.maximum(top, far)
    keep_own = jnp.exp(top - joined)
    keep_far = jnp.exp(far - joined)
    q_float = q_ref[...].astype(jnp.float32)
    far_den = jnp.sum(q_float * own_vector, axis=1, keepdims=True)
    denominator = keep_own * den + keep_far * far_den
    divisor = jnp.maximum(jnp.abs(denominator), jnp.exp(-(cum + joined)))
    for copy in backs:
        copy.wait()
    one, rest = split_two(mat_ref[...])
    two, three = split_two(mat_ref[...] - one.astype(jnp.float32))
    q = q_ref[...]
    far_num = (
        jnp.dot(q, one, preferred_element_type=jnp.float32)
        + jnp.dot(q, two, preferred_element_type=jnp.float32)
        + jnp.dot(q, three, preferred_element_type=jnp.float32)
    )
    numerator = keep_own * num_ref[...] + keep_far * far_num
    rows_ref[...] = (numerator / divisor).astype(rows_ref.dtype)

    share = seq_len // heads
    columns = pl.ds(pl.multiple_of(head * width, width), width)
    turns = []
    for step in range(1, heads):
        peer = lax.rem(head + step, heads)
        turn = pltpu.make_async_remote_copy(
            src_ref=rows_ref.at[pl.ds(pl.multiple_of(peer * share, share), share)],
            dst_ref=out_ref.at[:, columns],
            send_sem=turn_send_sems.at[step - 1],
            recv_sem=turn_recv_sems.at[step - 1],
            device_id={"tp": peer},
            device_id_type=pl.DeviceIdType.MESH,
        )
        turn.start()
        turns.append(turn)
    own_copy = pltpu.make_async_copy(
        rows_ref.at[pl.ds(pl.multiple_of(head * share, share), share)],
        out_ref.at[:, columns],
        own_sem,
    )
    own_copy.start()
    own_copy.wait()
    for turn in turns:
        turn.wait()


def run_cell_scan(query, keys, values, forget_pre, input_pre):
    seq_len, width = query.shape
    count, heads = lax.axis_size("sp"), lax.axis_size("tp")
    tile = 4 * BLOCK if seq_len % (4 * BLOCK) == 0 else BLOCK
    cut = width // count
    vmem = pl.BlockSpec(memory_space=pltpu.VMEM)
    dma = pltpu.SemaphoreType.DMA
    return pl.pallas_call(
        functools.partial(cell_kernel, count=count, heads=heads, tile=tile),
        out_shape=jax.ShapeDtypeStruct((seq_len // heads, heads * width), jnp.bfloat16),
        in_specs=[vmem] * 5,
        out_specs=vmem,
        scratch_shapes=[
            pltpu.VMEM((width + EXTRA, width), jnp.float32),
            pltpu.VMEM((count, cut, width), jnp.float32),
            pltpu.VMEM((count, EXTRA, width), jnp.float32),
            pltpu.VMEM((count, cut, width), jnp.float32),
            pltpu.VMEM((width, width), jnp.float32),
            pltpu.VMEM((seq_len, width), jnp.float32),
            pltpu.VMEM((seq_len, 128), jnp.float32),
            pltpu.VMEM((seq_len, width), jnp.bfloat16),
            dma((count - 1,)),
            dma((count - 1,)),
            dma((count - 1,)),
            dma((count - 1,)),
            dma((count - 1,)),
            dma((count - 1,)),
            dma((heads - 1,)),
            dma((heads - 1,)),
            dma(()),
        ],
        compiler_params=pltpu.CompilerParams(
            vmem_limit_bytes=VMEM_LIMIT, collective_id=3, has_side_effects=True
        ),
        cost_estimate=pl.CostEstimate(flops=10**10, bytes_accessed=2**21, transcendentals=0),
        name="cell",
    )(query, keys, values, forget_pre, input_pre)


def token_cell(query, keys, values, forget_pre, input_pre):
    if query.shape[1] % (8 * lax.axis_size("sp")) == 0:
        return run_cell_scan(query, keys, values, forget_pre, input_pre)
    rows = run_cell(query, keys, values, forget_pre, input_pre)
    return lax.all_to_all(rows, "tp", split_axis=0, concat_axis=1, tiled=True)


def slot_select(expert_ids, expert_count, capacity):
    flat_ids = expert_ids.reshape(-1)
    one_hot = (flat_ids[:, None] == jnp.arange(expert_count, dtype=jnp.int32)[None, :]).astype(
        jnp.int32
    )
    slot_rank = jnp.sum((jnp.cumsum(one_hot, axis=0) - 1) * one_hot, axis=1)
    target = flat_ids * capacity + slot_rank
    return (
        jnp.arange(expert_count * capacity, dtype=jnp.int32)[:, None] == target[None, :]
    ).astype(jnp.bfloat16)


def exchange_kernel(send_ref, recv_ref, send_sems, recv_sems, own_sem, *, axis, count):
    place = lax.axis_index(axis)
    barrier = pltpu.get_barrier_semaphore()
    for step in range(1, count):
        peer = lax.rem(place + step, count)
        pl.semaphore_signal(
            barrier, inc=1, device_id={axis: peer}, device_id_type=pl.DeviceIdType.MESH
        )
    own = pltpu.make_async_copy(send_ref.at[place], recv_ref.at[place], own_sem)
    own.start()
    pl.semaphore_wait(barrier, count - 1)
    copies = []
    for step in range(1, count):
        peer = lax.rem(place + step, count)
        copy = pltpu.make_async_remote_copy(
            src_ref=send_ref.at[peer],
            dst_ref=recv_ref.at[place],
            send_sem=send_sems.at[step - 1],
            recv_sem=recv_sems.at[step - 1],
            device_id={axis: peer},
            device_id_type=pl.DeviceIdType.MESH,
        )
        copy.start()
        copies.append(copy)
    own.wait()
    for copy in copies:
        copy.wait()


def exchange(blocks, axis, collective_id):
    count = lax.axis_size(axis)
    grouped = blocks.reshape((count, -1) + blocks.shape[2:])
    out = pl.pallas_call(
        functools.partial(exchange_kernel, axis=axis, count=count),
        out_shape=jax.ShapeDtypeStruct(grouped.shape, grouped.dtype),
        in_specs=[pl.BlockSpec(memory_space=pl.ANY)],
        out_specs=pl.BlockSpec(memory_space=pl.ANY),
        scratch_shapes=[
            pltpu.SemaphoreType.DMA((count - 1,)),
            pltpu.SemaphoreType.DMA((count - 1,)),
            pltpu.SemaphoreType.DMA(()),
        ],
        compiler_params=pltpu.CompilerParams(collective_id=collective_id, has_side_effects=True),
        name="exchange",
    )(grouped)
    return out.reshape(blocks.shape)


def run_experts(arrived, w_gate, w_up, w_down, sources):
    local_count = w_gate.shape[0]
    grouped = arrived.reshape(sources, local_count, arrived.shape[1], arrived.shape[2])
    gate_pre = jnp.einsum("pesd,edf->pesf", grouped, w_gate, preferred_element_type=jnp.float32)
    up_pre = jnp.einsum("pesd,edf->pesf", grouped, w_up, preferred_element_type=jnp.float32)
    active = (jax.nn.silu(gate_pre) * up_pre).astype(jnp.bfloat16)
    result = jnp.einsum(
        "pesf,efd->pesd", active, w_down, preferred_element_type=jnp.float32
    ).astype(jnp.bfloat16)
    return result.reshape(arrived.shape)


def line_kernel(
    rows_ref,
    mix_ref,
    info_ref,
    gate_hbm,
    up_hbm,
    down_hbm,
    out_ref,
    gate_ref,
    up_ref,
    down_ref,
    infos_ref,
    held_ref,
    cross_ref,
    crossed_ref,
    answer_ref,
    done_ref,
    batch_ref,
    part_ref,
    own_ref,
    sum_ref,
    load_sems,
    info_send,
    info_recv,
    row_send,
    row_recv,
    cross_send,
    cross_recv,
    answer_send,
    answer_recv,
    sum_send,
    sum_recv,
    *,
    line,
    halves,
    slots,
    pieces,
):
    place = lax.axis_index("sp")
    here = place // 2
    side = lax.rem(place, 2)
    twin = place + 1 - 2 * side
    units = line * halves
    tokens = rows_ref.shape[1]
    grain = tokens // pieces
    last = line - 1

    def remote(src, dst, send, recv, peer):
        return pltpu.make_async_remote_copy(
            src_ref=src,
            dst_ref=dst,
            send_sem=send,
            recv_sem=recv,
            device_id={"sp": peer},
            device_id_type=pl.DeviceIdType.MESH,
        )

    loads = [
        pltpu.make_async_copy(src, dst, load_sems.at[i])
        for i, (src, dst) in enumerate(
            [(gate_hbm, gate_ref), (up_hbm, up_ref), (down_hbm, down_ref)]
        )
    ]
    for load in loads:
        load.start()

    barrier = pltpu.get_barrier_semaphore()
    for step in range(1, line):
        pl.semaphore_signal(
            barrier,
            inc=1,
            device_id={"sp": lax.rem(here + step, line) * 2 + side},
            device_id_type=pl.DeviceIdType.MESH,
        )
    pl.semaphore_signal(
        barrier, inc=1, device_id={"sp": twin}, device_id_type=pl.DeviceIdType.MESH
    )
    pl.semaphore_wait(barrier, line)

    def info_copy(step):
        peer = lax.rem(here + step, line)
        return remote(
            info_ref,
            infos_ref.at[here],
            info_send.at[step - 1],
            info_recv.at[step - 1],
            peer * 2 + side,
        )

    def row_copy(src, source, half, way):
        unit = source * halves + half
        return remote(
            src,
            held_ref.at[unit],
            row_send.at[way, unit],
            row_recv.at[unit],
            place + (4 * way - 2),
        )

    def cross_copy(unit):
        return remote(
            cross_ref.at[unit],
            crossed_ref.at[unit],
            cross_send.at[unit],
            cross_recv.at[unit],
            twin,
        )

    def answer_copy(unit):
        return remote(
            answer_ref.at[unit],
            done_ref.at[unit, pl.ds(slots, slots)],
            answer_send.at[unit],
            answer_recv.at[unit],
            twin,
        )

    def sum_copy(target, half, way, piece):
        landing = ((target + way) * halves + half) * pieces + piece
        leaving = (target * halves + half) * pieces + piece
        return remote(
            part_ref.at[leaving],
            sum_ref.at[landing],
            sum_send.at[leaving],
            sum_recv.at[landing],
            place + (4 * way - 2),
        )

    def sum_wait(landing):
        remote(
            part_ref.at[0], sum_ref.at[landing], sum_send.at[0], sum_recv.at[landing], twin
        ).wait_recv()

    for step in range(1, line):
        info_copy(step).start()
    for way in range(2):

        @pl.when((here < last) if way else (here > 0))
        def _():
            row_copy(rows_ref.at[0], here, 0, way).start()

    def later_halves(way):
        for half in range(1, halves):
            row_copy(rows_ref.at[half], here, half, way).start()

    @pl.when(here == 0)
    def _():
        later_halves(1)

    @pl.when(here == last)
    def _():
        later_halves(0)

    infos_ref[here] = info_ref[...]
    for half in range(halves):
        held_ref[here * halves + half] = rows_ref[half]
    batch_ref[...] = jnp.zeros_like(batch_ref)
    for step in range(1, line):
        info_copy(step).wait()

    shorter = jnp.minimum(here, last - here)

    def in_stream(p, reach):
        first = p < reach
        turn = p - reach
        ahead = jnp.where(first, p + 1, reach - turn // (halves - 1))
        return ahead, jnp.where(first, 0, 1 + lax.rem(turn, halves - 1))

    def source_of(k):
        p = k - halves
        both = shorter * 2 * halves
        paired = p < both
        way = jnp.where(paired, lax.rem(p, 2), jnp.where(here < last - here, 1, 0))
        spot = jnp.where(paired, p // 2, p - shorter * halves)
        reach = jnp.where(way == 1, last - here, here)
        ahead, half = in_stream(spot, reach)
        is_own = k < halves
        final = spot == reach * halves - 1
        return (
            jnp.where(is_own, here, here + ahead * (2 * way - 1)),
            jnp.where(is_own, k, half),
            final,
        )

    def matches(source, half, weighted):
        info = infos_ref[source, half]
        rank = lax.broadcasted_iota(jnp.int32, (slots, tokens), 0).astype(jnp.float32)
        tables = []
        for expert in (place, twin):
            name = expert.astype(jnp.float32)
            table = jnp.zeros((slots, tokens), jnp.float32)
            for route in range(2):
                hit = jnp.where(info[route : route + 1] == name, info[2 + route : 3 + route], -1.0)
                value = info[4 + route : 5 + route] if weighted else 1.0
                table += jnp.where(hit == rank, value, 0.0)
            tables.append(table)
        return jnp.concatenate(tables, axis=0)

    first_way = jnp.where(last - here <= here, 0, 1)

    def relay(way, spot):
        reach = jnp.where(way == 1, last - here, here)

        @pl.when((spot >= 0) & (spot < reach * halves) & (here > 0) & (here < last))
        def _():
            ahead, half = in_stream(spot, reach)
            target = here + ahead * (2 * way - 1)
            for piece in range(pieces):
                unit = (target * halves + half) * pieces + piece
                landing = ((target + way) * halves + half) * pieces + piece
                sum_wait(landing)
                part_ref[unit] = (
                    part_ref[unit].astype(jnp.float32) + sum_ref[landing].astype(jnp.float32)
                ).astype(jnp.bfloat16)
                sum_copy(target, half, way, piece).start()

    def step_body(k, carry):
        @pl.when(k < units)
        def _():
            source, half, final = source_of(k)
            unit = source * halves + half

            @pl.when(source != here)
            def _():
                remote(
                    held_ref.at[unit], held_ref.at[unit], row_send.at[0, unit], row_recv.at[unit], twin
                ).wait_recv()

            @pl.when((source < here) & (here < last))
            def _():
                row_copy(held_ref.at[unit], source, half, 1).start()

                @pl.when(final)
                def _():
                    later_halves(1)

            @pl.when((source > here) & (here > 0))
            def _():
                row_copy(held_ref.at[unit], source, half, 0).start()

                @pl.when(final)
                def _():
                    later_halves(0)

            packed = jnp.dot(
                matches(source, half, False).astype(jnp.bfloat16),
                held_ref[unit],
                preferred_element_type=jnp.float32,
            ).astype(jnp.bfloat16)
            cross_ref[unit] = packed[slots:]
            cross_copy(unit).start()
            batch_ref[0:slots, :] = packed[:slots]

        @pl.when(k == 0)
        def _():
            for load in loads:
                load.wait()

        relay(first_way, k - units)

        @pl.when((k > 0) & (k <= units))
        def _():
            source, half, _ = source_of(k - 1)
            unit = source * halves + half
            cross_copy(unit).wait_recv()
            batch_ref[slots : 2 * slots, :] = crossed_ref[unit]

        @pl.when(k <= units)
        def _():
            rows = batch_ref[...]
            gate = jnp.dot(rows, gate_ref[0], preferred_element_type=jnp.float32)
            up = jnp.dot(rows, up_ref[0], preferred_element_type=jnp.float32)
            active = (jax.nn.silu(gate) * up).astype(jnp.bfloat16)
            batch_ref[...] = jnp.dot(
                active, down_ref[0], preferred_element_type=jnp.float32
            ).astype(jnp.bfloat16)

        @pl.when(k < units)
        def _():
            source, half, _ = source_of(k)
            done_ref[source * halves + half, 0:slots, :] = batch_ref[0:slots, :]

        @pl.when((k > 0) & (k <= units))
        def _():
            source, half, _ = source_of(k - 1)
            unit = source * halves + half
            answer_ref[unit] = batch_ref[slots : 2 * slots, :]

            @pl.when(source != here)
            def _():
                answer_copy(unit).start()

        @pl.when(k == units)
        def _():
            for half in range(halves):
                answer_copy(here * halves + half).start()

        relay(1 - first_way, k - units - 2)

        @pl.when(k > 1 + halves)
        def _():
            source, half, _ = source_of(jnp.where(k > units + 1, k - units - 2, k - 2))
            unit = source * halves + half
            answer_copy(unit).wait_recv()
            high, low = split_two(matches(source, half, True))
            answers = done_ref[unit]
            turned = (((0,), (0,)), ((), ()))
            part = lax.dot_general(
                high, answers, turned, preferred_element_type=jnp.float32
            ) + lax.dot_general(low, answers, turned, preferred_element_type=jnp.float32)

            @pl.when(source == here)
            def _():
                own_ref[half] = part

            @pl.when(source != here)
            def _():
                for piece in range(pieces):
                    part_ref[unit * pieces + piece] = part[
                        piece * grain : (piece + 1) * grain
                    ].astype(jnp.bfloat16)

            @pl.when((source < here) & (here == last))
            def _():
                for piece in range(pieces):
                    sum_copy(source, half, 0, piece).start()

            @pl.when((source > here) & (here == 0))
            def _():
                for piece in range(pieces):
                    sum_copy(source, half, 1, piece).start()

        return carry

    lax.fori_loop(0, units + 2 + halves, step_body, 0)

    for half in range(halves):
        for piece in range(pieces):
            rows = pl.ds(piece * grain, grain)
            own_ref[half, rows] = own_ref[half, rows] + mix_ref[half, rows]
            for way in range(2):

                @pl.when((here > 0) if way else (here < last))
                def _():
                    landing = ((here + way) * halves + half) * pieces + piece
                    sum_wait(landing)
                    own_ref[half, rows] = own_ref[half, rows] + sum_ref[landing].astype(jnp.float32)

            out_ref[half, rows] = own_ref[half, rows].astype(out_ref.dtype)

    def drain(unit, carry):
        source = unit // halves
        half = lax.rem(unit, halves)
        cross_copy(unit).wait_send()
        answer_copy(unit).wait_send()

        @pl.when((source <= here) & (here < last))
        def _():
            row_copy(held_ref.at[unit], source, half, 1).wait_send()

        @pl.when((source >= here) & (here > 0))
        def _():
            row_copy(held_ref.at[unit], source, half, 0).wait_send()

        @pl.when(source != here)
        def _():
            for piece in range(pieces):
                sum_copy(source, half, 0, piece).wait_send()

        return carry

    lax.fori_loop(0, units, drain, 0)


def run_line(normed_rows, after_mix, info, w_gate, w_up, w_down, slots):
    count = lax.axis_size("sp")
    line, halves = count // 2, info.shape[0]
    units = line * halves
    row_count, width = normed_rows.shape
    tokens = row_count // halves
    pieces = 2
    grain = tokens // pieces
    vmem = pl.BlockSpec(memory_space=pltpu.VMEM)
    whole = pl.BlockSpec(memory_space=pl.ANY)
    dma = pltpu.SemaphoreType.DMA
    out = pl.pallas_call(
        functools.partial(line_kernel, line=line, halves=halves, slots=slots, pieces=pieces),
        out_shape=jax.ShapeDtypeStruct((halves, tokens, width), jnp.bfloat16),
        in_specs=[vmem, vmem, vmem, whole, whole, whole],
        out_specs=vmem,
        scratch_shapes=[
            pltpu.VMEM(w_gate.shape, jnp.bfloat16),
            pltpu.VMEM(w_up.shape, jnp.bfloat16),
            pltpu.VMEM(w_down.shape, jnp.bfloat16),
            pltpu.VMEM((line,) + info.shape, jnp.float32),
            pltpu.VMEM((units, tokens, width), jnp.bfloat16),
            pltpu.VMEM((units, slots, width), jnp.bfloat16),
            pltpu.VMEM((units, slots, width), jnp.bfloat16),
            pltpu.VMEM((units, slots, width), jnp.bfloat16),
            pltpu.VMEM((units, 2 * slots, width), jnp.bfloat16),
            pltpu.VMEM((2 * slots, width), jnp.bfloat16),
            pltpu.VMEM((units * pieces, grain, width), jnp.bfloat16),
            pltpu.VMEM((halves, tokens, width), jnp.float32),
            pltpu.VMEM(((units + halves) * pieces, grain, width), jnp.bfloat16),
            dma((3,)),
            dma((line - 1,)),
            dma((line - 1,)),
            dma((2, units)),
            dma((units,)),
            dma((units,)),
            dma((units,)),
            dma((units,)),
            dma((units,)),
            dma((units * pieces,)),
            dma(((units + halves) * pieces,)),
        ],
        compiler_params=pltpu.CompilerParams(
            vmem_limit_bytes=VMEM_LIMIT, collective_id=4, has_side_effects=True
        ),
        cost_estimate=pl.CostEstimate(flops=10**10, bytes_accessed=2**23, transcendentals=0),
        name="experts",
    )(
        normed_rows.reshape(halves, tokens, width),
        after_mix.reshape(halves, tokens, width),
        info,
        w_gate,
        w_up,
        w_down,
    )
    return out.reshape(row_count, width)


def route_info(routes, route_weight, halves):
    tokens = routes.shape[0] // halves
    ids = routes.reshape(halves, -1)
    order = jnp.arange(ids.shape[1], dtype=jnp.int32)
    same = (ids[:, :, None] == ids[:, None, :]) & (order[None, None, :] < order[None, :, None])
    rank = jnp.sum(same.astype(jnp.float32), axis=2)

    def turned(a):
        return a.astype(jnp.float32).reshape(halves, tokens, -1).transpose(0, 2, 1)

    return jnp.concatenate(
        [turned(routes), turned(rank), turned(route_weight), jnp.zeros((halves, 2, tokens), jnp.float32)],
        axis=1,
    )


def shards(
    resid,
    query,
    keys,
    values,
    out_gate,
    forget_pre,
    input_pre,
    head_gain,
    out_proj,
    ffn_gain,
    routes,
    route_scores,
    w_gate,
    w_up,
    w_down,
):
    head_width = query.shape[1]
    row_count, route_count = routes.shape
    sources = lax.axis_size("sp")
    local_experts = w_gate.shape[0]
    expert_count = local_experts * sources
    half_rows = row_count // 2
    capacity = max(2, 2 * half_rows * route_count // expert_count)
    route_weight = route_scores / jnp.sum(route_scores, axis=1, keepdims=True)
    token_rows = token_cell(query, keys, values, forget_pre, input_pre)
    cell_float = token_rows.astype(jnp.float32)
    headed = (
        cell_float
        * lax.rsqrt(jnp.mean(cell_float * cell_float, axis=1, keepdims=True) + EPS)
        * head_gain[None, :]
    )
    gated_out = (headed * jax.nn.sigmoid(out_gate.astype(jnp.float32))).astype(jnp.bfloat16)
    after_mix = resid.astype(jnp.float32) + jnp.dot(
        gated_out, out_proj, preferred_element_type=jnp.float32
    )
    normed_rows = (
        after_mix
        * lax.rsqrt(jnp.mean(after_mix * after_mix, axis=1, keepdims=True) + EPS)
        * ffn_gain[None, :]
    ).astype(jnp.bfloat16)
    dense = local_experts == 1 and sources % 2 == 0 and sources <= 8 and route_count == 2
    if dense and 2 * capacity >= half_rows and capacity % 16 == 0 and half_rows % 32 == 0:
        info = route_info(routes, route_weight, 2)
        return run_line(normed_rows, after_mix, info, w_gate, w_up, w_down, capacity)
    selects = [
        slot_select(
            routes[half_idx * half_rows : (half_idx + 1) * half_rows], expert_count, capacity
        )
        for half_idx in range(2)
    ]

    def pack_rows(half_idx):
        selection = (
            selects[half_idx].reshape(expert_count * capacity, half_rows, route_count).sum(axis=2)
        )
        packed = jnp.dot(
            selection,
            normed_rows[half_idx * half_rows : (half_idx + 1) * half_rows],
            preferred_element_type=jnp.float32,
        )
        return packed.astype(jnp.bfloat16).reshape(expert_count, capacity, normed_rows.shape[1])

    send_rows = jnp.concatenate([pack_rows(0), pack_rows(1)], axis=1)
    finished = run_experts(
        exchange(send_rows, "sp", 1),
        w_gate,
        w_up,
        w_down,
        sources,
    )
    returned = exchange(finished, "sp", 2)
    answers = [returned[:, :capacity], returned[:, capacity:]]
    pieces = []
    for half_idx in range(2):
        gathered = lax.dot_general(
            selects[half_idx],
            answers[half_idx].reshape(expert_count * capacity, -1),
            (((0,), (0,)), ((), ())),
            preferred_element_type=jnp.float32,
        )
        weights_half = route_weight[half_idx * half_rows : (half_idx + 1) * half_rows]
        pieces.append(
            jnp.sum(gathered.reshape(half_rows, route_count, -1) * weights_half[:, :, None], axis=1)
        )
    return (after_mix + jnp.concatenate(pieces, axis=0)).astype(jnp.bfloat16)


def solution(mesh):
    placed = (
        P(("sp", "tp"), None),
        P("sp", "tp"),
        P("sp", "tp"),
        P("sp", "tp"),
        P(("sp", "tp"), None),
        P("tp", "sp"),
        P("tp", "sp"),
        P(),
        P(),
        P(),
        P(("sp", "tp"), None),
        P(("sp", "tp"), None),
        P("sp", None, None),
        P("sp", None, None),
        P("sp", None, None),
    )
    return jax.shard_map(
        shards, mesh=mesh, in_specs=placed, out_specs=P(("sp", "tp"), None), check_vma=False
    )
```

```python
import functools

import jax
import jax.numpy as jnp
from jax import lax
from jax.experimental import pallas as pl
from jax.experimental.pallas import tpu as pltpu
from jax.sharding import PartitionSpec as P

BLOCK = 64


EPS = 1e-06
FLOOR_LOG = -1e30
HIGHEST = lax.Precision.HIGHEST


EXTRA = 8
VMEM_LIMIT = 56 * 1024 * 1024
LAYER_VMEM = 60 * 1024 * 1024
WEIGHT_PIECES = 4


def col_mask(first_row, rows, cols):
    row = lax.broadcasted_iota(jnp.int32, (rows, cols), 0) + first_row
    col = lax.broadcasted_iota(jnp.int32, (rows, cols), 1)
    return row, col


def split_two(a):
    high = a.astype(jnp.bfloat16)
    return high, (a - high.astype(jnp.float32)).astype(jnp.bfloat16)


def log_rows(forget_ref, input_ref):
    pre = forget_ref[...]
    log_forget = jnp.minimum(pre, 0.0) - jnp.log1p(jnp.exp(-jnp.abs(pre)))
    seq_len = pre.shape[1]
    row, col = col_mask(0, seq_len, seq_len)
    upper = jnp.where(row <= col, 1.0, 0.0).astype(jnp.bfloat16)
    one, rest = split_two(log_forget)
    two, three = split_two(log_forget - one.astype(jnp.float32))
    stacked = jnp.concatenate([one, two, three, jnp.zeros((13, seq_len), jnp.bfloat16)], axis=0)
    sums = jnp.dot(stacked, upper, preferred_element_type=jnp.float32)
    cum_row = sums[0:1] + sums[1:2] + sums[2:3]
    return log_forget, cum_row, input_ref[...] - cum_row


def cell_state_kernel(k_ref, v_ref, forget_ref, input_ref, state_ref):
    width = k_ref.shape[1]
    seq_len = k_ref.shape[0]
    log_forget, cum_row, gap_row = log_rows(forget_ref, input_ref)
    total = jnp.sum(log_forget, axis=1, keepdims=True)
    top = jnp.max(gap_row, axis=1, keepdims=True)
    keep_row = jnp.exp(gap_row - top) * width ** (-0.5)
    k_turned = k_ref[...].astype(jnp.float32).T
    weighted = k_turned * keep_row
    high, low = split_two(weighted)
    v = v_ref[...]
    state_ref[0:width, :] = jnp.dot(high, v, preferred_element_type=jnp.float32) + jnp.dot(
        low, v, preferred_element_type=jnp.float32
    )
    vector = jnp.dot(
        jnp.broadcast_to(keep_row, (8, seq_len)),
        k_ref[...].astype(jnp.float32),
        precision=HIGHEST,
        preferred_element_type=jnp.float32,
    )[0:1]
    lanes = jnp.zeros((1, width), jnp.float32)
    state_ref[width : width + EXTRA, :] = jnp.concatenate(
        [vector, lanes + total, lanes + total + top, jnp.zeros((EXTRA - 3, width), jnp.float32)],
        axis=0,
    )


def cell_local_kernel(q_ref, k_ref, v_ref, forget_ref, input_ref, num_ref, aux_ref, *, tile):
    seq_len, width = q_ref.shape
    log_forget, cum_row, gap_row = log_rows(forget_ref, input_ref)
    for first in range(0, seq_len, tile):
        span = first + tile
        row, col = col_mask(first, tile, span)
        causal = col <= row
        own = (col // BLOCK) == (row // BLOCK)
        gap = jnp.where(causal, gap_row[:, :span], -jnp.inf)
        top = jnp.max(gap, axis=1, keepdims=True)
        cum = jnp.sum(jnp.where(causal, log_forget[:, :span], 0.0), axis=1, keepdims=True)
        scores = lax.dot_general(
            q_ref[first:span, :],
            k_ref[0:span, :],
            (((1,), (1,)), ((), ())),
            preferred_element_type=jnp.float32,
        ) * width ** (-0.5)
        weights = scores * jnp.exp(gap - top)
        high = weights.astype(jnp.bfloat16)
        high_float = high.astype(jnp.float32)
        low_float = jnp.where(own, 0.0, weights - high_float)
        v = v_ref[0:span, :]
        num_ref[first:span, :] = jnp.dot(high, v, preferred_element_type=jnp.float32) + jnp.dot(
            low_float.astype(jnp.bfloat16), v, preferred_element_type=jnp.float32
        )
        den = jnp.sum(high_float + low_float, axis=1, keepdims=True)
        lane = lax.broadcasted_iota(jnp.int32, (tile, 128), 1)
        aux_ref[first:span, :] = jnp.where(lane == 0, den, jnp.where(lane == 1, top, cum))


def cell_join_kernel(q_ref, num_ref, aux_ref, states_ref, rows_ref, mat_ref, *, axis):
    width = q_ref.shape[1]
    place = lax.axis_index(axis)
    mat_ref[...] = jnp.zeros_like(mat_ref)

    def join(step, carry):
        vector, old_max = carry
        extra = states_ref[step, width : width + EXTRA, :]
        new_max, total = extra[2:3], extra[1:2]
        joined = jnp.maximum(total + old_max, new_max)
        keep_old = jnp.exp(total + old_max - joined)
        keep_new = jnp.exp(new_max - joined)
        mat_ref[...] = keep_old * mat_ref[...] + keep_new * states_ref[step, 0:width, :]
        return keep_old * vector + keep_new * extra[0:1], joined

    vector, far_max = lax.fori_loop(
        0,
        place,
        join,
        (jnp.zeros((1, width), jnp.float32), jnp.full((1, width), FLOOR_LOG, jnp.float32)),
    )
    aux = aux_ref[...]
    den, top, cum = aux[:, 0:1], aux[:, 1:2], aux[:, 2:3]
    far = far_max[:, 0:1]
    joined = jnp.maximum(top, far)
    keep_own = jnp.exp(top - joined)
    keep_far = jnp.exp(far - joined)
    q_float = q_ref[...].astype(jnp.float32)
    one, rest = split_two(mat_ref[...])
    two, three = split_two(mat_ref[...] - one.astype(jnp.float32))
    q = q_ref[...]
    far_num = (
        jnp.dot(q, one, preferred_element_type=jnp.float32)
        + jnp.dot(q, two, preferred_element_type=jnp.float32)
        + jnp.dot(q, three, preferred_element_type=jnp.float32)
    )
    far_den = jnp.sum(q_float * vector, axis=1, keepdims=True)
    numerator = keep_own * num_ref[...] + keep_far * far_num
    denominator = keep_own * den + keep_far * far_den
    divisor = jnp.maximum(jnp.abs(denominator), jnp.exp(-(cum + joined)))
    rows_ref[...] = (numerator / divisor).astype(rows_ref.dtype)


def run_cell(query, keys, values, forget_pre, input_pre):
    seq_len, width = query.shape
    params = pltpu.CompilerParams(vmem_limit_bytes=VMEM_LIMIT)
    state = pl.pallas_call(
        cell_state_kernel,
        out_shape=jax.ShapeDtypeStruct((width + EXTRA, width), jnp.float32),
        compiler_params=params,
        cost_estimate=pl.CostEstimate(flops=10**9, bytes_accessed=2**20, transcendentals=0),
        name="cell_state",
    )(keys, values, forget_pre, input_pre)
    cut = (width + EXTRA) // 3
    parts = [lax.all_gather(state[i * cut : (i + 1) * cut], "sp") for i in range(3)]
    gathered = jnp.concatenate(parts, axis=1)
    tile = 4 * BLOCK if seq_len % (4 * BLOCK) == 0 else BLOCK
    numerator, aux = pl.pallas_call(
        functools.partial(cell_local_kernel, tile=tile),
        out_shape=(
            jax.ShapeDtypeStruct((seq_len, width), jnp.float32),
            jax.ShapeDtypeStruct((seq_len, 128), jnp.float32),
        ),
        compiler_params=params,
        cost_estimate=pl.CostEstimate(flops=5 * 10**9, bytes_accessed=2**21, transcendentals=0),
        name="cell_local",
    )(query, keys, values, forget_pre, input_pre)
    rows = pl.pallas_call(
        functools.partial(cell_join_kernel, axis="sp"),
        out_shape=jax.ShapeDtypeStruct((seq_len, width), jnp.bfloat16),
        scratch_shapes=[pltpu.VMEM((width, width), jnp.float32)],
        compiler_params=params,
        name="cell_join",
    )(query, numerator, aux, gathered)
    return rows


def sp_tp_barrier(barrier, counts):
    total = 0
    for axis, count in counts.items():
        place = lax.axis_index(axis)
        for step in range(1, count):
            pl.semaphore_signal(
                barrier,
                inc=1,
                device_id={axis: lax.rem(place + step, count)},
                device_id_type=pl.DeviceIdType.MESH,
            )
        total += count - 1
    return total


def cell_kernel(
    q_ref,
    k_ref,
    v_ref,
    forget_ref,
    input_ref,
    out_ref,
    state_ref,
    piece_ref,
    extra_ref,
    prefix_ref,
    mat_ref,
    num_ref,
    aux_ref,
    rows_ref,
    send_sems,
    recv_sems,
    extra_send_sems,
    extra_recv_sems,
    back_send_sems,
    back_recv_sems,
    turn_send_sems,
    turn_recv_sems,
    own_sem,
    *,
    count,
    heads,
    tile,
):
    seq_len, width = q_ref.shape
    cut = width // count
    place = lax.axis_index("sp")
    head = lax.axis_index("tp")
    barrier = pltpu.get_barrier_semaphore()
    greeted = sp_tp_barrier(barrier, {"sp": count, "tp": heads})
    log_forget, cum_row, gap_row = log_rows(forget_ref, input_ref)
    total = jnp.sum(log_forget, axis=1, keepdims=True)
    best = jnp.max(gap_row, axis=1, keepdims=True)
    keep_row = jnp.exp(gap_row - best) * width ** (-0.5)
    weighted = k_ref[...].astype(jnp.float32).T * keep_row
    high, low = split_two(weighted)
    v_all = v_ref[...]
    state_ref[0:width, :] = jnp.dot(high, v_all, preferred_element_type=jnp.float32) + jnp.dot(
        low, v_all, preferred_element_type=jnp.float32
    )
    vector = jnp.dot(
        jnp.broadcast_to(keep_row, (8, seq_len)),
        k_ref[...].astype(jnp.float32),
        precision=HIGHEST,
        preferred_element_type=jnp.float32,
    )[0:1]
    lanes = jnp.zeros((1, width), jnp.float32)
    state_ref[width : width + EXTRA, :] = jnp.concatenate(
        [vector, lanes + total, lanes + total + best, jnp.zeros((EXTRA - 3, width), jnp.float32)],
        axis=0,
    )
    pl.semaphore_wait(barrier, greeted)
    sends = []
    for step in range(1, count):
        peer = lax.rem(place + step, count)
        extra_copy = pltpu.make_async_remote_copy(
            src_ref=state_ref.at[pl.ds(width, EXTRA)],
            dst_ref=extra_ref.at[place],
            send_sem=extra_send_sems.at[step - 1],
            recv_sem=extra_recv_sems.at[step - 1],
            device_id={"sp": peer},
            device_id_type=pl.DeviceIdType.MESH,
        )
        piece_copy = pltpu.make_async_remote_copy(
            src_ref=state_ref.at[pl.ds(pl.multiple_of(peer * cut, cut), cut)],
            dst_ref=piece_ref.at[place],
            send_sem=send_sems.at[step - 1],
            recv_sem=recv_sems.at[step - 1],
            device_id={"sp": peer},
            device_id_type=pl.DeviceIdType.MESH,
        )
        extra_copy.start()
        piece_copy.start()
        sends += [extra_copy, piece_copy]
    extra_ref[place] = state_ref[width : width + EXTRA, :]
    piece_ref[place] = state_ref[pl.ds(pl.multiple_of(place * cut, cut), cut), :]

    for first in range(0, seq_len, tile):
        span = first + tile
        row, col = col_mask(first, tile, span)
        causal = col <= row
        own = (col // BLOCK) == (row // BLOCK)
        gap = jnp.where(causal, gap_row[:, :span], -jnp.inf)
        top = jnp.max(gap, axis=1, keepdims=True)
        cum = jnp.sum(jnp.where(causal, log_forget[:, :span], 0.0), axis=1, keepdims=True)
        scores = lax.dot_general(
            q_ref[first:span, :],
            k_ref[0:span, :],
            (((1,), (1,)), ((), ())),
            preferred_element_type=jnp.float32,
        ) * width ** (-0.5)
        weights = scores * jnp.exp(gap - top)
        high = weights.astype(jnp.bfloat16)
        high_float = high.astype(jnp.float32)
        low_float = jnp.where(own, 0.0, weights - high_float)
        v = v_ref[0:span, :]
        num_ref[first:span, :] = jnp.dot(high, v, preferred_element_type=jnp.float32) + jnp.dot(
            low_float.astype(jnp.bfloat16), v, preferred_element_type=jnp.float32
        )
        den = jnp.sum(high_float + low_float, axis=1, keepdims=True)
        lane = lax.broadcasted_iota(jnp.int32, (tile, 128), 1)
        aux_ref[first:span, :] = jnp.where(lane == 0, den, jnp.where(lane == 1, top, cum))

    for copy in sends:
        copy.wait()

    running = jnp.zeros((cut, width), jnp.float32)
    vector = jnp.zeros((1, width), jnp.float32)
    far_max = jnp.full((1, width), FLOOR_LOG, jnp.float32)
    own_vector, own_max = vector, far_max
    for step in range(count):
        prefix_ref[step] = running
        own_vector = jnp.where(place == step, vector, own_vector)
        own_max = jnp.where(place == step, far_max, own_max)
        if step < count - 1:
            extra = extra_ref[step]
            new_max, step_total = extra[2:3], extra[1:2]
            joined = jnp.maximum(step_total + far_max, new_max)
            keep_old = jnp.exp(step_total + far_max - joined)
            keep_new = jnp.exp(new_max - joined)
            running = keep_old * running + keep_new * piece_ref[step]
            vector = keep_old * vector + keep_new * extra[0:1]
            far_max = joined
    backs = []
    for step in range(1, count):
        peer = lax.rem(place + step, count)
        back = pltpu.make_async_remote_copy(
            src_ref=prefix_ref.at[peer],
            dst_ref=mat_ref.at[pl.ds(pl.multiple_of(place * cut, cut), cut)],
            send_sem=back_send_sems.at[step - 1],
            recv_sem=back_recv_sems.at[step - 1],
            device_id={"sp": peer},
            device_id_type=pl.DeviceIdType.MESH,
        )
        back.start()
        backs.append(back)
    mat_ref[pl.ds(pl.multiple_of(place * cut, cut), cut), :] = prefix_ref[place]

    aux = aux_ref[...]
    den, top, cum = aux[:, 0:1], aux[:, 1:2], aux[:, 2:3]
    far = own_max[:, 0:1]
    joined = jnp.maximum(top, far)
    keep_own = jnp.exp(top - joined)
    keep_far = jnp.exp(far - joined)
    q_float = q_ref[...].astype(jnp.float32)
    far_den = jnp.sum(q_float * own_vector, axis=1, keepdims=True)
    denominator = keep_own * den + keep_far * far_den
    divisor = jnp.maximum(jnp.abs(denominator), jnp.exp(-(cum + joined)))
    for copy in backs:
        copy.wait()
    one, rest = split_two(mat_ref[...])
    two, three = split_two(mat_ref[...] - one.astype(jnp.float32))
    q = q_ref[...]
    far_num = (
        jnp.dot(q, one, preferred_element_type=jnp.float32)
        + jnp.dot(q, two, preferred_element_type=jnp.float32)
        + jnp.dot(q, three, preferred_element_type=jnp.float32)
    )
    numerator = keep_own * num_ref[...] + keep_far * far_num
    rows_ref[...] = (numerator / divisor).astype(rows_ref.dtype)

    share = seq_len // heads
    columns = pl.ds(pl.multiple_of(head * width, width), width)
    turns = []
    for step in range(1, heads):
        peer = lax.rem(head + step, heads)
        turn = pltpu.make_async_remote_copy(
            src_ref=rows_ref.at[pl.ds(pl.multiple_of(peer * share, share), share)],
            dst_ref=out_ref.at[:, columns],
            send_sem=turn_send_sems.at[step - 1],
            recv_sem=turn_recv_sems.at[step - 1],
            device_id={"tp": peer},
            device_id_type=pl.DeviceIdType.MESH,
        )
        turn.start()
        turns.append(turn)
    own_copy = pltpu.make_async_copy(
        rows_ref.at[pl.ds(pl.multiple_of(head * share, share), share)],
        out_ref.at[:, columns],
        own_sem,
    )
    own_copy.start()
    own_copy.wait()
    for turn in turns:
        turn.wait()


def run_cell_scan(query, keys, values, forget_pre, input_pre):
    seq_len, width = query.shape
    count, heads = lax.axis_size("sp"), lax.axis_size("tp")
    tile = 4 * BLOCK if seq_len % (4 * BLOCK) == 0 else BLOCK
    cut = width // count
    vmem = pl.BlockSpec(memory_space=pltpu.VMEM)
    dma = pltpu.SemaphoreType.DMA
    return pl.pallas_call(
        functools.partial(cell_kernel, count=count, heads=heads, tile=tile),
        out_shape=jax.ShapeDtypeStruct((seq_len // heads, heads * width), jnp.bfloat16),
        in_specs=[vmem] * 5,
        out_specs=vmem,
        scratch_shapes=[
            pltpu.VMEM((width + EXTRA, width), jnp.float32),
            pltpu.VMEM((count, cut, width), jnp.float32),
            pltpu.VMEM((count, EXTRA, width), jnp.float32),
            pltpu.VMEM((count, cut, width), jnp.float32),
            pltpu.VMEM((width, width), jnp.float32),
            pltpu.VMEM((seq_len, width), jnp.float32),
            pltpu.VMEM((seq_len, 128), jnp.float32),
            pltpu.VMEM((seq_len, width), jnp.bfloat16),
            dma((count - 1,)),
            dma((count - 1,)),
            dma((count - 1,)),
            dma((count - 1,)),
            dma((count - 1,)),
            dma((count - 1,)),
            dma((heads - 1,)),
            dma((heads - 1,)),
            dma(()),
        ],
        compiler_params=pltpu.CompilerParams(
            vmem_limit_bytes=VMEM_LIMIT, collective_id=3, has_side_effects=True
        ),
        cost_estimate=pl.CostEstimate(flops=10**10, bytes_accessed=2**21, transcendentals=0),
        name="cell",
    )(query, keys, values, forget_pre, input_pre)


def token_cell(query, keys, values, forget_pre, input_pre):
    if query.shape[1] % (8 * lax.axis_size("sp")) == 0:
        return run_cell_scan(query, keys, values, forget_pre, input_pre)
    rows = run_cell(query, keys, values, forget_pre, input_pre)
    return lax.all_to_all(rows, "tp", split_axis=0, concat_axis=1, tiled=True)


def layer_kernel(
    q_ref,
    k_ref,
    v_ref,
    forget_ref,
    input_ref,
    head_gain_ref,
    ffn_gain_ref,
    routes_ref,
    scores_ref,
    resid_hbm,
    out_gate_hbm,
    out_proj_hbm,
    gate_hbm,
    up_hbm,
    down_hbm,
    out_ref,
    state_ref,
    piece_ref,
    extra_ref,
    prefix_ref,
    mat_ref,
    num_ref,
    aux_ref,
    cell_ref,
    token_ref,
    resid_ref,
    out_gate_ref,
    out_proj_ref,
    gate_ref,
    up_ref,
    down_ref,
    twin_gate_ref,
    twin_up_ref,
    twin_down_ref,
    infos_ref,
    rows_ref,
    held_ref,
    cross_ref,
    done_ref,
    part_ref,
    own_ref,
    sum_ref,
    load_sems,
    own_sem,
    send_sems,
    recv_sems,
    extra_send_sems,
    extra_recv_sems,
    back_send_sems,
    back_recv_sems,
    turn_send_sems,
    turn_recv_sems,
    info_send,
    info_recv,
    row_send,
    row_recv,
    sum_send,
    sum_recv,
    weight_send,
    weight_recv,
    *,
    count,
    heads,
    line,
    halves,
    slots,
    pieces,
    tile,
):
    seq_len, width = q_ref.shape
    cut = width // count
    place = lax.axis_index("sp")
    head = lax.axis_index("tp")
    here = place // 2
    side = lax.rem(place, 2)
    twin = place + 1 - 2 * side
    mate = head + 1 - 2 * lax.rem(head, 2)
    across = lax.rem(head + 2, heads)
    units = line * halves
    tokens = rows_ref.shape[1]
    grain = tokens // pieces
    last = line - 1
    shares = WEIGHT_PIECES
    chunks = 3 * shares

    def remote(src, dst, send, recv, peer, axis="sp"):
        return pltpu.make_async_remote_copy(
            src_ref=src,
            dst_ref=dst,
            send_sem=send,
            recv_sem=recv,
            device_id={axis: peer},
            device_id_type=pl.DeviceIdType.MESH,
        )

    loads = [
        pltpu.make_async_copy(src, dst, load_sems.at[i])
        for i, (src, dst) in enumerate(
            [
                (out_gate_hbm, out_gate_ref),
                (resid_hbm, resid_ref),
                (out_proj_hbm, out_proj_ref),
                (gate_hbm, gate_ref),
                (up_hbm, up_ref),
                (down_hbm, down_ref),
            ]
        )
    ]
    for load in loads:
        load.start()

    barrier = pltpu.get_barrier_semaphore()
    greeted = sp_tp_barrier(barrier, {"sp": count, "tp": heads})

    def weight_rows(chunk, owner):
        source = (gate_hbm, up_hbm, down_hbm)[chunk // shares]
        target = (twin_gate_ref, twin_up_ref, twin_down_ref)[chunk // shares]
        quarter = target.shape[0] // heads
        size = quarter // shares
        start = owner * quarter + (chunk % shares) * size
        rows = pl.ds(pl.multiple_of(start, size), size)
        return source.at[0, rows], target.at[rows]

    def weight_copy(stage, chunk):
        owner, peer, axis = (
            (head, twin, "sp"),
            (head, across, "tp"),
            (head, mate, "tp"),
            (across, mate, "tp"),
        )[stage]
        whole, landed = weight_rows(chunk, owner)
        return remote(
            whole if stage == 0 else landed,
            landed,
            weight_send.at[stage, chunk],
            weight_recv.at[stage, chunk],
            peer,
            axis,
        )

    def fetch(*span):
        for chunk in range(*span):
            weight_copy(0, chunk).start()

    def pass_on(*span):
        for chunk in range(*span):
            weight_copy(0, chunk).wait_recv()
            weight_copy(1, chunk).start()
            weight_copy(2, chunk).start()

    def hand_over(*span):
        for chunk in range(*span):
            weight_copy(1, chunk).wait_recv()
            weight_copy(3, chunk).start()

    def info_copy(step):
        peer = lax.rem(here + step, line)
        return remote(
            infos_ref.at[here],
            infos_ref.at[here],
            info_send.at[step - 1],
            info_recv.at[step - 1],
            peer * 2 + side,
        )

    eye_row, eye_col = col_mask(0, tokens, tokens)
    eye = jnp.where(eye_row == eye_col, 1.0, 0.0)
    for half in range(halves):
        span = slice(half * tokens, (half + 1) * tokens)
        ids = routes_ref[:, span].astype(jnp.float32)
        scores = scores_ref[:, span]
        zeros = jnp.zeros((8 - ids.shape[0], tokens), jnp.float32)
        columns = lax.dot_general(
            eye,
            jnp.concatenate([ids, zeros], axis=0),
            (((1,), (1,)), ((), ())),
            precision=HIGHEST,
            preferred_element_type=jnp.float32,
        )
        ranks = []
        for route in range(2):
            rank = jnp.zeros((1, tokens), jnp.float32)
            for other in range(2):
                same = (columns[:, other : other + 1] == ids[route : route + 1]) & (eye_row < eye_col)
                rank += jnp.sum(jnp.where(same, 1.0, 0.0), axis=0, keepdims=True)
            ranks.append(rank)
        infos_ref[here, half] = jnp.concatenate(
            [ids] + ranks + [scores / jnp.sum(scores, axis=0, keepdims=True), zeros[0:2]], axis=0
        )

    log_forget, cum_row, gap_row = log_rows(forget_ref, input_ref)
    pl.semaphore_wait(barrier, greeted)
    fetch(0, 2)
    total = jnp.sum(log_forget, axis=1, keepdims=True)
    best = jnp.max(gap_row, axis=1, keepdims=True)
    keep_row = jnp.exp(gap_row - best) * width ** (-0.5)
    weighted = k_ref[...].astype(jnp.float32).T * keep_row
    high, low = split_two(weighted)
    v_all = v_ref[...]
    state_ref[0:width, :] = jnp.dot(high, v_all, preferred_element_type=jnp.float32) + jnp.dot(
        low, v_all, preferred_element_type=jnp.float32
    )
    vector = jnp.dot(
        jnp.broadcast_to(keep_row, (8, seq_len)),
        k_ref[...].astype(jnp.float32),
        precision=HIGHEST,
        preferred_element_type=jnp.float32,
    )[0:1]
    lanes = jnp.zeros((1, width), jnp.float32)
    state_ref[width : width + EXTRA, :] = jnp.concatenate(
        [vector, lanes + total, lanes + total + best, jnp.zeros((EXTRA - 3, width), jnp.float32)],
        axis=0,
    )
    for step in range(1, line):
        info_copy(step).start()
    sends = []
    for step in range(1, count):
        peer = lax.rem(place + step, count)
        extra_copy = pltpu.make_async_remote_copy(
            src_ref=state_ref.at[pl.ds(width, EXTRA)],
            dst_ref=extra_ref.at[place],
            send_sem=extra_send_sems.at[step - 1],
            recv_sem=extra_recv_sems.at[step - 1],
            device_id={"sp": peer},
            device_id_type=pl.DeviceIdType.MESH,
        )
        piece_copy = pltpu.make_async_remote_copy(
            src_ref=state_ref.at[pl.ds(pl.multiple_of(peer * cut, cut), cut)],
            dst_ref=piece_ref.at[place],
            send_sem=send_sems.at[step - 1],
            recv_sem=recv_sems.at[step - 1],
            device_id={"sp": peer},
            device_id_type=pl.DeviceIdType.MESH,
        )
        extra_copy.start()
        piece_copy.start()
        sends += [extra_copy, piece_copy]
    extra_ref[place] = state_ref[width : width + EXTRA, :]
    piece_ref[place] = state_ref[pl.ds(pl.multiple_of(place * cut, cut), cut), :]

    fetch(2, 4)

    for first in range(0, seq_len, tile):
        span = first + tile
        row, col = col_mask(first, tile, span)
        causal = col <= row
        own = (col // BLOCK) == (row // BLOCK)
        gap = jnp.where(causal, gap_row[:, :span], -jnp.inf)
        top = jnp.max(gap, axis=1, keepdims=True)
        cum = jnp.sum(jnp.where(causal, log_forget[:, :span], 0.0), axis=1, keepdims=True)
        scores = lax.dot_general(
            q_ref[first:span, :],
            k_ref[0:span, :],
            (((1,), (1,)), ((), ())),
            preferred_element_type=jnp.float32,
        ) * width ** (-0.5)
        weights = scores * jnp.exp(gap - top)
        high = weights.astype(jnp.bfloat16)
        high_float = high.astype(jnp.float32)
        low_float = jnp.where(own, 0.0, weights - high_float)
        v = v_ref[0:span, :]
        num_ref[first:span, :] = jnp.dot(high, v, preferred_element_type=jnp.float32) + jnp.dot(
            low_float.astype(jnp.bfloat16), v, preferred_element_type=jnp.float32
        )
        den = jnp.sum(high_float + low_float, axis=1, keepdims=True)
        lane = lax.broadcasted_iota(jnp.int32, (tile, 128), 1)
        aux_ref[first:span, :] = jnp.where(lane == 0, den, jnp.where(lane == 1, top, cum))

    for copy in sends:
        copy.wait()

    pass_on(0, 2)
    running = jnp.zeros((cut, width), jnp.float32)
    vector = jnp.zeros((1, width), jnp.float32)
    far_max = jnp.full((1, width), FLOOR_LOG, jnp.float32)
    own_vector, own_max = vector, far_max
    for step in range(count):
        prefix_ref[step] = running
        own_vector = jnp.where(place == step, vector, own_vector)
        own_max = jnp.where(place == step, far_max, own_max)
        if step < count - 1:
            extra = extra_ref[step]
            new_max, step_total = extra[2:3], extra[1:2]
            joined = jnp.maximum(step_total + far_max, new_max)
            keep_old = jnp.exp(step_total + far_max - joined)
            keep_new = jnp.exp(new_max - joined)
            running = keep_old * running + keep_new * piece_ref[step]
            vector = keep_old * vector + keep_new * extra[0:1]
            far_max = joined
    backs = []
    for step in range(1, count):
        peer = lax.rem(place + step, count)
        back = pltpu.make_async_remote_copy(
            src_ref=prefix_ref.at[peer],
            dst_ref=mat_ref.at[pl.ds(pl.multiple_of(place * cut, cut), cut)],
            send_sem=back_send_sems.at[step - 1],
            recv_sem=back_recv_sems.at[step - 1],
            device_id={"sp": peer},
            device_id_type=pl.DeviceIdType.MESH,
        )
        back.start()
        backs.append(back)
    mat_ref[pl.ds(pl.multiple_of(place * cut, cut), cut), :] = prefix_ref[place]

    fetch(4, 8)
    aux = aux_ref[...]
    den, top, cum = aux[:, 0:1], aux[:, 1:2], aux[:, 2:3]
    far = own_max[:, 0:1]
    joined = jnp.maximum(top, far)
    keep_own = jnp.exp(top - joined)
    keep_far = jnp.exp(far - joined)
    q_float = q_ref[...].astype(jnp.float32)
    far_den = jnp.sum(q_float * own_vector, axis=1, keepdims=True)
    denominator = keep_own * den + keep_far * far_den
    divisor = jnp.maximum(jnp.abs(denominator), jnp.exp(-(cum + joined)))
    pass_on(2, 4)
    for copy in backs:
        copy.wait()
    one, rest = split_two(mat_ref[...])
    two, three = split_two(mat_ref[...] - one.astype(jnp.float32))
    q = q_ref[...]
    far_num = (
        jnp.dot(q, one, preferred_element_type=jnp.float32)
        + jnp.dot(q, two, preferred_element_type=jnp.float32)
        + jnp.dot(q, three, preferred_element_type=jnp.float32)
    )
    numerator = keep_own * num_ref[...] + keep_far * far_num
    cell_ref[...] = (numerator / divisor).astype(cell_ref.dtype)

    share = seq_len // heads
    columns = pl.ds(pl.multiple_of(head * width, width), width)
    turns = []
    for step in range(1, heads):
        peer = lax.rem(head + step, heads)
        turn = pltpu.make_async_remote_copy(
            src_ref=cell_ref.at[pl.ds(pl.multiple_of(peer * share, share), share)],
            dst_ref=token_ref.at[:, columns],
            send_sem=turn_send_sems.at[step - 1],
            recv_sem=turn_recv_sems.at[step - 1],
            device_id={"tp": peer},
            device_id_type=pl.DeviceIdType.MESH,
        )
        turn.start()
        turns.append(turn)
    own_copy = pltpu.make_async_copy(
        cell_ref.at[pl.ds(pl.multiple_of(head * share, share), share)],
        token_ref.at[:, columns],
        own_sem,
    )
    own_copy.start()
    fetch(8, chunks)
    for load in loads[:3]:
        load.wait()
    own_copy.wait()
    for copy in turns:
        copy.wait()

    def row_copy(src, source, half, way):
        unit = source * halves + half
        return remote(
            src,
            held_ref.at[unit],
            row_send.at[way, unit],
            row_recv.at[unit],
            place + (4 * way - 2),
        )

    def sum_copy(target, half, way, piece):
        landing = ((target + way) * halves + half) * pieces + piece
        leaving = (target * halves + half) * pieces + piece
        return remote(
            part_ref.at[leaving],
            sum_ref.at[landing],
            sum_send.at[leaving],
            sum_recv.at[landing],
            place + (4 * way - 2),
        )

    def sum_wait(landing):
        remote(
            part_ref.at[0], sum_ref.at[landing], sum_send.at[0], sum_recv.at[landing], twin
        ).wait_recv()

    for half in range(halves):
        span = slice(half * tokens, (half + 1) * tokens)
        cell_float = token_ref[span, :].astype(jnp.float32)
        headed = (
            cell_float
            * lax.rsqrt(jnp.mean(cell_float * cell_float, axis=1, keepdims=True) + EPS)
            * head_gain_ref[...]
        )
        gated = (headed * jax.nn.sigmoid(out_gate_ref[span, :].astype(jnp.float32))).astype(
            jnp.bfloat16
        )
        mixed = resid_ref[span, :].astype(jnp.float32) + jnp.dot(
            gated, out_proj_ref[...], preferred_element_type=jnp.float32
        )
        own_ref[half] = mixed
        normed = (
            mixed
            * lax.rsqrt(jnp.mean(mixed * mixed, axis=1, keepdims=True) + EPS)
            * ffn_gain_ref[...]
        ).astype(jnp.bfloat16)
        rows_ref[half] = normed
        held_ref[here * halves + half] = normed
        if half == 0:
            for way in range(2):

                @pl.when((here < last) if way else (here > 0))
                def _():
                    row_copy(rows_ref.at[0], here, 0, way).start()

    def later_halves(way):
        for half in range(1, halves):
            row_copy(rows_ref.at[half], here, half, way).start()

    @pl.when(here == 0)
    def _():
        later_halves(1)

    @pl.when(here == last)
    def _():
        later_halves(0)

    for step in range(1, line):
        info_copy(step).wait()
    for load in loads[3:]:
        load.wait()

    shorter = jnp.minimum(here, last - here)

    def in_stream(p, reach):
        first = p < reach
        turn = p - reach
        ahead = jnp.where(first, p + 1, reach - turn // (halves - 1))
        return ahead, jnp.where(first, 0, 1 + lax.rem(turn, halves - 1))

    def source_of(k):
        p = k - halves
        both = shorter * 2 * halves
        paired = p < both
        way = jnp.where(paired, lax.rem(p, 2), jnp.where(here < last - here, 1, 0))
        spot = jnp.where(paired, p // 2, p - shorter * halves)
        reach = jnp.where(way == 1, last - here, here)
        ahead, half = in_stream(spot, reach)
        is_own = k < halves
        final = spot == reach * halves - 1
        return (
            jnp.where(is_own, here, here + ahead * (2 * way - 1)),
            jnp.where(is_own, k, half),
            final,
        )

    def matches(source, half, weighted):
        info = infos_ref[source, half]
        rank = lax.broadcasted_iota(jnp.int32, (slots, tokens), 0).astype(jnp.float32)
        tables = []
        for expert in (place, twin):
            name = expert.astype(jnp.float32)
            table = jnp.zeros((slots, tokens), jnp.float32)
            for route in range(2):
                hit = jnp.where(info[route : route + 1] == name, info[2 + route : 3 + route], -1.0)
                value = info[4 + route : 5 + route] if weighted else 1.0
                table += jnp.where(hit == rank, value, 0.0)
            tables.append(table)
        return jnp.concatenate(tables, axis=0)

    first_way = jnp.where(last - here <= here, 0, 1)

    def relay(way, spot):
        reach = jnp.where(way == 1, last - here, here)

        @pl.when((spot >= 0) & (spot < reach * halves) & (here > 0) & (here < last))
        def _():
            ahead, half = in_stream(spot, reach)
            target = here + ahead * (2 * way - 1)
            for piece in range(pieces):
                unit = (target * halves + half) * pieces + piece
                landing = ((target + way) * halves + half) * pieces + piece
                sum_wait(landing)
                part_ref[unit] = (
                    part_ref[unit].astype(jnp.float32) + sum_ref[landing].astype(jnp.float32)
                ).astype(jnp.bfloat16)
                sum_copy(target, half, way, piece).start()

    def expert(rows, gate_mat, up_mat, down_mat):
        gate = jnp.dot(rows, gate_mat[...], preferred_element_type=jnp.float32)
        up = jnp.dot(rows, up_mat[...], preferred_element_type=jnp.float32)
        active = (jax.nn.silu(gate) * up).astype(jnp.bfloat16)
        return jnp.dot(active, down_mat[...], preferred_element_type=jnp.float32).astype(
            jnp.bfloat16
        )

    def combine(k, carry):
        source, half, _ = source_of(jnp.where(k < units, k, k - units))
        unit = source * halves + half
        done_ref[unit, slots : 2 * slots, :] = expert(
            cross_ref[unit], twin_gate_ref, twin_up_ref, twin_down_ref
        )
        high, low = split_two(matches(source, half, True))
        answers = done_ref[unit]
        turned = (((0,), (0,)), ((), ()))
        part = lax.dot_general(
            high, answers, turned, preferred_element_type=jnp.float32
        ) + lax.dot_general(low, answers, turned, preferred_element_type=jnp.float32)

        @pl.when(source == here)
        def _():
            own_ref[half] = own_ref[half] + part

        @pl.when(source != here)
        def _():
            for piece in range(pieces):
                part_ref[unit * pieces + piece] = part[
                    piece * grain : (piece + 1) * grain
                ].astype(jnp.bfloat16)

        @pl.when((source < here) & (here == last))
        def _():
            for piece in range(pieces):
                sum_copy(source, half, 0, piece).start()

        @pl.when((source > here) & (here == 0))
        def _():
            for piece in range(pieces):
                sum_copy(source, half, 1, piece).start()

        return carry

    ready = min(3, units - 1)

    def step_body(k, carry):
        @pl.when(k < units)
        def _():
            source, half, final = source_of(k)
            unit = source * halves + half

            @pl.when(source != here)
            def _():
                remote(
                    held_ref.at[unit], held_ref.at[unit], row_send.at[0, unit], row_recv.at[unit], twin
                ).wait_recv()

            @pl.when((source < here) & (here < last))
            def _():
                row_copy(held_ref.at[unit], source, half, 1).start()

                @pl.when(final)
                def _():
                    later_halves(1)

            @pl.when((source > here) & (here > 0))
            def _():
                row_copy(held_ref.at[unit], source, half, 0).start()

                @pl.when(final)
                def _():
                    later_halves(0)

            packed = jnp.dot(
                matches(source, half, False).astype(jnp.bfloat16),
                held_ref[unit],
                preferred_element_type=jnp.float32,
            ).astype(jnp.bfloat16)
            cross_ref[unit] = packed[slots:]
            done_ref[unit, 0:slots, :] = expert(
                packed[:slots], gate_ref.at[0], up_ref.at[0], down_ref.at[0]
            )

        @pl.when(k == 0)
        def _():
            pass_on(4, 8)
            hand_over(0, 2)

        @pl.when(k == 1)
        def _():
            pass_on(8, chunks)
            hand_over(2, 6)

        @pl.when(k == 2)
        def _():
            hand_over(6, 9)

        @pl.when(k == ready)
        def _():
            hand_over(9, chunks)
            for chunk in range(chunks):
                weight_copy(2, chunk).wait_recv()
                weight_copy(3, chunk).wait_recv()

        relay(first_way, k - units)
        relay(1 - first_way, k - units - 2)
        low = jnp.where(k == ready, halves, k)
        lax.fori_loop(low, jnp.where(k >= ready, k + 1, low), combine, 0)
        return carry

    lax.fori_loop(0, units + halves, step_body, 0)
    for spot in range(halves, last * halves):
        relay(first_way, spot)
        relay(1 - first_way, spot - 2)

    for half in range(halves):
        for piece in range(pieces):
            rows = pl.ds(piece * grain, grain)
            for way in range(2):

                @pl.when((here > 0) if way else (here < last))
                def _():
                    landing = ((here + way) * halves + half) * pieces + piece
                    sum_wait(landing)
                    own_ref[half, rows] = own_ref[half, rows] + sum_ref[landing].astype(jnp.float32)

            out_ref[half, rows] = own_ref[half, rows].astype(out_ref.dtype)

    def drain(unit, carry):
        source = unit // halves
        half = lax.rem(unit, halves)

        @pl.when((source <= here) & (here < last))
        def _():
            row_copy(held_ref.at[unit], source, half, 1).wait_send()

        @pl.when((source >= here) & (here > 0))
        def _():
            row_copy(held_ref.at[unit], source, half, 0).wait_send()

        @pl.when(source != here)
        def _():
            for piece in range(pieces):
                sum_copy(source, half, 0, piece).wait_send()

        return carry

    lax.fori_loop(0, units, drain, 0)
    for chunk in range(chunks):
        for stage in range(4):
            weight_copy(stage, chunk).wait_send()


def run_layer(
    resid,
    query,
    keys,
    values,
    out_gate,
    forget_pre,
    input_pre,
    head_gain,
    out_proj,
    ffn_gain,
    routes,
    route_scores,
    w_gate,
    w_up,
    w_down,
    halves,
    slots,
):
    count, heads = lax.axis_size("sp"), lax.axis_size("tp")
    line = count // 2
    units = line * halves
    seq_len, width = query.shape
    cut = width // count
    share = seq_len // heads
    wide = resid.shape[1]
    tokens = share // halves
    pieces = 2
    grain = tokens // pieces
    tile = 4 * BLOCK if seq_len % (4 * BLOCK) == 0 else BLOCK
    vmem = pl.BlockSpec(memory_space=pltpu.VMEM)
    whole = pl.BlockSpec(memory_space=pl.ANY)
    dma = pltpu.SemaphoreType.DMA
    f32, bf16 = jnp.float32, jnp.bfloat16
    chunks = 3 * WEIGHT_PIECES
    out = pl.pallas_call(
        functools.partial(
            layer_kernel,
            count=count,
            heads=heads,
            line=line,
            halves=halves,
            slots=slots,
            pieces=pieces,
            tile=tile,
        ),
        out_shape=jax.ShapeDtypeStruct((halves, tokens, wide), bf16),
        in_specs=[vmem] * 9 + [whole] * 6,
        out_specs=vmem,
        scratch_shapes=[
            pltpu.VMEM((width + EXTRA, width), f32),
            pltpu.VMEM((count, cut, width), f32),
            pltpu.VMEM((count, EXTRA, width), f32),
            pltpu.VMEM((count, cut, width), f32),
            pltpu.VMEM((width, width), f32),
            pltpu.VMEM((seq_len, width), f32),
            pltpu.VMEM((seq_len, 128), f32),
            pltpu.VMEM((seq_len, width), bf16),
            pltpu.VMEM((share, heads * width), bf16),
            pltpu.VMEM(resid.shape, bf16),
            pltpu.VMEM(out_gate.shape, bf16),
            pltpu.VMEM(out_proj.shape, bf16),
            pltpu.VMEM(w_gate.shape, bf16),
            pltpu.VMEM(w_up.shape, bf16),
            pltpu.VMEM(w_down.shape, bf16),
            pltpu.VMEM(w_gate.shape[1:], bf16),
            pltpu.VMEM(w_up.shape[1:], bf16),
            pltpu.VMEM(w_down.shape[1:], bf16),
            pltpu.VMEM((line, halves, 8, tokens), f32),
            pltpu.VMEM((halves, tokens, wide), bf16),
            pltpu.VMEM((units, tokens, wide), bf16),
            pltpu.VMEM((units, slots, wide), bf16),
            pltpu.VMEM((units, 2 * slots, wide), bf16),
            pltpu.VMEM((units * pieces, grain, wide), bf16),
            pltpu.VMEM((halves, tokens, wide), f32),
            pltpu.VMEM(((units + halves) * pieces, grain, wide), bf16),
            dma((6,)),
            dma(()),
            dma((count - 1,)),
            dma((count - 1,)),
            dma((count - 1,)),
            dma((count - 1,)),
            dma((count - 1,)),
            dma((count - 1,)),
            dma((heads - 1,)),
            dma((heads - 1,)),
            dma((line - 1,)),
            dma((line - 1,)),
            dma((2, units)),
            dma((units,)),
            dma((units * pieces,)),
            dma(((units + halves) * pieces,)),
            dma((4, chunks)),
            dma((4, chunks)),
        ],
        compiler_params=pltpu.CompilerParams(
            vmem_limit_bytes=LAYER_VMEM, collective_id=5, has_side_effects=True
        ),
        cost_estimate=pl.CostEstimate(flops=10**10, bytes_accessed=2**24, transcendentals=0),
        name="layer",
    )(
        query,
        keys,
        values,
        forget_pre,
        input_pre,
        head_gain[None, :],
        ffn_gain[None, :],
        routes.T,
        route_scores.T,
        resid,
        out_gate,
        out_proj,
        w_gate,
        w_up,
        w_down,
    )
    return out.reshape(share, wide)


def slot_select(expert_ids, expert_count, capacity):
    flat_ids = expert_ids.reshape(-1)
    one_hot = (flat_ids[:, None] == jnp.arange(expert_count, dtype=jnp.int32)[None, :]).astype(
        jnp.int32
    )
    slot_rank = jnp.sum((jnp.cumsum(one_hot, axis=0) - 1) * one_hot, axis=1)
    target = flat_ids * capacity + slot_rank
    return (
        jnp.arange(expert_count * capacity, dtype=jnp.int32)[:, None] == target[None, :]
    ).astype(jnp.bfloat16)


def exchange_kernel(send_ref, recv_ref, send_sems, recv_sems, own_sem, *, axis, count):
    place = lax.axis_index(axis)
    barrier = pltpu.get_barrier_semaphore()
    for step in range(1, count):
        peer = lax.rem(place + step, count)
        pl.semaphore_signal(
            barrier, inc=1, device_id={axis: peer}, device_id_type=pl.DeviceIdType.MESH
        )
    own = pltpu.make_async_copy(send_ref.at[place], recv_ref.at[place], own_sem)
    own.start()
    pl.semaphore_wait(barrier, count - 1)
    copies = []
    for step in range(1, count):
        peer = lax.rem(place + step, count)
        copy = pltpu.make_async_remote_copy(
            src_ref=send_ref.at[peer],
            dst_ref=recv_ref.at[place],
            send_sem=send_sems.at[step - 1],
            recv_sem=recv_sems.at[step - 1],
            device_id={axis: peer},
            device_id_type=pl.DeviceIdType.MESH,
        )
        copy.start()
        copies.append(copy)
    own.wait()
    for copy in copies:
        copy.wait()


def exchange(blocks, axis, collective_id):
    count = lax.axis_size(axis)
    grouped = blocks.reshape((count, -1) + blocks.shape[2:])
    out = pl.pallas_call(
        functools.partial(exchange_kernel, axis=axis, count=count),
        out_shape=jax.ShapeDtypeStruct(grouped.shape, grouped.dtype),
        in_specs=[pl.BlockSpec(memory_space=pl.ANY)],
        out_specs=pl.BlockSpec(memory_space=pl.ANY),
        scratch_shapes=[
            pltpu.SemaphoreType.DMA((count - 1,)),
            pltpu.SemaphoreType.DMA((count - 1,)),
            pltpu.SemaphoreType.DMA(()),
        ],
        compiler_params=pltpu.CompilerParams(collective_id=collective_id, has_side_effects=True),
        name="exchange",
    )(grouped)
    return out.reshape(blocks.shape)


def run_experts(arrived, w_gate, w_up, w_down, sources):
    local_count = w_gate.shape[0]
    grouped = arrived.reshape(sources, local_count, arrived.shape[1], arrived.shape[2])
    gate_pre = jnp.einsum("pesd,edf->pesf", grouped, w_gate, preferred_element_type=jnp.float32)
    up_pre = jnp.einsum("pesd,edf->pesf", grouped, w_up, preferred_element_type=jnp.float32)
    active = (jax.nn.silu(gate_pre) * up_pre).astype(jnp.bfloat16)
    result = jnp.einsum(
        "pesf,efd->pesd", active, w_down, preferred_element_type=jnp.float32
    ).astype(jnp.bfloat16)
    return result.reshape(arrived.shape)


def line_kernel(
    rows_ref,
    mix_ref,
    info_ref,
    gate_hbm,
    up_hbm,
    down_hbm,
    out_ref,
    gate_ref,
    up_ref,
    down_ref,
    infos_ref,
    held_ref,
    cross_ref,
    crossed_ref,
    answer_ref,
    done_ref,
    batch_ref,
    part_ref,
    own_ref,
    sum_ref,
    load_sems,
    info_send,
    info_recv,
    row_send,
    row_recv,
    cross_send,
    cross_recv,
    answer_send,
    answer_recv,
    sum_send,
    sum_recv,
    *,
    line,
    halves,
    slots,
    pieces,
):
    place = lax.axis_index("sp")
    here = place // 2
    side = lax.rem(place, 2)
    twin = place + 1 - 2 * side
    units = line * halves
    tokens = rows_ref.shape[1]
    grain = tokens // pieces
    last = line - 1

    def remote(src, dst, send, recv, peer):
        return pltpu.make_async_remote_copy(
            src_ref=src,
            dst_ref=dst,
            send_sem=send,
            recv_sem=recv,
            device_id={"sp": peer},
            device_id_type=pl.DeviceIdType.MESH,
        )

    loads = [
        pltpu.make_async_copy(src, dst, load_sems.at[i])
        for i, (src, dst) in enumerate(
            [(gate_hbm, gate_ref), (up_hbm, up_ref), (down_hbm, down_ref)]
        )
    ]
    for load in loads:
        load.start()

    barrier = pltpu.get_barrier_semaphore()
    for step in range(1, line):
        pl.semaphore_signal(
            barrier,
            inc=1,
            device_id={"sp": lax.rem(here + step, line) * 2 + side},
            device_id_type=pl.DeviceIdType.MESH,
        )
    pl.semaphore_signal(
        barrier, inc=1, device_id={"sp": twin}, device_id_type=pl.DeviceIdType.MESH
    )
    pl.semaphore_wait(barrier, line)

    def info_copy(step):
        peer = lax.rem(here + step, line)
        return remote(
            info_ref,
            infos_ref.at[here],
            info_send.at[step - 1],
            info_recv.at[step - 1],
            peer * 2 + side,
        )

    def row_copy(src, source, half, way):
        unit = source * halves + half
        return remote(
            src,
            held_ref.at[unit],
            row_send.at[way, unit],
            row_recv.at[unit],
            place + (4 * way - 2),
        )

    def cross_copy(unit):
        return remote(
            cross_ref.at[unit],
            crossed_ref.at[unit],
            cross_send.at[unit],
            cross_recv.at[unit],
            twin,
        )

    def answer_copy(unit):
        return remote(
            answer_ref.at[unit],
            done_ref.at[unit, pl.ds(slots, slots)],
            answer_send.at[unit],
            answer_recv.at[unit],
            twin,
        )

    def sum_copy(target, half, way, piece):
        landing = ((target + way) * halves + half) * pieces + piece
        leaving = (target * halves + half) * pieces + piece
        return remote(
            part_ref.at[leaving],
            sum_ref.at[landing],
            sum_send.at[leaving],
            sum_recv.at[landing],
            place + (4 * way - 2),
        )

    def sum_wait(landing):
        remote(
            part_ref.at[0], sum_ref.at[landing], sum_send.at[0], sum_recv.at[landing], twin
        ).wait_recv()

    for step in range(1, line):
        info_copy(step).start()
    for way in range(2):

        @pl.when((here < last) if way else (here > 0))
        def _():
            row_copy(rows_ref.at[0], here, 0, way).start()

    def later_halves(way):
        for half in range(1, halves):
            row_copy(rows_ref.at[half], here, half, way).start()

    @pl.when(here == 0)
    def _():
        later_halves(1)

    @pl.when(here == last)
    def _():
        later_halves(0)

    infos_ref[here] = info_ref[...]
    for half in range(halves):
        held_ref[here * halves + half] = rows_ref[half]
    batch_ref[...] = jnp.zeros_like(batch_ref)
    for step in range(1, line):
        info_copy(step).wait()

    shorter = jnp.minimum(here, last - here)

    def in_stream(p, reach):
        first = p < reach
        turn = p - reach
        ahead = jnp.where(first, p + 1, reach - turn // (halves - 1))
        return ahead, jnp.where(first, 0, 1 + lax.rem(turn, halves - 1))

    def source_of(k):
        p = k - halves
        both = shorter * 2 * halves
        paired = p < both
        way = jnp.where(paired, lax.rem(p, 2), jnp.where(here < last - here, 1, 0))
        spot = jnp.where(paired, p // 2, p - shorter * halves)
        reach = jnp.where(way == 1, last - here, here)
        ahead, half = in_stream(spot, reach)
        is_own = k < halves
        final = spot == reach * halves - 1
        return (
            jnp.where(is_own, here, here + ahead * (2 * way - 1)),
            jnp.where(is_own, k, half),
            final,
        )

    def matches(source, half, weighted):
        info = infos_ref[source, half]
        rank = lax.broadcasted_iota(jnp.int32, (slots, tokens), 0).astype(jnp.float32)
        tables = []
        for expert in (place, twin):
            name = expert.astype(jnp.float32)
            table = jnp.zeros((slots, tokens), jnp.float32)
            for route in range(2):
                hit = jnp.where(info[route : route + 1] == name, info[2 + route : 3 + route], -1.0)
                value = info[4 + route : 5 + route] if weighted else 1.0
                table += jnp.where(hit == rank, value, 0.0)
            tables.append(table)
        return jnp.concatenate(tables, axis=0)

    first_way = jnp.where(last - here <= here, 0, 1)

    def relay(way, spot):
        reach = jnp.where(way == 1, last - here, here)

        @pl.when((spot >= 0) & (spot < reach * halves) & (here > 0) & (here < last))
        def _():
            ahead, half = in_stream(spot, reach)
            target = here + ahead * (2 * way - 1)
            for piece in range(pieces):
                unit = (target * halves + half) * pieces + piece
                landing = ((target + way) * halves + half) * pieces + piece
                sum_wait(landing)
                part_ref[unit] = (
                    part_ref[unit].astype(jnp.float32) + sum_ref[landing].astype(jnp.float32)
                ).astype(jnp.bfloat16)
                sum_copy(target, half, way, piece).start()

    def step_body(k, carry):
        @pl.when(k < units)
        def _():
            source, half, final = source_of(k)
            unit = source * halves + half

            @pl.when(source != here)
            def _():
                remote(
                    held_ref.at[unit], held_ref.at[unit], row_send.at[0, unit], row_recv.at[unit], twin
                ).wait_recv()

            @pl.when((source < here) & (here < last))
            def _():
                row_copy(held_ref.at[unit], source, half, 1).start()

                @pl.when(final)
                def _():
                    later_halves(1)

            @pl.when((source > here) & (here > 0))
            def _():
                row_copy(held_ref.at[unit], source, half, 0).start()

                @pl.when(final)
                def _():
                    later_halves(0)

            packed = jnp.dot(
                matches(source, half, False).astype(jnp.bfloat16),
                held_ref[unit],
                preferred_element_type=jnp.float32,
            ).astype(jnp.bfloat16)
            cross_ref[unit] = packed[slots:]
            cross_copy(unit).start()
            batch_ref[0:slots, :] = packed[:slots]

        @pl.when(k == 0)
        def _():
            for load in loads:
                load.wait()

        relay(first_way, k - units)

        @pl.when((k > 0) & (k <= units))
        def _():
            source, half, _ = source_of(k - 1)
            unit = source * halves + half
            cross_copy(unit).wait_recv()
            batch_ref[slots : 2 * slots, :] = crossed_ref[unit]

        @pl.when(k <= units)
        def _():
            rows = batch_ref[...]
            gate = jnp.dot(rows, gate_ref[0], preferred_element_type=jnp.float32)
            up = jnp.dot(rows, up_ref[0], preferred_element_type=jnp.float32)
            active = (jax.nn.silu(gate) * up).astype(jnp.bfloat16)
            batch_ref[...] = jnp.dot(
                active, down_ref[0], preferred_element_type=jnp.float32
            ).astype(jnp.bfloat16)

        @pl.when(k < units)
        def _():
            source, half, _ = source_of(k)
            done_ref[source * halves + half, 0:slots, :] = batch_ref[0:slots, :]

        @pl.when((k > 0) & (k <= units))
        def _():
            source, half, _ = source_of(k - 1)
            unit = source * halves + half
            answer_ref[unit] = batch_ref[slots : 2 * slots, :]

            @pl.when(source != here)
            def _():
                answer_copy(unit).start()

        @pl.when(k == units)
        def _():
            for half in range(halves):
                answer_copy(here * halves + half).start()

        relay(1 - first_way, k - units - 2)

        @pl.when(k > 1 + halves)
        def _():
            source, half, _ = source_of(jnp.where(k > units + 1, k - units - 2, k - 2))
            unit = source * halves + half
            answer_copy(unit).wait_recv()
            high, low = split_two(matches(source, half, True))
            answers = done_ref[unit]
            turned = (((0,), (0,)), ((), ()))
            part = lax.dot_general(
                high, answers, turned, preferred_element_type=jnp.float32
            ) + lax.dot_general(low, answers, turned, preferred_element_type=jnp.float32)

            @pl.when(source == here)
            def _():
                own_ref[half] = part

            @pl.when(source != here)
            def _():
                for piece in range(pieces):
                    part_ref[unit * pieces + piece] = part[
                        piece * grain : (piece + 1) * grain
                    ].astype(jnp.bfloat16)

            @pl.when((source < here) & (here == last))
            def _():
                for piece in range(pieces):
                    sum_copy(source, half, 0, piece).start()

            @pl.when((source > here) & (here == 0))
            def _():
                for piece in range(pieces):
                    sum_copy(source, half, 1, piece).start()

        return carry

    lax.fori_loop(0, units + 2 + halves, step_body, 0)

    for half in range(halves):
        for piece in range(pieces):
            rows = pl.ds(piece * grain, grain)
            own_ref[half, rows] = own_ref[half, rows] + mix_ref[half, rows]
            for way in range(2):

                @pl.when((here > 0) if way else (here < last))
                def _():
                    landing = ((here + way) * halves + half) * pieces + piece
                    sum_wait(landing)
                    own_ref[half, rows] = own_ref[half, rows] + sum_ref[landing].astype(jnp.float32)

            out_ref[half, rows] = own_ref[half, rows].astype(out_ref.dtype)

    def drain(unit, carry):
        source = unit // halves
        half = lax.rem(unit, halves)
        cross_copy(unit).wait_send()
        answer_copy(unit).wait_send()

        @pl.when((source <= here) & (here < last))
        def _():
            row_copy(held_ref.at[unit], source, half, 1).wait_send()

        @pl.when((source >= here) & (here > 0))
        def _():
            row_copy(held_ref.at[unit], source, half, 0).wait_send()

        @pl.when(source != here)
        def _():
            for piece in range(pieces):
                sum_copy(source, half, 0, piece).wait_send()

        return carry

    lax.fori_loop(0, units, drain, 0)


def run_line(normed_rows, after_mix, info, w_gate, w_up, w_down, slots):
    count = lax.axis_size("sp")
    line, halves = count // 2, info.shape[0]
    units = line * halves
    row_count, width = normed_rows.shape
    tokens = row_count // halves
    pieces = 2
    grain = tokens // pieces
    vmem = pl.BlockSpec(memory_space=pltpu.VMEM)
    whole = pl.BlockSpec(memory_space=pl.ANY)
    dma = pltpu.SemaphoreType.DMA
    out = pl.pallas_call(
        functools.partial(line_kernel, line=line, halves=halves, slots=slots, pieces=pieces),
        out_shape=jax.ShapeDtypeStruct((halves, tokens, width), jnp.bfloat16),
        in_specs=[vmem, vmem, vmem, whole, whole, whole],
        out_specs=vmem,
        scratch_shapes=[
            pltpu.VMEM(w_gate.shape, jnp.bfloat16),
            pltpu.VMEM(w_up.shape, jnp.bfloat16),
            pltpu.VMEM(w_down.shape, jnp.bfloat16),
            pltpu.VMEM((line,) + info.shape, jnp.float32),
            pltpu.VMEM((units, tokens, width), jnp.bfloat16),
            pltpu.VMEM((units, slots, width), jnp.bfloat16),
            pltpu.VMEM((units, slots, width), jnp.bfloat16),
            pltpu.VMEM((units, slots, width), jnp.bfloat16),
            pltpu.VMEM((units, 2 * slots, width), jnp.bfloat16),
            pltpu.VMEM((2 * slots, width), jnp.bfloat16),
            pltpu.VMEM((units * pieces, grain, width), jnp.bfloat16),
            pltpu.VMEM((halves, tokens, width), jnp.float32),
            pltpu.VMEM(((units + halves) * pieces, grain, width), jnp.bfloat16),
            dma((3,)),
            dma((line - 1,)),
            dma((line - 1,)),
            dma((2, units)),
            dma((units,)),
            dma((units,)),
            dma((units,)),
            dma((units,)),
            dma((units,)),
            dma((units * pieces,)),
            dma(((units + halves) * pieces,)),
        ],
        compiler_params=pltpu.CompilerParams(
            vmem_limit_bytes=VMEM_LIMIT, collective_id=4, has_side_effects=True
        ),
        cost_estimate=pl.CostEstimate(flops=10**10, bytes_accessed=2**23, transcendentals=0),
        name="experts",
    )(
        normed_rows.reshape(halves, tokens, width),
        after_mix.reshape(halves, tokens, width),
        info,
        w_gate,
        w_up,
        w_down,
    )
    return out.reshape(row_count, width)


def route_info(routes, route_weight, halves):
    tokens = routes.shape[0] // halves
    ids = routes.reshape(halves, -1)
    order = jnp.arange(ids.shape[1], dtype=jnp.int32)
    same = (ids[:, :, None] == ids[:, None, :]) & (order[None, None, :] < order[None, :, None])
    rank = jnp.sum(same.astype(jnp.float32), axis=2)

    def turned(a):
        return a.astype(jnp.float32).reshape(halves, tokens, -1).transpose(0, 2, 1)

    return jnp.concatenate(
        [turned(routes), turned(rank), turned(route_weight), jnp.zeros((halves, 2, tokens), jnp.float32)],
        axis=1,
    )


def shards(
    resid,
    query,
    keys,
    values,
    out_gate,
    forget_pre,
    input_pre,
    head_gain,
    out_proj,
    ffn_gain,
    routes,
    route_scores,
    w_gate,
    w_up,
    w_down,
):
    head_width = query.shape[1]
    row_count, route_count = routes.shape
    sources = lax.axis_size("sp")
    local_experts = w_gate.shape[0]
    expert_count = local_experts * sources
    half_rows = row_count // 2
    capacity = max(2, 2 * half_rows * route_count // expert_count)
    dense = local_experts == 1 and sources % 2 == 0 and sources <= 8 and route_count == 2
    dense = dense and 2 * capacity >= half_rows and capacity % 16 == 0 and half_rows % 32 == 0
    if dense and lax.axis_size("tp") == 4 and head_width % (8 * sources) == 0:
        return run_layer(
            resid,
            query,
            keys,
            values,
            out_gate,
            forget_pre,
            input_pre,
            head_gain,
            out_proj,
            ffn_gain,
            routes,
            route_scores,
            w_gate,
            w_up,
            w_down,
            2,
            capacity,
        )
    route_weight = route_scores / jnp.sum(route_scores, axis=1, keepdims=True)
    token_rows = token_cell(query, keys, values, forget_pre, input_pre)
    cell_float = token_rows.astype(jnp.float32)
    headed = (
        cell_float
        * lax.rsqrt(jnp.mean(cell_float * cell_float, axis=1, keepdims=True) + EPS)
        * head_gain[None, :]
    )
    gated_out = (headed * jax.nn.sigmoid(out_gate.astype(jnp.float32))).astype(jnp.bfloat16)
    after_mix = resid.astype(jnp.float32) + jnp.dot(
        gated_out, out_proj, preferred_element_type=jnp.float32
    )
    normed_rows = (
        after_mix
        * lax.rsqrt(jnp.mean(after_mix * after_mix, axis=1, keepdims=True) + EPS)
        * ffn_gain[None, :]
    ).astype(jnp.bfloat16)
    if dense:
        info = route_info(routes, route_weight, 2)
        return run_line(normed_rows, after_mix, info, w_gate, w_up, w_down, capacity)
    selects = [
        slot_select(
            routes[half_idx * half_rows : (half_idx + 1) * half_rows], expert_count, capacity
        )
        for half_idx in range(2)
    ]

    def pack_rows(half_idx):
        selection = (
            selects[half_idx].reshape(expert_count * capacity, half_rows, route_count).sum(axis=2)
        )
        packed = jnp.dot(
            selection,
            normed_rows[half_idx * half_rows : (half_idx + 1) * half_rows],
            preferred_element_type=jnp.float32,
        )
        return packed.astype(jnp.bfloat16).reshape(expert_count, capacity, normed_rows.shape[1])

    send_rows = jnp.concatenate([pack_rows(0), pack_rows(1)], axis=1)
    finished = run_experts(
        exchange(send_rows, "sp", 1),
        w_gate,
        w_up,
        w_down,
        sources,
    )
    returned = exchange(finished, "sp", 2)
    answers = [returned[:, :capacity], returned[:, capacity:]]
    pieces = []
    for half_idx in range(2):
        gathered = lax.dot_general(
            selects[half_idx],
            answers[half_idx].reshape(expert_count * capacity, -1),
            (((0,), (0,)), ((), ())),
            preferred_element_type=jnp.float32,
        )
        weights_half = route_weight[half_idx * half_rows : (half_idx + 1) * half_rows]
        pieces.append(
            jnp.sum(gathered.reshape(half_rows, route_count, -1) * weights_half[:, :, None], axis=1)
        )
    return (after_mix + jnp.concatenate(pieces, axis=0)).astype(jnp.bfloat16)


def solution(mesh):
    placed = (
        P(("sp", "tp"), None),
        P("sp", "tp"),
        P("sp", "tp"),
        P("sp", "tp"),
        P(("sp", "tp"), None),
        P("tp", "sp"),
        P("tp", "sp"),
        P(),
        P(),
        P(),
        P(("sp", "tp"), None),
        P(("sp", "tp"), None),
        P("sp", None, None),
        P("sp", None, None),
        P("sp", None, None),
    )
    return jax.shard_map(
        shards, mesh=mesh, in_specs=placed, out_specs=P(("sp", "tp"), None), check_vma=False
    )
```

```python
import functools

import jax
import jax.numpy as jnp
from jax import lax
from jax.experimental import pallas as pl
from jax.experimental.pallas import tpu as pltpu
from jax.sharding import PartitionSpec as P

BLOCK = 64


EPS = 1e-06
FLOOR_LOG = -1e30
HIGHEST = lax.Precision.HIGHEST


EXTRA = 8
VMEM_LIMIT = 56 * 1024 * 1024
LAYER_VMEM = 60 * 1024 * 1024
WEIGHT_PIECES = 4


def col_mask(first_row, rows, cols):
    row = lax.broadcasted_iota(jnp.int32, (rows, cols), 0) + first_row
    col = lax.broadcasted_iota(jnp.int32, (rows, cols), 1)
    return row, col


def split_two(a):
    high = a.astype(jnp.bfloat16)
    return high, (a - high.astype(jnp.float32)).astype(jnp.bfloat16)


def log_rows(forget_ref, input_ref):
    pre = forget_ref[...]
    log_forget = jnp.minimum(pre, 0.0) - jnp.log1p(jnp.exp(-jnp.abs(pre)))
    seq_len = pre.shape[1]
    row, col = col_mask(0, seq_len, seq_len)
    upper = jnp.where(row <= col, 1.0, 0.0).astype(jnp.bfloat16)
    one, rest = split_two(log_forget)
    two, three = split_two(log_forget - one.astype(jnp.float32))
    stacked = jnp.concatenate([one, two, three, jnp.zeros((13, seq_len), jnp.bfloat16)], axis=0)
    sums = jnp.dot(stacked, upper, preferred_element_type=jnp.float32)
    cum_row = sums[0:1] + sums[1:2] + sums[2:3]
    return log_forget, cum_row, input_ref[...] - cum_row


def cell_state_kernel(k_ref, v_ref, forget_ref, input_ref, state_ref):
    width = k_ref.shape[1]
    seq_len = k_ref.shape[0]
    log_forget, cum_row, gap_row = log_rows(forget_ref, input_ref)
    total = jnp.sum(log_forget, axis=1, keepdims=True)
    top = jnp.max(gap_row, axis=1, keepdims=True)
    keep_row = jnp.exp(gap_row - top) * width ** (-0.5)
    k_turned = k_ref[...].astype(jnp.float32).T
    weighted = k_turned * keep_row
    high, low = split_two(weighted)
    v = v_ref[...]
    state_ref[0:width, :] = jnp.dot(high, v, preferred_element_type=jnp.float32) + jnp.dot(
        low, v, preferred_element_type=jnp.float32
    )
    vector = jnp.dot(
        jnp.broadcast_to(keep_row, (8, seq_len)),
        k_ref[...].astype(jnp.float32),
        precision=HIGHEST,
        preferred_element_type=jnp.float32,
    )[0:1]
    lanes = jnp.zeros((1, width), jnp.float32)
    state_ref[width : width + EXTRA, :] = jnp.concatenate(
        [vector, lanes + total, lanes + total + top, jnp.zeros((EXTRA - 3, width), jnp.float32)],
        axis=0,
    )


def cell_local_kernel(q_ref, k_ref, v_ref, forget_ref, input_ref, num_ref, aux_ref, *, tile):
    seq_len, width = q_ref.shape
    log_forget, cum_row, gap_row = log_rows(forget_ref, input_ref)
    for first in range(0, seq_len, tile):
        span = first + tile
        row, col = col_mask(first, tile, span)
        causal = col <= row
        own = (col // BLOCK) == (row // BLOCK)
        gap = jnp.where(causal, gap_row[:, :span], -jnp.inf)
        top = jnp.max(gap, axis=1, keepdims=True)
        cum = jnp.sum(jnp.where(causal, log_forget[:, :span], 0.0), axis=1, keepdims=True)
        scores = lax.dot_general(
            q_ref[first:span, :],
            k_ref[0:span, :],
            (((1,), (1,)), ((), ())),
            preferred_element_type=jnp.float32,
        ) * width ** (-0.5)
        weights = scores * jnp.exp(gap - top)
        high = weights.astype(jnp.bfloat16)
        high_float = high.astype(jnp.float32)
        low_float = jnp.where(own, 0.0, weights - high_float)
        v = v_ref[0:span, :]
        num_ref[first:span, :] = jnp.dot(high, v, preferred_element_type=jnp.float32) + jnp.dot(
            low_float.astype(jnp.bfloat16), v, preferred_element_type=jnp.float32
        )
        den = jnp.sum(high_float + low_float, axis=1, keepdims=True)
        lane = lax.broadcasted_iota(jnp.int32, (tile, 128), 1)
        aux_ref[first:span, :] = jnp.where(lane == 0, den, jnp.where(lane == 1, top, cum))


def cell_join_kernel(q_ref, num_ref, aux_ref, states_ref, rows_ref, mat_ref, *, axis):
    width = q_ref.shape[1]
    place = lax.axis_index(axis)
    mat_ref[...] = jnp.zeros_like(mat_ref)

    def join(step, carry):
        vector, old_max = carry
        extra = states_ref[step, width : width + EXTRA, :]
        new_max, total = extra[2:3], extra[1:2]
        joined = jnp.maximum(total + old_max, new_max)
        keep_old = jnp.exp(total + old_max - joined)
        keep_new = jnp.exp(new_max - joined)
        mat_ref[...] = keep_old * mat_ref[...] + keep_new * states_ref[step, 0:width, :]
        return keep_old * vector + keep_new * extra[0:1], joined

    vector, far_max = lax.fori_loop(
        0,
        place,
        join,
        (jnp.zeros((1, width), jnp.float32), jnp.full((1, width), FLOOR_LOG, jnp.float32)),
    )
    aux = aux_ref[...]
    den, top, cum = aux[:, 0:1], aux[:, 1:2], aux[:, 2:3]
    far = far_max[:, 0:1]
    joined = jnp.maximum(top, far)
    keep_own = jnp.exp(top - joined)
    keep_far = jnp.exp(far - joined)
    q_float = q_ref[...].astype(jnp.float32)
    one, rest = split_two(mat_ref[...])
    two, three = split_two(mat_ref[...] - one.astype(jnp.float32))
    q = q_ref[...]
    far_num = (
        jnp.dot(q, one, preferred_element_type=jnp.float32)
        + jnp.dot(q, two, preferred_element_type=jnp.float32)
        + jnp.dot(q, three, preferred_element_type=jnp.float32)
    )
    far_den = jnp.sum(q_float * vector, axis=1, keepdims=True)
    numerator = keep_own * num_ref[...] + keep_far * far_num
    denominator = keep_own * den + keep_far * far_den
    divisor = jnp.maximum(jnp.abs(denominator), jnp.exp(-(cum + joined)))
    rows_ref[...] = (numerator / divisor).astype(rows_ref.dtype)


def run_cell(query, keys, values, forget_pre, input_pre):
    seq_len, width = query.shape
    params = pltpu.CompilerParams(vmem_limit_bytes=VMEM_LIMIT)
    state = pl.pallas_call(
        cell_state_kernel,
        out_shape=jax.ShapeDtypeStruct((width + EXTRA, width), jnp.float32),
        compiler_params=params,
        cost_estimate=pl.CostEstimate(flops=10**9, bytes_accessed=2**20, transcendentals=0),
        name="cell_state",
    )(keys, values, forget_pre, input_pre)
    cut = (width + EXTRA) // 3
    parts = [lax.all_gather(state[i * cut : (i + 1) * cut], "sp") for i in range(3)]
    gathered = jnp.concatenate(parts, axis=1)
    tile = 4 * BLOCK if seq_len % (4 * BLOCK) == 0 else BLOCK
    numerator, aux = pl.pallas_call(
        functools.partial(cell_local_kernel, tile=tile),
        out_shape=(
            jax.ShapeDtypeStruct((seq_len, width), jnp.float32),
            jax.ShapeDtypeStruct((seq_len, 128), jnp.float32),
        ),
        compiler_params=params,
        cost_estimate=pl.CostEstimate(flops=5 * 10**9, bytes_accessed=2**21, transcendentals=0),
        name="cell_local",
    )(query, keys, values, forget_pre, input_pre)
    rows = pl.pallas_call(
        functools.partial(cell_join_kernel, axis="sp"),
        out_shape=jax.ShapeDtypeStruct((seq_len, width), jnp.bfloat16),
        scratch_shapes=[pltpu.VMEM((width, width), jnp.float32)],
        compiler_params=params,
        name="cell_join",
    )(query, numerator, aux, gathered)
    return rows


def sp_tp_barrier(barrier, counts):
    total = 0
    for axis, count in counts.items():
        place = lax.axis_index(axis)
        for step in range(1, count):
            pl.semaphore_signal(
                barrier,
                inc=1,
                device_id={axis: lax.rem(place + step, count)},
                device_id_type=pl.DeviceIdType.MESH,
            )
        total += count - 1
    return total


def cell_kernel(
    q_ref,
    k_ref,
    v_ref,
    forget_ref,
    input_ref,
    out_ref,
    state_ref,
    piece_ref,
    extra_ref,
    prefix_ref,
    mat_ref,
    num_ref,
    aux_ref,
    rows_ref,
    send_sems,
    recv_sems,
    extra_send_sems,
    extra_recv_sems,
    back_send_sems,
    back_recv_sems,
    turn_send_sems,
    turn_recv_sems,
    own_sem,
    *,
    count,
    heads,
    tile,
):
    seq_len, width = q_ref.shape
    cut = width // count
    place = lax.axis_index("sp")
    head = lax.axis_index("tp")
    barrier = pltpu.get_barrier_semaphore()
    greeted = sp_tp_barrier(barrier, {"sp": count, "tp": heads})
    log_forget, cum_row, gap_row = log_rows(forget_ref, input_ref)
    total = jnp.sum(log_forget, axis=1, keepdims=True)
    best = jnp.max(gap_row, axis=1, keepdims=True)
    keep_row = jnp.exp(gap_row - best) * width ** (-0.5)
    weighted = k_ref[...].astype(jnp.float32).T * keep_row
    high, low = split_two(weighted)
    v_all = v_ref[...]
    state_ref[0:width, :] = jnp.dot(high, v_all, preferred_element_type=jnp.float32) + jnp.dot(
        low, v_all, preferred_element_type=jnp.float32
    )
    vector = jnp.dot(
        jnp.broadcast_to(keep_row, (8, seq_len)),
        k_ref[...].astype(jnp.float32),
        precision=HIGHEST,
        preferred_element_type=jnp.float32,
    )[0:1]
    lanes = jnp.zeros((1, width), jnp.float32)
    state_ref[width : width + EXTRA, :] = jnp.concatenate(
        [vector, lanes + total, lanes + total + best, jnp.zeros((EXTRA - 3, width), jnp.float32)],
        axis=0,
    )
    pl.semaphore_wait(barrier, greeted)
    sends = []
    for step in range(1, count):
        peer = lax.rem(place + step, count)
        extra_copy = pltpu.make_async_remote_copy(
            src_ref=state_ref.at[pl.ds(width, EXTRA)],
            dst_ref=extra_ref.at[place],
            send_sem=extra_send_sems.at[step - 1],
            recv_sem=extra_recv_sems.at[step - 1],
            device_id={"sp": peer},
            device_id_type=pl.DeviceIdType.MESH,
        )
        piece_copy = pltpu.make_async_remote_copy(
            src_ref=state_ref.at[pl.ds(pl.multiple_of(peer * cut, cut), cut)],
            dst_ref=piece_ref.at[place],
            send_sem=send_sems.at[step - 1],
            recv_sem=recv_sems.at[step - 1],
            device_id={"sp": peer},
            device_id_type=pl.DeviceIdType.MESH,
        )
        extra_copy.start()
        piece_copy.start()
        sends += [extra_copy, piece_copy]
    extra_ref[place] = state_ref[width : width + EXTRA, :]
    piece_ref[place] = state_ref[pl.ds(pl.multiple_of(place * cut, cut), cut), :]

    for first in range(0, seq_len, tile):
        span = first + tile
        row, col = col_mask(first, tile, span)
        causal = col <= row
        own = (col // BLOCK) == (row // BLOCK)
        gap = jnp.where(causal, gap_row[:, :span], -jnp.inf)
        top = jnp.max(gap, axis=1, keepdims=True)
        cum = jnp.sum(jnp.where(causal, log_forget[:, :span], 0.0), axis=1, keepdims=True)
        scores = lax.dot_general(
            q_ref[first:span, :],
            k_ref[0:span, :],
            (((1,), (1,)), ((), ())),
            preferred_element_type=jnp.float32,
        ) * width ** (-0.5)
        weights = scores * jnp.exp(gap - top)
        high = weights.astype(jnp.bfloat16)
        high_float = high.astype(jnp.float32)
        low_float = jnp.where(own, 0.0, weights - high_float)
        v = v_ref[0:span, :]
        num_ref[first:span, :] = jnp.dot(high, v, preferred_element_type=jnp.float32) + jnp.dot(
            low_float.astype(jnp.bfloat16), v, preferred_element_type=jnp.float32
        )
        den = jnp.sum(high_float + low_float, axis=1, keepdims=True)
        lane = lax.broadcasted_iota(jnp.int32, (tile, 128), 1)
        aux_ref[first:span, :] = jnp.where(lane == 0, den, jnp.where(lane == 1, top, cum))

    for copy in sends:
        copy.wait()

    running = jnp.zeros((cut, width), jnp.float32)
    vector = jnp.zeros((1, width), jnp.float32)
    far_max = jnp.full((1, width), FLOOR_LOG, jnp.float32)
    own_vector, own_max = vector, far_max
    for step in range(count):
        prefix_ref[step] = running
        own_vector = jnp.where(place == step, vector, own_vector)
        own_max = jnp.where(place == step, far_max, own_max)
        if step < count - 1:
            extra = extra_ref[step]
            new_max, step_total = extra[2:3], extra[1:2]
            joined = jnp.maximum(step_total + far_max, new_max)
            keep_old = jnp.exp(step_total + far_max - joined)
            keep_new = jnp.exp(new_max - joined)
            running = keep_old * running + keep_new * piece_ref[step]
            vector = keep_old * vector + keep_new * extra[0:1]
            far_max = joined
    backs = []
    for step in range(1, count):
        peer = lax.rem(place + step, count)
        back = pltpu.make_async_remote_copy(
            src_ref=prefix_ref.at[peer],
            dst_ref=mat_ref.at[pl.ds(pl.multiple_of(place * cut, cut), cut)],
            send_sem=back_send_sems.at[step - 1],
            recv_sem=back_recv_sems.at[step - 1],
            device_id={"sp": peer},
            device_id_type=pl.DeviceIdType.MESH,
        )
        back.start()
        backs.append(back)
    mat_ref[pl.ds(pl.multiple_of(place * cut, cut), cut), :] = prefix_ref[place]

    aux = aux_ref[...]
    den, top, cum = aux[:, 0:1], aux[:, 1:2], aux[:, 2:3]
    far = own_max[:, 0:1]
    joined = jnp.maximum(top, far)
    keep_own = jnp.exp(top - joined)
    keep_far = jnp.exp(far - joined)
    q_float = q_ref[...].astype(jnp.float32)
    far_den = jnp.sum(q_float * own_vector, axis=1, keepdims=True)
    denominator = keep_own * den + keep_far * far_den
    divisor = jnp.maximum(jnp.abs(denominator), jnp.exp(-(cum + joined)))
    for copy in backs:
        copy.wait()
    one, rest = split_two(mat_ref[...])
    two, three = split_two(mat_ref[...] - one.astype(jnp.float32))
    q = q_ref[...]
    far_num = (
        jnp.dot(q, one, preferred_element_type=jnp.float32)
        + jnp.dot(q, two, preferred_element_type=jnp.float32)
        + jnp.dot(q, three, preferred_element_type=jnp.float32)
    )
    numerator = keep_own * num_ref[...] + keep_far * far_num
    rows_ref[...] = (numerator / divisor).astype(rows_ref.dtype)

    share = seq_len // heads
    columns = pl.ds(pl.multiple_of(head * width, width), width)
    turns = []
    for step in range(1, heads):
        peer = lax.rem(head + step, heads)
        turn = pltpu.make_async_remote_copy(
            src_ref=rows_ref.at[pl.ds(pl.multiple_of(peer * share, share), share)],
            dst_ref=out_ref.at[:, columns],
            send_sem=turn_send_sems.at[step - 1],
            recv_sem=turn_recv_sems.at[step - 1],
            device_id={"tp": peer},
            device_id_type=pl.DeviceIdType.MESH,
        )
        turn.start()
        turns.append(turn)
    own_copy = pltpu.make_async_copy(
        rows_ref.at[pl.ds(pl.multiple_of(head * share, share), share)],
        out_ref.at[:, columns],
        own_sem,
    )
    own_copy.start()
    own_copy.wait()
    for turn in turns:
        turn.wait()


def run_cell_scan(query, keys, values, forget_pre, input_pre):
    seq_len, width = query.shape
    count, heads = lax.axis_size("sp"), lax.axis_size("tp")
    tile = 4 * BLOCK if seq_len % (4 * BLOCK) == 0 else BLOCK
    cut = width // count
    vmem = pl.BlockSpec(memory_space=pltpu.VMEM)
    dma = pltpu.SemaphoreType.DMA
    return pl.pallas_call(
        functools.partial(cell_kernel, count=count, heads=heads, tile=tile),
        out_shape=jax.ShapeDtypeStruct((seq_len // heads, heads * width), jnp.bfloat16),
        in_specs=[vmem] * 5,
        out_specs=vmem,
        scratch_shapes=[
            pltpu.VMEM((width + EXTRA, width), jnp.float32),
            pltpu.VMEM((count, cut, width), jnp.float32),
            pltpu.VMEM((count, EXTRA, width), jnp.float32),
            pltpu.VMEM((count, cut, width), jnp.float32),
            pltpu.VMEM((width, width), jnp.float32),
            pltpu.VMEM((seq_len, width), jnp.float32),
            pltpu.VMEM((seq_len, 128), jnp.float32),
            pltpu.VMEM((seq_len, width), jnp.bfloat16),
            dma((count - 1,)),
            dma((count - 1,)),
            dma((count - 1,)),
            dma((count - 1,)),
            dma((count - 1,)),
            dma((count - 1,)),
            dma((heads - 1,)),
            dma((heads - 1,)),
            dma(()),
        ],
        compiler_params=pltpu.CompilerParams(
            vmem_limit_bytes=VMEM_LIMIT, collective_id=3, has_side_effects=True
        ),
        cost_estimate=pl.CostEstimate(flops=10**10, bytes_accessed=2**21, transcendentals=0),
        name="cell",
    )(query, keys, values, forget_pre, input_pre)


def token_cell(query, keys, values, forget_pre, input_pre):
    if query.shape[1] % (8 * lax.axis_size("sp")) == 0:
        return run_cell_scan(query, keys, values, forget_pre, input_pre)
    rows = run_cell(query, keys, values, forget_pre, input_pre)
    return lax.all_to_all(rows, "tp", split_axis=0, concat_axis=1, tiled=True)


def layer_kernel(
    q_ref,
    k_ref,
    v_ref,
    forget_ref,
    input_ref,
    head_gain_ref,
    ffn_gain_ref,
    routes_ref,
    scores_ref,
    resid_hbm,
    out_gate_hbm,
    out_proj_hbm,
    gate_hbm,
    up_hbm,
    down_hbm,
    out_ref,
    state_ref,
    piece_ref,
    extra_ref,
    prefix_ref,
    mat_ref,
    num_ref,
    aux_ref,
    cell_ref,
    token_ref,
    resid_ref,
    out_gate_ref,
    out_proj_ref,
    gate_ref,
    up_ref,
    down_ref,
    twin_down_ref,
    infos_ref,
    rows_ref,
    held_ref,
    cross_ref,
    crossed_ref,
    answer_ref,
    back_ref,
    batch_ref,
    done_ref,
    part_ref,
    own_ref,
    sum_ref,
    load_sems,
    own_sem,
    send_sems,
    recv_sems,
    extra_send_sems,
    extra_recv_sems,
    back_send_sems,
    back_recv_sems,
    turn_send_sems,
    turn_recv_sems,
    info_send,
    info_recv,
    row_send,
    row_recv,
    cross_send,
    cross_recv,
    answer_send,
    answer_recv,
    sum_send,
    sum_recv,
    weight_send,
    weight_recv,
    *,
    count,
    heads,
    line,
    halves,
    slots,
    pieces,
    tile,
):
    seq_len, width = q_ref.shape
    cut = width // count
    place = lax.axis_index("sp")
    head = lax.axis_index("tp")
    here = place // 2
    side = lax.rem(place, 2)
    twin = place + 1 - 2 * side
    mate = head + 1 - 2 * lax.rem(head, 2)
    across = lax.rem(head + 2, heads)
    units = line * halves
    tokens = rows_ref.shape[1]
    grain = tokens // pieces
    last = line - 1
    shares = WEIGHT_PIECES
    chunks = shares

    def remote(src, dst, send, recv, peer, axis="sp"):
        return pltpu.make_async_remote_copy(
            src_ref=src,
            dst_ref=dst,
            send_sem=send,
            recv_sem=recv,
            device_id={axis: peer},
            device_id_type=pl.DeviceIdType.MESH,
        )

    loads = [
        pltpu.make_async_copy(src, dst, load_sems.at[i])
        for i, (src, dst) in enumerate(
            [
                (out_gate_hbm, out_gate_ref),
                (resid_hbm, resid_ref),
                (out_proj_hbm, out_proj_ref),
                (gate_hbm, gate_ref),
                (up_hbm, up_ref),
                (down_hbm, down_ref),
            ]
        )
    ]
    for load in loads:
        load.start()

    barrier = pltpu.get_barrier_semaphore()
    greeted = sp_tp_barrier(barrier, {"sp": count, "tp": heads})

    def weight_rows(chunk, owner):
        quarter = twin_down_ref.shape[0] // heads
        size = quarter // shares
        rows = pl.ds(pl.multiple_of(owner * quarter + chunk * size, size), size)
        return down_hbm.at[0, rows], twin_down_ref.at[rows]

    def weight_copy(stage, chunk):
        owner, peer, axis = (
            (head, twin, "sp"),
            (head, across, "tp"),
            (head, mate, "tp"),
            (across, mate, "tp"),
        )[stage]
        whole, landed = weight_rows(chunk, owner)
        return remote(
            whole if stage == 0 else landed,
            landed,
            weight_send.at[stage, chunk],
            weight_recv.at[stage, chunk],
            peer,
            axis,
        )

    def fetch(*span):
        for chunk in range(*span):
            weight_copy(0, chunk).start()

    def pass_on(*span):
        for chunk in range(*span):
            weight_copy(0, chunk).wait_recv()
            weight_copy(1, chunk).start()
            weight_copy(2, chunk).start()

    def hand_over(*span):
        for chunk in range(*span):
            weight_copy(1, chunk).wait_recv()
            weight_copy(3, chunk).start()

    def info_copy(step):
        peer = lax.rem(here + step, line)
        return remote(
            infos_ref.at[here],
            infos_ref.at[here],
            info_send.at[step - 1],
            info_recv.at[step - 1],
            peer * 2 + side,
        )

    eye_row, eye_col = col_mask(0, tokens, tokens)
    eye = jnp.where(eye_row == eye_col, 1.0, 0.0)
    for half in range(halves):
        span = slice(half * tokens, (half + 1) * tokens)
        ids = routes_ref[:, span].astype(jnp.float32)
        scores = scores_ref[:, span]
        zeros = jnp.zeros((8 - ids.shape[0], tokens), jnp.float32)
        columns = lax.dot_general(
            eye,
            jnp.concatenate([ids, zeros], axis=0),
            (((1,), (1,)), ((), ())),
            precision=HIGHEST,
            preferred_element_type=jnp.float32,
        )
        ranks = []
        for route in range(2):
            rank = jnp.zeros((1, tokens), jnp.float32)
            for other in range(2):
                same = (columns[:, other : other + 1] == ids[route : route + 1]) & (eye_row < eye_col)
                rank += jnp.sum(jnp.where(same, 1.0, 0.0), axis=0, keepdims=True)
            ranks.append(rank)
        infos_ref[here, half] = jnp.concatenate(
            [ids] + ranks + [scores / jnp.sum(scores, axis=0, keepdims=True), zeros[0:2]], axis=0
        )

    log_forget, cum_row, gap_row = log_rows(forget_ref, input_ref)
    pl.semaphore_wait(barrier, greeted)
    total = jnp.sum(log_forget, axis=1, keepdims=True)
    best = jnp.max(gap_row, axis=1, keepdims=True)
    keep_row = jnp.exp(gap_row - best) * width ** (-0.5)
    weighted = k_ref[...].astype(jnp.float32).T * keep_row
    high, low = split_two(weighted)
    v_all = v_ref[...]
    state_ref[0:width, :] = jnp.dot(high, v_all, preferred_element_type=jnp.float32) + jnp.dot(
        low, v_all, preferred_element_type=jnp.float32
    )
    vector = jnp.dot(
        jnp.broadcast_to(keep_row, (8, seq_len)),
        k_ref[...].astype(jnp.float32),
        precision=HIGHEST,
        preferred_element_type=jnp.float32,
    )[0:1]
    lanes = jnp.zeros((1, width), jnp.float32)
    state_ref[width : width + EXTRA, :] = jnp.concatenate(
        [vector, lanes + total, lanes + total + best, jnp.zeros((EXTRA - 3, width), jnp.float32)],
        axis=0,
    )
    for step in range(1, line):
        info_copy(step).start()
    sends = []
    for step in range(1, count):
        peer = lax.rem(place + step, count)
        extra_copy = pltpu.make_async_remote_copy(
            src_ref=state_ref.at[pl.ds(width, EXTRA)],
            dst_ref=extra_ref.at[place],
            send_sem=extra_send_sems.at[step - 1],
            recv_sem=extra_recv_sems.at[step - 1],
            device_id={"sp": peer},
            device_id_type=pl.DeviceIdType.MESH,
        )
        piece_copy = pltpu.make_async_remote_copy(
            src_ref=state_ref.at[pl.ds(pl.multiple_of(peer * cut, cut), cut)],
            dst_ref=piece_ref.at[place],
            send_sem=send_sems.at[step - 1],
            recv_sem=recv_sems.at[step - 1],
            device_id={"sp": peer},
            device_id_type=pl.DeviceIdType.MESH,
        )
        extra_copy.start()
        piece_copy.start()
        sends += [extra_copy, piece_copy]
    extra_ref[place] = state_ref[width : width + EXTRA, :]
    piece_ref[place] = state_ref[pl.ds(pl.multiple_of(place * cut, cut), cut), :]


    fetch(0, 2)
    for first in range(0, seq_len, tile):
        span = first + tile
        row, col = col_mask(first, tile, span)
        causal = col <= row
        own = (col // BLOCK) == (row // BLOCK)
        gap = jnp.where(causal, gap_row[:, :span], -jnp.inf)
        top = jnp.max(gap, axis=1, keepdims=True)
        cum = jnp.sum(jnp.where(causal, log_forget[:, :span], 0.0), axis=1, keepdims=True)
        scores = lax.dot_general(
            q_ref[first:span, :],
            k_ref[0:span, :],
            (((1,), (1,)), ((), ())),
            preferred_element_type=jnp.float32,
        ) * width ** (-0.5)
        weights = scores * jnp.exp(gap - top)
        high = weights.astype(jnp.bfloat16)
        high_float = high.astype(jnp.float32)
        low_float = jnp.where(own, 0.0, weights - high_float)
        v = v_ref[0:span, :]
        num_ref[first:span, :] = jnp.dot(high, v, preferred_element_type=jnp.float32) + jnp.dot(
            low_float.astype(jnp.bfloat16), v, preferred_element_type=jnp.float32
        )
        den = jnp.sum(high_float + low_float, axis=1, keepdims=True)
        lane = lax.broadcasted_iota(jnp.int32, (tile, 128), 1)
        aux_ref[first:span, :] = jnp.where(lane == 0, den, jnp.where(lane == 1, top, cum))

    for copy in sends:
        copy.wait()

    running = jnp.zeros((cut, width), jnp.float32)
    vector = jnp.zeros((1, width), jnp.float32)
    far_max = jnp.full((1, width), FLOOR_LOG, jnp.float32)
    own_vector, own_max = vector, far_max
    for step in range(count):
        prefix_ref[step] = running
        own_vector = jnp.where(place == step, vector, own_vector)
        own_max = jnp.where(place == step, far_max, own_max)
        if step < count - 1:
            extra = extra_ref[step]
            new_max, step_total = extra[2:3], extra[1:2]
            joined = jnp.maximum(step_total + far_max, new_max)
            keep_old = jnp.exp(step_total + far_max - joined)
            keep_new = jnp.exp(new_max - joined)
            running = keep_old * running + keep_new * piece_ref[step]
            vector = keep_old * vector + keep_new * extra[0:1]
            far_max = joined
    backs = []
    for step in range(1, count):
        peer = lax.rem(place + step, count)
        back = pltpu.make_async_remote_copy(
            src_ref=prefix_ref.at[peer],
            dst_ref=mat_ref.at[pl.ds(pl.multiple_of(place * cut, cut), cut)],
            send_sem=back_send_sems.at[step - 1],
            recv_sem=back_recv_sems.at[step - 1],
            device_id={"sp": peer},
            device_id_type=pl.DeviceIdType.MESH,
        )
        back.start()
        backs.append(back)
    mat_ref[pl.ds(pl.multiple_of(place * cut, cut), cut), :] = prefix_ref[place]

    fetch(2, chunks)
    aux = aux_ref[...]
    den, top, cum = aux[:, 0:1], aux[:, 1:2], aux[:, 2:3]
    far = own_max[:, 0:1]
    joined = jnp.maximum(top, far)
    keep_own = jnp.exp(top - joined)
    keep_far = jnp.exp(far - joined)
    q_float = q_ref[...].astype(jnp.float32)
    far_den = jnp.sum(q_float * own_vector, axis=1, keepdims=True)
    denominator = keep_own * den + keep_far * far_den
    divisor = jnp.maximum(jnp.abs(denominator), jnp.exp(-(cum + joined)))
    for copy in backs:
        copy.wait()
    one, rest = split_two(mat_ref[...])
    two, three = split_two(mat_ref[...] - one.astype(jnp.float32))
    q = q_ref[...]
    far_num = (
        jnp.dot(q, one, preferred_element_type=jnp.float32)
        + jnp.dot(q, two, preferred_element_type=jnp.float32)
        + jnp.dot(q, three, preferred_element_type=jnp.float32)
    )
    numerator = keep_own * num_ref[...] + keep_far * far_num
    cell_ref[...] = (numerator / divisor).astype(cell_ref.dtype)

    share = seq_len // heads
    columns = pl.ds(pl.multiple_of(head * width, width), width)
    turns = []
    for step in range(1, heads):
        peer = lax.rem(head + step, heads)
        turn = pltpu.make_async_remote_copy(
            src_ref=cell_ref.at[pl.ds(pl.multiple_of(peer * share, share), share)],
            dst_ref=token_ref.at[:, columns],
            send_sem=turn_send_sems.at[step - 1],
            recv_sem=turn_recv_sems.at[step - 1],
            device_id={"tp": peer},
            device_id_type=pl.DeviceIdType.MESH,
        )
        turn.start()
        turns.append(turn)
    own_copy = pltpu.make_async_copy(
        cell_ref.at[pl.ds(pl.multiple_of(head * share, share), share)],
        token_ref.at[:, columns],
        own_sem,
    )
    own_copy.start()
    for load in loads[:3]:
        load.wait()
    own_copy.wait()
    for copy in turns:
        copy.wait()
    pass_on(0, chunks)

    def row_copy(src, source, half, way):
        unit = source * halves + half
        return remote(
            src,
            held_ref.at[unit],
            row_send.at[way, unit],
            row_recv.at[unit],
            place + (4 * way - 2),
        )

    def cross_copy(unit):
        return remote(
            cross_ref.at[unit],
            crossed_ref.at[unit],
            cross_send.at[unit],
            cross_recv.at[unit],
            twin,
        )

    def answer_copy(unit):
        return remote(
            answer_ref.at[unit],
            back_ref.at[unit],
            answer_send.at[unit],
            answer_recv.at[unit],
            twin,
        )

    def sum_copy(target, half, way, piece):
        landing = ((target + way) * halves + half) * pieces + piece
        leaving = (target * halves + half) * pieces + piece
        return remote(
            part_ref.at[leaving],
            sum_ref.at[landing],
            sum_send.at[leaving],
            sum_recv.at[landing],
            place + (4 * way - 2),
        )

    def sum_wait(landing):
        remote(
            part_ref.at[0], sum_ref.at[landing], sum_send.at[0], sum_recv.at[landing], twin
        ).wait_recv()

    for half in range(halves):
        span = slice(half * tokens, (half + 1) * tokens)
        cell_float = token_ref[span, :].astype(jnp.float32)
        headed = (
            cell_float
            * lax.rsqrt(jnp.mean(cell_float * cell_float, axis=1, keepdims=True) + EPS)
            * head_gain_ref[...]
        )
        gated = (headed * jax.nn.sigmoid(out_gate_ref[span, :].astype(jnp.float32))).astype(
            jnp.bfloat16
        )
        mixed = resid_ref[span, :].astype(jnp.float32) + jnp.dot(
            gated, out_proj_ref[...], preferred_element_type=jnp.float32
        )
        own_ref[half] = mixed
        normed = (
            mixed
            * lax.rsqrt(jnp.mean(mixed * mixed, axis=1, keepdims=True) + EPS)
            * ffn_gain_ref[...]
        ).astype(jnp.bfloat16)
        rows_ref[half] = normed
        held_ref[here * halves + half] = normed
        if half == 0:
            for way in range(2):

                @pl.when((here < last) if way else (here > 0))
                def _():
                    row_copy(rows_ref.at[0], here, 0, way).start()

    def later_halves(way):
        for half in range(1, halves):
            row_copy(rows_ref.at[half], here, half, way).start()

    @pl.when(here == 0)
    def _():
        later_halves(1)

    @pl.when(here == last)
    def _():
        later_halves(0)

    for step in range(1, line):
        info_copy(step).wait()
    shorter = jnp.minimum(here, last - here)

    def in_stream(p, reach):
        first = p < reach
        turn = p - reach
        ahead = jnp.where(first, p + 1, reach - turn // (halves - 1))
        return ahead, jnp.where(first, 0, 1 + lax.rem(turn, halves - 1))

    def source_of(k):
        p = k - halves
        both = shorter * 2 * halves
        paired = p < both
        way = jnp.where(paired, lax.rem(p, 2), jnp.where(here < last - here, 1, 0))
        spot = jnp.where(paired, p // 2, p - shorter * halves)
        reach = jnp.where(way == 1, last - here, here)
        ahead, half = in_stream(spot, reach)
        is_own = k < halves
        final = spot == reach * halves - 1
        return (
            jnp.where(is_own, here, here + ahead * (2 * way - 1)),
            jnp.where(is_own, k, half),
            final,
        )

    def matches(source, half, weighted):
        info = infos_ref[source, half]
        rank = lax.broadcasted_iota(jnp.int32, (slots, tokens), 0).astype(jnp.float32)
        tables = []
        for expert in (place, twin):
            name = expert.astype(jnp.float32)
            table = jnp.zeros((slots, tokens), jnp.float32)
            for route in range(2):
                hit = jnp.where(info[route : route + 1] == name, info[2 + route : 3 + route], -1.0)
                value = info[4 + route : 5 + route] if weighted else 1.0
                table += jnp.where(hit == rank, value, 0.0)
            tables.append(table)
        return jnp.concatenate(tables, axis=0)

    first_way = jnp.where(last - here <= here, 0, 1)

    def relay(way, spot):
        reach = jnp.where(way == 1, last - here, here)

        @pl.when((spot >= 0) & (spot < reach * halves) & (here > 0) & (here < last))
        def _():
            ahead, half = in_stream(spot, reach)
            target = here + ahead * (2 * way - 1)
            for piece in range(pieces):
                unit = (target * halves + half) * pieces + piece
                landing = ((target + way) * halves + half) * pieces + piece
                sum_wait(landing)
                part_ref[unit] = (
                    part_ref[unit].astype(jnp.float32) + sum_ref[landing].astype(jnp.float32)
                ).astype(jnp.bfloat16)
                sum_copy(target, half, way, piece).start()

    def down(active, mat):
        return jnp.dot(active, mat, preferred_element_type=jnp.float32).astype(jnp.bfloat16)

    def activate(rows):
        gate = jnp.dot(rows, gate_ref[0], preferred_element_type=jnp.float32)
        up = jnp.dot(rows, up_ref[0], preferred_element_type=jnp.float32)
        return (jax.nn.silu(gate) * up).astype(jnp.bfloat16)

    inner_stop = (here > 0) & (here < last)
    lag = jnp.where(inner_stop, 1, 0)

    def step_body(k, carry):
        @pl.when(k < units)
        def _():
            source, half, final = source_of(k)
            unit = source * halves + half

            @pl.when(source != here)
            def _():
                remote(
                    held_ref.at[unit], held_ref.at[unit], row_send.at[0, unit], row_recv.at[unit], twin
                ).wait_recv()

            @pl.when((source < here) & (here < last))
            def _():
                row_copy(held_ref.at[unit], source, half, 1).start()

                @pl.when(final)
                def _():
                    later_halves(1)

            @pl.when((source > here) & (here > 0))
            def _():
                row_copy(held_ref.at[unit], source, half, 0).start()

                @pl.when(final)
                def _():
                    later_halves(0)

            packed = jnp.dot(
                matches(source, half, False).astype(jnp.bfloat16),
                held_ref[unit],
                preferred_element_type=jnp.float32,
            ).astype(jnp.bfloat16)
            cross_ref[unit] = packed[slots:]
            cross_copy(unit).start()
            batch_ref[...] = packed[:slots]

        @pl.when(k == 0)
        def _():
            for load in loads[3:]:
                load.wait()

        @pl.when(k == 1)
        def _():
            hand_over(0, chunks)

        @pl.when(k < units)
        def _():
            source, half, _ = source_of(k)
            done_ref[source * halves + half, 0:slots, :] = down(
                activate(batch_ref[...]), down_ref[0]
            )

        @pl.when(k == 1 + halves)
        def _():
            for chunk in range(chunks):
                weight_copy(2, chunk).wait_recv()
                weight_copy(3, chunk).wait_recv()

        def answer_twin():
            source, half, _ = source_of(k - lag)
            unit = source * halves + half
            cross_copy(unit).wait_recv()
            answer_ref[unit] = activate(crossed_ref[unit])
            answer_copy(unit).start()

        pl.when(inner_stop & (k >= lag) & (k < units + lag))(answer_twin)

        relay(first_way, k - units)
        relay(1 - first_way, k - units - 2)
        turn_now = k - 1 - lag

        @pl.when((turn_now >= halves) & (turn_now < units + halves))
        def _():
            source, half, _ = source_of(jnp.where(turn_now < units, turn_now, turn_now - units))
            unit = source * halves + half
            answer_copy(unit).wait_recv()
            done_ref[unit, slots : 2 * slots, :] = down(back_ref[unit], twin_down_ref[...])
            high, low = split_two(matches(source, half, True))
            answers = done_ref[unit]
            turned = (((0,), (0,)), ((), ()))
            part = lax.dot_general(
                high, answers, turned, preferred_element_type=jnp.float32
            ) + lax.dot_general(low, answers, turned, preferred_element_type=jnp.float32)

            @pl.when(source == here)
            def _():
                own_ref[half] = own_ref[half] + part

            @pl.when(source != here)
            def _():
                for piece in range(pieces):
                    part_ref[unit * pieces + piece] = part[
                        piece * grain : (piece + 1) * grain
                    ].astype(jnp.bfloat16)

            @pl.when((source < here) & (here == last))
            def _():
                for piece in range(pieces):
                    sum_copy(source, half, 0, piece).start()

            @pl.when((source > here) & (here == 0))
            def _():
                for piece in range(pieces):
                    sum_copy(source, half, 1, piece).start()

        pl.when(~inner_stop & (k < units))(answer_twin)

        return carry

    lax.fori_loop(0, units + 2 + halves, step_body, 0)

    for half in range(halves):
        for piece in range(pieces):
            rows = pl.ds(piece * grain, grain)
            for way in range(2):

                @pl.when((here > 0) if way else (here < last))
                def _():
                    landing = ((here + way) * halves + half) * pieces + piece
                    sum_wait(landing)
                    own_ref[half, rows] = own_ref[half, rows] + sum_ref[landing].astype(jnp.float32)

            out_ref[half, rows] = own_ref[half, rows].astype(out_ref.dtype)

    def drain(unit, carry):
        source = unit // halves
        half = lax.rem(unit, halves)
        cross_copy(unit).wait_send()
        answer_copy(unit).wait_send()

        @pl.when((source <= here) & (here < last))
        def _():
            row_copy(held_ref.at[unit], source, half, 1).wait_send()

        @pl.when((source >= here) & (here > 0))
        def _():
            row_copy(held_ref.at[unit], source, half, 0).wait_send()

        @pl.when(source != here)
        def _():
            for piece in range(pieces):
                sum_copy(source, half, 0, piece).wait_send()

        return carry

    lax.fori_loop(0, units, drain, 0)
    for chunk in range(chunks):
        for stage in range(4):
            weight_copy(stage, chunk).wait_send()


def run_layer(
    resid,
    query,
    keys,
    values,
    out_gate,
    forget_pre,
    input_pre,
    head_gain,
    out_proj,
    ffn_gain,
    routes,
    route_scores,
    w_gate,
    w_up,
    w_down,
    halves,
    slots,
):
    count, heads = lax.axis_size("sp"), lax.axis_size("tp")
    line = count // 2
    units = line * halves
    seq_len, width = query.shape
    cut = width // count
    share = seq_len // heads
    wide, inner = resid.shape[1], w_down.shape[1]
    tokens = share // halves
    pieces = 2
    grain = tokens // pieces
    tile = 4 * BLOCK if seq_len % (4 * BLOCK) == 0 else BLOCK
    vmem = pl.BlockSpec(memory_space=pltpu.VMEM)
    whole = pl.BlockSpec(memory_space=pl.ANY)
    dma = pltpu.SemaphoreType.DMA
    f32, bf16 = jnp.float32, jnp.bfloat16
    chunks = WEIGHT_PIECES
    out = pl.pallas_call(
        functools.partial(
            layer_kernel,
            count=count,
            heads=heads,
            line=line,
            halves=halves,
            slots=slots,
            pieces=pieces,
            tile=tile,
        ),
        out_shape=jax.ShapeDtypeStruct((halves, tokens, wide), bf16),
        in_specs=[vmem] * 9 + [whole] * 6,
        out_specs=vmem,
        scratch_shapes=[
            pltpu.VMEM((width + EXTRA, width), f32),
            pltpu.VMEM((count, cut, width), f32),
            pltpu.VMEM((count, EXTRA, width), f32),
            pltpu.VMEM((count, cut, width), f32),
            pltpu.VMEM((width, width), f32),
            pltpu.VMEM((seq_len, width), f32),
            pltpu.VMEM((seq_len, 128), f32),
            pltpu.VMEM((seq_len, width), bf16),
            pltpu.VMEM((share, heads * width), bf16),
            pltpu.VMEM(resid.shape, bf16),
            pltpu.VMEM(out_gate.shape, bf16),
            pltpu.VMEM(out_proj.shape, bf16),
            pltpu.VMEM(w_gate.shape, bf16),
            pltpu.VMEM(w_up.shape, bf16),
            pltpu.VMEM(w_down.shape, bf16),
            pltpu.VMEM(w_down.shape[1:], bf16),
            pltpu.VMEM((line, halves, 8, tokens), f32),
            pltpu.VMEM((halves, tokens, wide), bf16),
            pltpu.VMEM((units, tokens, wide), bf16),
            pltpu.VMEM((units, slots, wide), bf16),
            pltpu.VMEM((units, slots, wide), bf16),
            pltpu.VMEM((units, slots, inner), bf16),
            pltpu.VMEM((units, slots, inner), bf16),
            pltpu.VMEM((slots, wide), bf16),
            pltpu.VMEM((units, 2 * slots, wide), bf16),
            pltpu.VMEM((units * pieces, grain, wide), bf16),
            pltpu.VMEM((halves, tokens, wide), f32),
            pltpu.VMEM(((units + halves) * pieces, grain, wide), bf16),
            dma((6,)),
            dma(()),
            dma((count - 1,)),
            dma((count - 1,)),
            dma((count - 1,)),
            dma((count - 1,)),
            dma((count - 1,)),
            dma((count - 1,)),
            dma((heads - 1,)),
            dma((heads - 1,)),
            dma((line - 1,)),
            dma((line - 1,)),
            dma((2, units)),
            dma((units,)),
            dma((units,)),
            dma((units,)),
            dma((units,)),
            dma((units,)),
            dma((units * pieces,)),
            dma(((units + halves) * pieces,)),
            dma((4, chunks)),
            dma((4, chunks)),
        ],
        compiler_params=pltpu.CompilerParams(
            vmem_limit_bytes=LAYER_VMEM, collective_id=5, has_side_effects=True
        ),
        cost_estimate=pl.CostEstimate(flops=10**10, bytes_accessed=2**24, transcendentals=0),
        name="layer",
    )(
        query,
        keys,
        values,
        forget_pre,
        input_pre,
        head_gain[None, :],
        ffn_gain[None, :],
        routes.T,
        route_scores.T,
        resid,
        out_gate,
        out_proj,
        w_gate,
        w_up,
        w_down,
    )
    return out.reshape(share, wide)


def slot_select(expert_ids, expert_count, capacity):
    flat_ids = expert_ids.reshape(-1)
    one_hot = (flat_ids[:, None] == jnp.arange(expert_count, dtype=jnp.int32)[None, :]).astype(
        jnp.int32
    )
    slot_rank = jnp.sum((jnp.cumsum(one_hot, axis=0) - 1) * one_hot, axis=1)
    target = flat_ids * capacity + slot_rank
    return (
        jnp.arange(expert_count * capacity, dtype=jnp.int32)[:, None] == target[None, :]
    ).astype(jnp.bfloat16)


def exchange_kernel(send_ref, recv_ref, send_sems, recv_sems, own_sem, *, axis, count):
    place = lax.axis_index(axis)
    barrier = pltpu.get_barrier_semaphore()
    for step in range(1, count):
        peer = lax.rem(place + step, count)
        pl.semaphore_signal(
            barrier, inc=1, device_id={axis: peer}, device_id_type=pl.DeviceIdType.MESH
        )
    own = pltpu.make_async_copy(send_ref.at[place], recv_ref.at[place], own_sem)
    own.start()
    pl.semaphore_wait(barrier, count - 1)
    copies = []
    for step in range(1, count):
        peer = lax.rem(place + step, count)
        copy = pltpu.make_async_remote_copy(
            src_ref=send_ref.at[peer],
            dst_ref=recv_ref.at[place],
            send_sem=send_sems.at[step - 1],
            recv_sem=recv_sems.at[step - 1],
            device_id={axis: peer},
            device_id_type=pl.DeviceIdType.MESH,
        )
        copy.start()
        copies.append(copy)
    own.wait()
    for copy in copies:
        copy.wait()


def exchange(blocks, axis, collective_id):
    count = lax.axis_size(axis)
    grouped = blocks.reshape((count, -1) + blocks.shape[2:])
    out = pl.pallas_call(
        functools.partial(exchange_kernel, axis=axis, count=count),
        out_shape=jax.ShapeDtypeStruct(grouped.shape, grouped.dtype),
        in_specs=[pl.BlockSpec(memory_space=pl.ANY)],
        out_specs=pl.BlockSpec(memory_space=pl.ANY),
        scratch_shapes=[
            pltpu.SemaphoreType.DMA((count - 1,)),
            pltpu.SemaphoreType.DMA((count - 1,)),
            pltpu.SemaphoreType.DMA(()),
        ],
        compiler_params=pltpu.CompilerParams(collective_id=collective_id, has_side_effects=True),
        name="exchange",
    )(grouped)
    return out.reshape(blocks.shape)


def run_experts(arrived, w_gate, w_up, w_down, sources):
    local_count = w_gate.shape[0]
    grouped = arrived.reshape(sources, local_count, arrived.shape[1], arrived.shape[2])
    gate_pre = jnp.einsum("pesd,edf->pesf", grouped, w_gate, preferred_element_type=jnp.float32)
    up_pre = jnp.einsum("pesd,edf->pesf", grouped, w_up, preferred_element_type=jnp.float32)
    active = (jax.nn.silu(gate_pre) * up_pre).astype(jnp.bfloat16)
    result = jnp.einsum(
        "pesf,efd->pesd", active, w_down, preferred_element_type=jnp.float32
    ).astype(jnp.bfloat16)
    return result.reshape(arrived.shape)


def line_kernel(
    rows_ref,
    mix_ref,
    info_ref,
    gate_hbm,
    up_hbm,
    down_hbm,
    out_ref,
    gate_ref,
    up_ref,
    down_ref,
    infos_ref,
    held_ref,
    cross_ref,
    crossed_ref,
    answer_ref,
    done_ref,
    batch_ref,
    part_ref,
    own_ref,
    sum_ref,
    load_sems,
    info_send,
    info_recv,
    row_send,
    row_recv,
    cross_send,
    cross_recv,
    answer_send,
    answer_recv,
    sum_send,
    sum_recv,
    *,
    line,
    halves,
    slots,
    pieces,
):
    place = lax.axis_index("sp")
    here = place // 2
    side = lax.rem(place, 2)
    twin = place + 1 - 2 * side
    units = line * halves
    tokens = rows_ref.shape[1]
    grain = tokens // pieces
    last = line - 1

    def remote(src, dst, send, recv, peer):
        return pltpu.make_async_remote_copy(
            src_ref=src,
            dst_ref=dst,
            send_sem=send,
            recv_sem=recv,
            device_id={"sp": peer},
            device_id_type=pl.DeviceIdType.MESH,
        )

    loads = [
        pltpu.make_async_copy(src, dst, load_sems.at[i])
        for i, (src, dst) in enumerate(
            [(gate_hbm, gate_ref), (up_hbm, up_ref), (down_hbm, down_ref)]
        )
    ]
    for load in loads:
        load.start()

    barrier = pltpu.get_barrier_semaphore()
    for step in range(1, line):
        pl.semaphore_signal(
            barrier,
            inc=1,
            device_id={"sp": lax.rem(here + step, line) * 2 + side},
            device_id_type=pl.DeviceIdType.MESH,
        )
    pl.semaphore_signal(
        barrier, inc=1, device_id={"sp": twin}, device_id_type=pl.DeviceIdType.MESH
    )
    pl.semaphore_wait(barrier, line)

    def info_copy(step):
        peer = lax.rem(here + step, line)
        return remote(
            info_ref,
            infos_ref.at[here],
            info_send.at[step - 1],
            info_recv.at[step - 1],
            peer * 2 + side,
        )

    def row_copy(src, source, half, way):
        unit = source * halves + half
        return remote(
            src,
            held_ref.at[unit],
            row_send.at[way, unit],
            row_recv.at[unit],
            place + (4 * way - 2),
        )

    def cross_copy(unit):
        return remote(
            cross_ref.at[unit],
            crossed_ref.at[unit],
            cross_send.at[unit],
            cross_recv.at[unit],
            twin,
        )

    def answer_copy(unit):
        return remote(
            answer_ref.at[unit],
            done_ref.at[unit, pl.ds(slots, slots)],
            answer_send.at[unit],
            answer_recv.at[unit],
            twin,
        )

    def sum_copy(target, half, way, piece):
        landing = ((target + way) * halves + half) * pieces + piece
        leaving = (target * halves + half) * pieces + piece
        return remote(
            part_ref.at[leaving],
            sum_ref.at[landing],
            sum_send.at[leaving],
            sum_recv.at[landing],
            place + (4 * way - 2),
        )

    def sum_wait(landing):
        remote(
            part_ref.at[0], sum_ref.at[landing], sum_send.at[0], sum_recv.at[landing], twin
        ).wait_recv()

    for step in range(1, line):
        info_copy(step).start()
    for way in range(2):

        @pl.when((here < last) if way else (here > 0))
        def _():
            row_copy(rows_ref.at[0], here, 0, way).start()

    def later_halves(way):
        for half in range(1, halves):
            row_copy(rows_ref.at[half], here, half, way).start()

    @pl.when(here == 0)
    def _():
        later_halves(1)

    @pl.when(here == last)
    def _():
        later_halves(0)

    infos_ref[here] = info_ref[...]
    for half in range(halves):
        held_ref[here * halves + half] = rows_ref[half]
    batch_ref[...] = jnp.zeros_like(batch_ref)
    for step in range(1, line):
        info_copy(step).wait()

    shorter = jnp.minimum(here, last - here)

    def in_stream(p, reach):
        first = p < reach
        turn = p - reach
        ahead = jnp.where(first, p + 1, reach - turn // (halves - 1))
        return ahead, jnp.where(first, 0, 1 + lax.rem(turn, halves - 1))

    def source_of(k):
        p = k - halves
        both = shorter * 2 * halves
        paired = p < both
        way = jnp.where(paired, lax.rem(p, 2), jnp.where(here < last - here, 1, 0))
        spot = jnp.where(paired, p // 2, p - shorter * halves)
        reach = jnp.where(way == 1, last - here, here)
        ahead, half = in_stream(spot, reach)
        is_own = k < halves
        final = spot == reach * halves - 1
        return (
            jnp.where(is_own, here, here + ahead * (2 * way - 1)),
            jnp.where(is_own, k, half),
            final,
        )

    def matches(source, half, weighted):
        info = infos_ref[source, half]
        rank = lax.broadcasted_iota(jnp.int32, (slots, tokens), 0).astype(jnp.float32)
        tables = []
        for expert in (place, twin):
            name = expert.astype(jnp.float32)
            table = jnp.zeros((slots, tokens), jnp.float32)
            for route in range(2):
                hit = jnp.where(info[route : route + 1] == name, info[2 + route : 3 + route], -1.0)
                value = info[4 + route : 5 + route] if weighted else 1.0
                table += jnp.where(hit == rank, value, 0.0)
            tables.append(table)
        return jnp.concatenate(tables, axis=0)

    first_way = jnp.where(last - here <= here, 0, 1)

    def relay(way, spot):
        reach = jnp.where(way == 1, last - here, here)

        @pl.when((spot >= 0) & (spot < reach * halves) & (here > 0) & (here < last))
        def _():
            ahead, half = in_stream(spot, reach)
            target = here + ahead * (2 * way - 1)
            for piece in range(pieces):
                unit = (target * halves + half) * pieces + piece
                landing = ((target + way) * halves + half) * pieces + piece
                sum_wait(landing)
                part_ref[unit] = (
                    part_ref[unit].astype(jnp.float32) + sum_ref[landing].astype(jnp.float32)
                ).astype(jnp.bfloat16)
                sum_copy(target, half, way, piece).start()

    def step_body(k, carry):
        @pl.when(k < units)
        def _():
            source, half, final = source_of(k)
            unit = source * halves + half

            @pl.when(source != here)
            def _():
                remote(
                    held_ref.at[unit], held_ref.at[unit], row_send.at[0, unit], row_recv.at[unit], twin
                ).wait_recv()

            @pl.when((source < here) & (here < last))
            def _():
                row_copy(held_ref.at[unit], source, half, 1).start()

                @pl.when(final)
                def _():
                    later_halves(1)

            @pl.when((source > here) & (here > 0))
            def _():
                row_copy(held_ref.at[unit], source, half, 0).start()

                @pl.when(final)
                def _():
                    later_halves(0)

            packed = jnp.dot(
                matches(source, half, False).astype(jnp.bfloat16),
                held_ref[unit],
                preferred_element_type=jnp.float32,
            ).astype(jnp.bfloat16)
            cross_ref[unit] = packed[slots:]
            cross_copy(unit).start()
            batch_ref[0:slots, :] = packed[:slots]

        @pl.when(k == 0)
        def _():
            for load in loads:
                load.wait()

        relay(first_way, k - units)

        @pl.when((k > 0) & (k <= units))
        def _():
            source, half, _ = source_of(k - 1)
            unit = source * halves + half
            cross_copy(unit).wait_recv()
            batch_ref[slots : 2 * slots, :] = crossed_ref[unit]

        @pl.when(k <= units)
        def _():
            rows = batch_ref[...]
            gate = jnp.dot(rows, gate_ref[0], preferred_element_type=jnp.float32)
            up = jnp.dot(rows, up_ref[0], preferred_element_type=jnp.float32)
            active = (jax.nn.silu(gate) * up).astype(jnp.bfloat16)
            batch_ref[...] = jnp.dot(
                active, down_ref[0], preferred_element_type=jnp.float32
            ).astype(jnp.bfloat16)

        @pl.when(k < units)
        def _():
            source, half, _ = source_of(k)
            done_ref[source * halves + half, 0:slots, :] = batch_ref[0:slots, :]

        @pl.when((k > 0) & (k <= units))
        def _():
            source, half, _ = source_of(k - 1)
            unit = source * halves + half
            answer_ref[unit] = batch_ref[slots : 2 * slots, :]

            @pl.when(source != here)
            def _():
                answer_copy(unit).start()

        @pl.when(k == units)
        def _():
            for half in range(halves):
                answer_copy(here * halves + half).start()

        relay(1 - first_way, k - units - 2)

        @pl.when(k > 1 + halves)
        def _():
            source, half, _ = source_of(jnp.where(k > units + 1, k - units - 2, k - 2))
            unit = source * halves + half
            answer_copy(unit).wait_recv()
            high, low = split_two(matches(source, half, True))
            answers = done_ref[unit]
            turned = (((0,), (0,)), ((), ()))
            part = lax.dot_general(
                high, answers, turned, preferred_element_type=jnp.float32
            ) + lax.dot_general(low, answers, turned, preferred_element_type=jnp.float32)

            @pl.when(source == here)
            def _():
                own_ref[half] = part

            @pl.when(source != here)
            def _():
                for piece in range(pieces):
                    part_ref[unit * pieces + piece] = part[
                        piece * grain : (piece + 1) * grain
                    ].astype(jnp.bfloat16)

            @pl.when((source < here) & (here == last))
            def _():
                for piece in range(pieces):
                    sum_copy(source, half, 0, piece).start()

            @pl.when((source > here) & (here == 0))
            def _():
                for piece in range(pieces):
                    sum_copy(source, half, 1, piece).start()

        return carry

    lax.fori_loop(0, units + 2 + halves, step_body, 0)

    for half in range(halves):
        for piece in range(pieces):
            rows = pl.ds(piece * grain, grain)
            own_ref[half, rows] = own_ref[half, rows] + mix_ref[half, rows]
            for way in range(2):

                @pl.when((here > 0) if way else (here < last))
                def _():
                    landing = ((here + way) * halves + half) * pieces + piece
                    sum_wait(landing)
                    own_ref[half, rows] = own_ref[half, rows] + sum_ref[landing].astype(jnp.float32)

            out_ref[half, rows] = own_ref[half, rows].astype(out_ref.dtype)

    def drain(unit, carry):
        source = unit // halves
        half = lax.rem(unit, halves)
        cross_copy(unit).wait_send()
        answer_copy(unit).wait_send()

        @pl.when((source <= here) & (here < last))
        def _():
            row_copy(held_ref.at[unit], source, half, 1).wait_send()

        @pl.when((source >= here) & (here > 0))
        def _():
            row_copy(held_ref.at[unit], source, half, 0).wait_send()

        @pl.when(source != here)
        def _():
            for piece in range(pieces):
                sum_copy(source, half, 0, piece).wait_send()

        return carry

    lax.fori_loop(0, units, drain, 0)


def run_line(normed_rows, after_mix, info, w_gate, w_up, w_down, slots):
    count = lax.axis_size("sp")
    line, halves = count // 2, info.shape[0]
    units = line * halves
    row_count, width = normed_rows.shape
    tokens = row_count // halves
    pieces = 2
    grain = tokens // pieces
    vmem = pl.BlockSpec(memory_space=pltpu.VMEM)
    whole = pl.BlockSpec(memory_space=pl.ANY)
    dma = pltpu.SemaphoreType.DMA
    out = pl.pallas_call(
        functools.partial(line_kernel, line=line, halves=halves, slots=slots, pieces=pieces),
        out_shape=jax.ShapeDtypeStruct((halves, tokens, width), jnp.bfloat16),
        in_specs=[vmem, vmem, vmem, whole, whole, whole],
        out_specs=vmem,
        scratch_shapes=[
            pltpu.VMEM(w_gate.shape, jnp.bfloat16),
            pltpu.VMEM(w_up.shape, jnp.bfloat16),
            pltpu.VMEM(w_down.shape, jnp.bfloat16),
            pltpu.VMEM((line,) + info.shape, jnp.float32),
            pltpu.VMEM((units, tokens, width), jnp.bfloat16),
            pltpu.VMEM((units, slots, width), jnp.bfloat16),
            pltpu.VMEM((units, slots, width), jnp.bfloat16),
            pltpu.VMEM((units, slots, width), jnp.bfloat16),
            pltpu.VMEM((units, 2 * slots, width), jnp.bfloat16),
            pltpu.VMEM((2 * slots, width), jnp.bfloat16),
            pltpu.VMEM((units * pieces, grain, width), jnp.bfloat16),
            pltpu.VMEM((halves, tokens, width), jnp.float32),
            pltpu.VMEM(((units + halves) * pieces, grain, width), jnp.bfloat16),
            dma((3,)),
            dma((line - 1,)),
            dma((line - 1,)),
            dma((2, units)),
            dma((units,)),
            dma((units,)),
            dma((units,)),
            dma((units,)),
            dma((units,)),
            dma((units * pieces,)),
            dma(((units + halves) * pieces,)),
        ],
        compiler_params=pltpu.CompilerParams(
            vmem_limit_bytes=VMEM_LIMIT, collective_id=4, has_side_effects=True
        ),
        cost_estimate=pl.CostEstimate(flops=10**10, bytes_accessed=2**23, transcendentals=0),
        name="experts",
    )(
        normed_rows.reshape(halves, tokens, width),
        after_mix.reshape(halves, tokens, width),
        info,
        w_gate,
        w_up,
        w_down,
    )
    return out.reshape(row_count, width)


def route_info(routes, route_weight, halves):
    tokens = routes.shape[0] // halves
    ids = routes.reshape(halves, -1)
    order = jnp.arange(ids.shape[1], dtype=jnp.int32)
    same = (ids[:, :, None] == ids[:, None, :]) & (order[None, None, :] < order[None, :, None])
    rank = jnp.sum(same.astype(jnp.float32), axis=2)

    def turned(a):
        return a.astype(jnp.float32).reshape(halves, tokens, -1).transpose(0, 2, 1)

    return jnp.concatenate(
        [turned(routes), turned(rank), turned(route_weight), jnp.zeros((halves, 2, tokens), jnp.float32)],
        axis=1,
    )


def shards(
    resid,
    query,
    keys,
    values,
    out_gate,
    forget_pre,
    input_pre,
    head_gain,
    out_proj,
    ffn_gain,
    routes,
    route_scores,
    w_gate,
    w_up,
    w_down,
):
    head_width = query.shape[1]
    row_count, route_count = routes.shape
    sources = lax.axis_size("sp")
    local_experts = w_gate.shape[0]
    expert_count = local_experts * sources
    half_rows = row_count // 2
    capacity = max(2, 2 * half_rows * route_count // expert_count)
    dense = local_experts == 1 and sources % 2 == 0 and sources <= 8 and route_count == 2
    dense = dense and 2 * capacity >= half_rows and capacity % 16 == 0 and half_rows % 32 == 0
    if dense and lax.axis_size("tp") == 4 and head_width % (8 * sources) == 0:
        return run_layer(
            resid,
            query,
            keys,
            values,
            out_gate,
            forget_pre,
            input_pre,
            head_gain,
            out_proj,
            ffn_gain,
            routes,
            route_scores,
            w_gate,
            w_up,
            w_down,
            2,
            capacity,
        )
    route_weight = route_scores / jnp.sum(route_scores, axis=1, keepdims=True)
    token_rows = token_cell(query, keys, values, forget_pre, input_pre)
    cell_float = token_rows.astype(jnp.float32)
    headed = (
        cell_float
        * lax.rsqrt(jnp.mean(cell_float * cell_float, axis=1, keepdims=True) + EPS)
        * head_gain[None, :]
    )
    gated_out = (headed * jax.nn.sigmoid(out_gate.astype(jnp.float32))).astype(jnp.bfloat16)
    after_mix = resid.astype(jnp.float32) + jnp.dot(
        gated_out, out_proj, preferred_element_type=jnp.float32
    )
    normed_rows = (
        after_mix
        * lax.rsqrt(jnp.mean(after_mix * after_mix, axis=1, keepdims=True) + EPS)
        * ffn_gain[None, :]
    ).astype(jnp.bfloat16)
    if dense:
        info = route_info(routes, route_weight, 2)
        return run_line(normed_rows, after_mix, info, w_gate, w_up, w_down, capacity)
    selects = [
        slot_select(
            routes[half_idx * half_rows : (half_idx + 1) * half_rows], expert_count, capacity
        )
        for half_idx in range(2)
    ]

    def pack_rows(half_idx):
        selection = (
            selects[half_idx].reshape(expert_count * capacity, half_rows, route_count).sum(axis=2)
        )
        packed = jnp.dot(
            selection,
            normed_rows[half_idx * half_rows : (half_idx + 1) * half_rows],
            preferred_element_type=jnp.float32,
        )
        return packed.astype(jnp.bfloat16).reshape(expert_count, capacity, normed_rows.shape[1])

    send_rows = jnp.concatenate([pack_rows(0), pack_rows(1)], axis=1)
    finished = run_experts(
        exchange(send_rows, "sp", 1),
        w_gate,
        w_up,
        w_down,
        sources,
    )
    returned = exchange(finished, "sp", 2)
    answers = [returned[:, :capacity], returned[:, capacity:]]
    pieces = []
    for half_idx in range(2):
        gathered = lax.dot_general(
            selects[half_idx],
            answers[half_idx].reshape(expert_count * capacity, -1),
            (((0,), (0,)), ((), ())),
            preferred_element_type=jnp.float32,
        )
        weights_half = route_weight[half_idx * half_rows : (half_idx + 1) * half_rows]
        pieces.append(
            jnp.sum(gathered.reshape(half_rows, route_count, -1) * weights_half[:, :, None], axis=1)
        )
    return (after_mix + jnp.concatenate(pieces, axis=0)).astype(jnp.bfloat16)


def solution(mesh):
    placed = (
        P(("sp", "tp"), None),
        P("sp", "tp"),
        P("sp", "tp"),
        P("sp", "tp"),
        P(("sp", "tp"), None),
        P("tp", "sp"),
        P("tp", "sp"),
        P(),
        P(),
        P(),
        P(("sp", "tp"), None),
        P(("sp", "tp"), None),
        P("sp", None, None),
        P("sp", None, None),
        P("sp", None, None),
    )
    return jax.shard_map(
        shards, mesh=mesh, in_specs=placed, out_specs=P(("sp", "tp"), None), check_vma=False
    )
```

```python
import functools

import jax
import jax.numpy as jnp
from jax import lax
from jax.experimental import pallas as pl
from jax.experimental.pallas import tpu as pltpu
from jax.sharding import PartitionSpec as P

BLOCK = 64


EPS = 1e-06
FLOOR_LOG = -1e30
HIGHEST = lax.Precision.HIGHEST


EXTRA = 8
VMEM_LIMIT = 56 * 1024 * 1024
LAYER_VMEM = 60 * 1024 * 1024
WEIGHT_PIECES = 4


def col_mask(first_row, rows, cols):
    row = lax.broadcasted_iota(jnp.int32, (rows, cols), 0) + first_row
    col = lax.broadcasted_iota(jnp.int32, (rows, cols), 1)
    return row, col


def split_two(a):
    high = a.astype(jnp.bfloat16)
    return high, (a - high.astype(jnp.float32)).astype(jnp.bfloat16)


def log_rows(forget_ref, input_ref):
    pre = forget_ref[...]
    log_forget = jnp.minimum(pre, 0.0) - jnp.log1p(jnp.exp(-jnp.abs(pre)))
    seq_len = pre.shape[1]
    row, col = col_mask(0, seq_len, seq_len)
    upper = jnp.where(row <= col, 1.0, 0.0).astype(jnp.bfloat16)
    one, rest = split_two(log_forget)
    two, three = split_two(log_forget - one.astype(jnp.float32))
    stacked = jnp.concatenate([one, two, three, jnp.zeros((13, seq_len), jnp.bfloat16)], axis=0)
    sums = jnp.dot(stacked, upper, preferred_element_type=jnp.float32)
    cum_row = sums[0:1] + sums[1:2] + sums[2:3]
    return log_forget, cum_row, input_ref[...] - cum_row


def cell_state_kernel(k_ref, v_ref, forget_ref, input_ref, state_ref):
    width = k_ref.shape[1]
    seq_len = k_ref.shape[0]
    log_forget, cum_row, gap_row = log_rows(forget_ref, input_ref)
    total = jnp.sum(log_forget, axis=1, keepdims=True)
    top = jnp.max(gap_row, axis=1, keepdims=True)
    keep_row = jnp.exp(gap_row - top) * width ** (-0.5)
    k_turned = k_ref[...].astype(jnp.float32).T
    weighted = k_turned * keep_row
    high, low = split_two(weighted)
    v = v_ref[...]
    state_ref[0:width, :] = jnp.dot(high, v, preferred_element_type=jnp.float32) + jnp.dot(
        low, v, preferred_element_type=jnp.float32
    )
    vector = jnp.dot(
        jnp.broadcast_to(keep_row, (8, seq_len)),
        k_ref[...].astype(jnp.float32),
        precision=HIGHEST,
        preferred_element_type=jnp.float32,
    )[0:1]
    lanes = jnp.zeros((1, width), jnp.float32)
    state_ref[width : width + EXTRA, :] = jnp.concatenate(
        [vector, lanes + total, lanes + total + top, jnp.zeros((EXTRA - 3, width), jnp.float32)],
        axis=0,
    )


def cell_local_kernel(q_ref, k_ref, v_ref, forget_ref, input_ref, num_ref, aux_ref, *, tile):
    seq_len, width = q_ref.shape
    log_forget, cum_row, gap_row = log_rows(forget_ref, input_ref)
    for first in range(0, seq_len, tile):
        span = first + tile
        row, col = col_mask(first, tile, span)
        causal = col <= row
        own = (col // BLOCK) == (row // BLOCK)
        gap = jnp.where(causal, gap_row[:, :span], -jnp.inf)
        top = jnp.max(gap, axis=1, keepdims=True)
        cum = jnp.sum(jnp.where(causal, log_forget[:, :span], 0.0), axis=1, keepdims=True)
        scores = lax.dot_general(
            q_ref[first:span, :],
            k_ref[0:span, :],
            (((1,), (1,)), ((), ())),
            preferred_element_type=jnp.float32,
        ) * width ** (-0.5)
        weights = scores * jnp.exp(gap - top)
        high = weights.astype(jnp.bfloat16)
        high_float = high.astype(jnp.float32)
        low_float = jnp.where(own, 0.0, weights - high_float)
        v = v_ref[0:span, :]
        num_ref[first:span, :] = jnp.dot(high, v, preferred_element_type=jnp.float32) + jnp.dot(
            low_float.astype(jnp.bfloat16), v, preferred_element_type=jnp.float32
        )
        den = jnp.sum(high_float + low_float, axis=1, keepdims=True)
        lane = lax.broadcasted_iota(jnp.int32, (tile, 128), 1)
        aux_ref[first:span, :] = jnp.where(lane == 0, den, jnp.where(lane == 1, top, cum))


def cell_join_kernel(q_ref, num_ref, aux_ref, states_ref, rows_ref, mat_ref, *, axis):
    width = q_ref.shape[1]
    place = lax.axis_index(axis)
    mat_ref[...] = jnp.zeros_like(mat_ref)

    def join(step, carry):
        vector, old_max = carry
        extra = states_ref[step, width : width + EXTRA, :]
        new_max, total = extra[2:3], extra[1:2]
        joined = jnp.maximum(total + old_max, new_max)
        keep_old = jnp.exp(total + old_max - joined)
        keep_new = jnp.exp(new_max - joined)
        mat_ref[...] = keep_old * mat_ref[...] + keep_new * states_ref[step, 0:width, :]
        return keep_old * vector + keep_new * extra[0:1], joined

    vector, far_max = lax.fori_loop(
        0,
        place,
        join,
        (jnp.zeros((1, width), jnp.float32), jnp.full((1, width), FLOOR_LOG, jnp.float32)),
    )
    aux = aux_ref[...]
    den, top, cum = aux[:, 0:1], aux[:, 1:2], aux[:, 2:3]
    far = far_max[:, 0:1]
    joined = jnp.maximum(top, far)
    keep_own = jnp.exp(top - joined)
    keep_far = jnp.exp(far - joined)
    q_float = q_ref[...].astype(jnp.float32)
    one, rest = split_two(mat_ref[...])
    two, three = split_two(mat_ref[...] - one.astype(jnp.float32))
    q = q_ref[...]
    far_num = (
        jnp.dot(q, one, preferred_element_type=jnp.float32)
        + jnp.dot(q, two, preferred_element_type=jnp.float32)
        + jnp.dot(q, three, preferred_element_type=jnp.float32)
    )
    far_den = jnp.sum(q_float * vector, axis=1, keepdims=True)
    numerator = keep_own * num_ref[...] + keep_far * far_num
    denominator = keep_own * den + keep_far * far_den
    divisor = jnp.maximum(jnp.abs(denominator), jnp.exp(-(cum + joined)))
    rows_ref[...] = (numerator / divisor).astype(rows_ref.dtype)


def run_cell(query, keys, values, forget_pre, input_pre):
    seq_len, width = query.shape
    params = pltpu.CompilerParams(vmem_limit_bytes=VMEM_LIMIT)
    state = pl.pallas_call(
        cell_state_kernel,
        out_shape=jax.ShapeDtypeStruct((width + EXTRA, width), jnp.float32),
        compiler_params=params,
        cost_estimate=pl.CostEstimate(flops=10**9, bytes_accessed=2**20, transcendentals=0),
        name="cell_state",
    )(keys, values, forget_pre, input_pre)
    cut = (width + EXTRA) // 3
    parts = [lax.all_gather(state[i * cut : (i + 1) * cut], "sp") for i in range(3)]
    gathered = jnp.concatenate(parts, axis=1)
    tile = 4 * BLOCK if seq_len % (4 * BLOCK) == 0 else BLOCK
    numerator, aux = pl.pallas_call(
        functools.partial(cell_local_kernel, tile=tile),
        out_shape=(
            jax.ShapeDtypeStruct((seq_len, width), jnp.float32),
            jax.ShapeDtypeStruct((seq_len, 128), jnp.float32),
        ),
        compiler_params=params,
        cost_estimate=pl.CostEstimate(flops=5 * 10**9, bytes_accessed=2**21, transcendentals=0),
        name="cell_local",
    )(query, keys, values, forget_pre, input_pre)
    rows = pl.pallas_call(
        functools.partial(cell_join_kernel, axis="sp"),
        out_shape=jax.ShapeDtypeStruct((seq_len, width), jnp.bfloat16),
        scratch_shapes=[pltpu.VMEM((width, width), jnp.float32)],
        compiler_params=params,
        name="cell_join",
    )(query, numerator, aux, gathered)
    return rows


def sp_tp_barrier(barrier, counts):
    total = 0
    for axis, count in counts.items():
        place = lax.axis_index(axis)
        for step in range(1, count):
            pl.semaphore_signal(
                barrier,
                inc=1,
                device_id={axis: lax.rem(place + step, count)},
                device_id_type=pl.DeviceIdType.MESH,
            )
        total += count - 1
    return total


def cell_kernel(
    q_ref,
    k_ref,
    v_ref,
    forget_ref,
    input_ref,
    out_ref,
    state_ref,
    piece_ref,
    extra_ref,
    prefix_ref,
    mat_ref,
    num_ref,
    aux_ref,
    rows_ref,
    send_sems,
    recv_sems,
    extra_send_sems,
    extra_recv_sems,
    back_send_sems,
    back_recv_sems,
    turn_send_sems,
    turn_recv_sems,
    own_sem,
    *,
    count,
    heads,
    tile,
):
    seq_len, width = q_ref.shape
    cut = width // count
    place = lax.axis_index("sp")
    head = lax.axis_index("tp")
    barrier = pltpu.get_barrier_semaphore()
    greeted = sp_tp_barrier(barrier, {"sp": count, "tp": heads})
    log_forget, cum_row, gap_row = log_rows(forget_ref, input_ref)
    total = jnp.sum(log_forget, axis=1, keepdims=True)
    best = jnp.max(gap_row, axis=1, keepdims=True)
    keep_row = jnp.exp(gap_row - best) * width ** (-0.5)
    weighted = k_ref[...].astype(jnp.float32).T * keep_row
    high, low = split_two(weighted)
    v_all = v_ref[...]
    state_ref[0:width, :] = jnp.dot(high, v_all, preferred_element_type=jnp.float32) + jnp.dot(
        low, v_all, preferred_element_type=jnp.float32
    )
    vector = jnp.dot(
        jnp.broadcast_to(keep_row, (8, seq_len)),
        k_ref[...].astype(jnp.float32),
        precision=HIGHEST,
        preferred_element_type=jnp.float32,
    )[0:1]
    lanes = jnp.zeros((1, width), jnp.float32)
    state_ref[width : width + EXTRA, :] = jnp.concatenate(
        [vector, lanes + total, lanes + total + best, jnp.zeros((EXTRA - 3, width), jnp.float32)],
        axis=0,
    )
    pl.semaphore_wait(barrier, greeted)
    sends = []
    for step in range(1, count):
        peer = lax.rem(place + step, count)
        extra_copy = pltpu.make_async_remote_copy(
            src_ref=state_ref.at[pl.ds(width, EXTRA)],
            dst_ref=extra_ref.at[place],
            send_sem=extra_send_sems.at[step - 1],
            recv_sem=extra_recv_sems.at[step - 1],
            device_id={"sp": peer},
            device_id_type=pl.DeviceIdType.MESH,
        )
        piece_copy = pltpu.make_async_remote_copy(
            src_ref=state_ref.at[pl.ds(pl.multiple_of(peer * cut, cut), cut)],
            dst_ref=piece_ref.at[place],
            send_sem=send_sems.at[step - 1],
            recv_sem=recv_sems.at[step - 1],
            device_id={"sp": peer},
            device_id_type=pl.DeviceIdType.MESH,
        )
        extra_copy.start()
        piece_copy.start()
        sends += [extra_copy, piece_copy]
    extra_ref[place] = state_ref[width : width + EXTRA, :]
    piece_ref[place] = state_ref[pl.ds(pl.multiple_of(place * cut, cut), cut), :]

    for first in range(0, seq_len, tile):
        span = first + tile
        row, col = col_mask(first, tile, span)
        causal = col <= row
        own = (col // BLOCK) == (row // BLOCK)
        gap = jnp.where(causal, gap_row[:, :span], -jnp.inf)
        top = jnp.max(gap, axis=1, keepdims=True)
        cum = jnp.sum(jnp.where(causal, log_forget[:, :span], 0.0), axis=1, keepdims=True)
        scores = lax.dot_general(
            q_ref[first:span, :],
            k_ref[0:span, :],
            (((1,), (1,)), ((), ())),
            preferred_element_type=jnp.float32,
        ) * width ** (-0.5)
        weights = scores * jnp.exp(gap - top)
        high = weights.astype(jnp.bfloat16)
        high_float = high.astype(jnp.float32)
        low_float = jnp.where(own, 0.0, weights - high_float)
        v = v_ref[0:span, :]
        num_ref[first:span, :] = jnp.dot(high, v, preferred_element_type=jnp.float32) + jnp.dot(
            low_float.astype(jnp.bfloat16), v, preferred_element_type=jnp.float32
        )
        den = jnp.sum(high_float + low_float, axis=1, keepdims=True)
        lane = lax.broadcasted_iota(jnp.int32, (tile, 128), 1)
        aux_ref[first:span, :] = jnp.where(lane == 0, den, jnp.where(lane == 1, top, cum))

    for copy in sends:
        copy.wait()

    running = jnp.zeros((cut, width), jnp.float32)
    vector = jnp.zeros((1, width), jnp.float32)
    far_max = jnp.full((1, width), FLOOR_LOG, jnp.float32)
    own_vector, own_max = vector, far_max
    for step in range(count):
        prefix_ref[step] = running
        own_vector = jnp.where(place == step, vector, own_vector)
        own_max = jnp.where(place == step, far_max, own_max)
        if step < count - 1:
            extra = extra_ref[step]
            new_max, step_total = extra[2:3], extra[1:2]
            joined = jnp.maximum(step_total + far_max, new_max)
            keep_old = jnp.exp(step_total + far_max - joined)
            keep_new = jnp.exp(new_max - joined)
            running = keep_old * running + keep_new * piece_ref[step]
            vector = keep_old * vector + keep_new * extra[0:1]
            far_max = joined
    backs = []
    for step in range(1, count):
        peer = lax.rem(place + step, count)
        back = pltpu.make_async_remote_copy(
            src_ref=prefix_ref.at[peer],
            dst_ref=mat_ref.at[pl.ds(pl.multiple_of(place * cut, cut), cut)],
            send_sem=back_send_sems.at[step - 1],
            recv_sem=back_recv_sems.at[step - 1],
            device_id={"sp": peer},
            device_id_type=pl.DeviceIdType.MESH,
        )
        back.start()
        backs.append(back)
    mat_ref[pl.ds(pl.multiple_of(place * cut, cut), cut), :] = prefix_ref[place]

    aux = aux_ref[...]
    den, top, cum = aux[:, 0:1], aux[:, 1:2], aux[:, 2:3]
    far = own_max[:, 0:1]
    joined = jnp.maximum(top, far)
    keep_own = jnp.exp(top - joined)
    keep_far = jnp.exp(far - joined)
    q_float = q_ref[...].astype(jnp.float32)
    far_den = jnp.sum(q_float * own_vector, axis=1, keepdims=True)
    denominator = keep_own * den + keep_far * far_den
    divisor = jnp.maximum(jnp.abs(denominator), jnp.exp(-(cum + joined)))
    for copy in backs:
        copy.wait()
    one, rest = split_two(mat_ref[...])
    two, three = split_two(mat_ref[...] - one.astype(jnp.float32))
    q = q_ref[...]
    far_num = (
        jnp.dot(q, one, preferred_element_type=jnp.float32)
        + jnp.dot(q, two, preferred_element_type=jnp.float32)
        + jnp.dot(q, three, preferred_element_type=jnp.float32)
    )
    numerator = keep_own * num_ref[...] + keep_far * far_num
    rows_ref[...] = (numerator / divisor).astype(rows_ref.dtype)

    share = seq_len // heads
    columns = pl.ds(pl.multiple_of(head * width, width), width)
    turns = []
    for step in range(1, heads):
        peer = lax.rem(head + step, heads)
        turn = pltpu.make_async_remote_copy(
            src_ref=rows_ref.at[pl.ds(pl.multiple_of(peer * share, share), share)],
            dst_ref=out_ref.at[:, columns],
            send_sem=turn_send_sems.at[step - 1],
            recv_sem=turn_recv_sems.at[step - 1],
            device_id={"tp": peer},
            device_id_type=pl.DeviceIdType.MESH,
        )
        turn.start()
        turns.append(turn)
    own_copy = pltpu.make_async_copy(
        rows_ref.at[pl.ds(pl.multiple_of(head * share, share), share)],
        out_ref.at[:, columns],
        own_sem,
    )
    own_copy.start()
    own_copy.wait()
    for turn in turns:
        turn.wait()


def run_cell_scan(query, keys, values, forget_pre, input_pre):
    seq_len, width = query.shape
    count, heads = lax.axis_size("sp"), lax.axis_size("tp")
    tile = 4 * BLOCK if seq_len % (4 * BLOCK) == 0 else BLOCK
    cut = width // count
    vmem = pl.BlockSpec(memory_space=pltpu.VMEM)
    dma = pltpu.SemaphoreType.DMA
    return pl.pallas_call(
        functools.partial(cell_kernel, count=count, heads=heads, tile=tile),
        out_shape=jax.ShapeDtypeStruct((seq_len // heads, heads * width), jnp.bfloat16),
        in_specs=[vmem] * 5,
        out_specs=vmem,
        scratch_shapes=[
            pltpu.VMEM((width + EXTRA, width), jnp.float32),
            pltpu.VMEM((count, cut, width), jnp.float32),
            pltpu.VMEM((count, EXTRA, width), jnp.float32),
            pltpu.VMEM((count, cut, width), jnp.float32),
            pltpu.VMEM((width, width), jnp.float32),
            pltpu.VMEM((seq_len, width), jnp.float32),
            pltpu.VMEM((seq_len, 128), jnp.float32),
            pltpu.VMEM((seq_len, width), jnp.bfloat16),
            dma((count - 1,)),
            dma((count - 1,)),
            dma((count - 1,)),
            dma((count - 1,)),
            dma((count - 1,)),
            dma((count - 1,)),
            dma((heads - 1,)),
            dma((heads - 1,)),
            dma(()),
        ],
        compiler_params=pltpu.CompilerParams(
            vmem_limit_bytes=VMEM_LIMIT, collective_id=3, has_side_effects=True
        ),
        cost_estimate=pl.CostEstimate(flops=10**10, bytes_accessed=2**21, transcendentals=0),
        name="cell",
    )(query, keys, values, forget_pre, input_pre)


def token_cell(query, keys, values, forget_pre, input_pre):
    if query.shape[1] % (8 * lax.axis_size("sp")) == 0:
        return run_cell_scan(query, keys, values, forget_pre, input_pre)
    rows = run_cell(query, keys, values, forget_pre, input_pre)
    return lax.all_to_all(rows, "tp", split_axis=0, concat_axis=1, tiled=True)


def layer_kernel(
    q_ref,
    k_ref,
    v_ref,
    forget_ref,
    input_ref,
    head_gain_ref,
    ffn_gain_ref,
    routes_ref,
    scores_ref,
    resid_hbm,
    out_gate_hbm,
    out_proj_hbm,
    gate_hbm,
    up_hbm,
    down_hbm,
    out_ref,
    state_ref,
    piece_ref,
    extra_ref,
    prefix_ref,
    mat_ref,
    num_ref,
    aux_ref,
    cell_ref,
    token_ref,
    resid_ref,
    out_gate_ref,
    out_proj_ref,
    gate_ref,
    up_ref,
    down_ref,
    twin_down_ref,
    infos_ref,
    rows_ref,
    held_ref,
    cross_ref,
    crossed_ref,
    answer_ref,
    back_ref,
    batch_ref,
    done_ref,
    part_ref,
    own_ref,
    sum_ref,
    load_sems,
    own_sem,
    send_sems,
    recv_sems,
    extra_send_sems,
    extra_recv_sems,
    back_send_sems,
    back_recv_sems,
    turn_send_sems,
    turn_recv_sems,
    info_send,
    info_recv,
    row_send,
    row_recv,
    cross_send,
    cross_recv,
    answer_send,
    answer_recv,
    sum_send,
    sum_recv,
    weight_send,
    weight_recv,
    *,
    count,
    heads,
    line,
    halves,
    slots,
    pieces,
    tile,
):
    seq_len, width = q_ref.shape
    cut = width // count
    place = lax.axis_index("sp")
    head = lax.axis_index("tp")
    here = place // 2
    side = lax.rem(place, 2)
    twin = place + 1 - 2 * side
    mate = head + 1 - 2 * lax.rem(head, 2)
    across = lax.rem(head + 2, heads)
    units = line * halves
    tokens = rows_ref.shape[1]
    grain = tokens // pieces
    last = line - 1
    shares = WEIGHT_PIECES
    chunks = shares

    def remote(src, dst, send, recv, peer, axis="sp"):
        return pltpu.make_async_remote_copy(
            src_ref=src,
            dst_ref=dst,
            send_sem=send,
            recv_sem=recv,
            device_id={axis: peer},
            device_id_type=pl.DeviceIdType.MESH,
        )

    loads = [
        pltpu.make_async_copy(src, dst, load_sems.at[i])
        for i, (src, dst) in enumerate(
            [
                (out_gate_hbm, out_gate_ref),
                (resid_hbm, resid_ref),
                (out_proj_hbm, out_proj_ref),
                (gate_hbm, gate_ref),
                (up_hbm, up_ref),
                (down_hbm, down_ref),
            ]
        )
    ]
    for load in loads:
        load.start()

    barrier = pltpu.get_barrier_semaphore()
    greeted = sp_tp_barrier(barrier, {"sp": count, "tp": heads})

    def weight_rows(chunk, owner):
        quarter = twin_down_ref.shape[0] // heads
        size = quarter // shares
        rows = pl.ds(pl.multiple_of(owner * quarter + chunk * size, size), size)
        return down_hbm.at[0, rows], twin_down_ref.at[rows]

    def weight_copy(stage, chunk):
        owner, peer, axis = (
            (head, twin, "sp"),
            (head, across, "tp"),
            (head, mate, "tp"),
            (across, mate, "tp"),
        )[stage]
        whole, landed = weight_rows(chunk, owner)
        return remote(
            whole if stage == 0 else landed,
            landed,
            weight_send.at[stage, chunk],
            weight_recv.at[stage, chunk],
            peer,
            axis,
        )

    def fetch(*span):
        for chunk in range(*span):
            weight_copy(0, chunk).start()

    def pass_on(*span):
        for chunk in range(*span):
            weight_copy(0, chunk).wait_recv()
            weight_copy(1, chunk).start()
            weight_copy(2, chunk).start()

    def hand_over(*span):
        for chunk in range(*span):
            weight_copy(1, chunk).wait_recv()
            weight_copy(3, chunk).start()

    def info_copy(step):
        peer = lax.rem(here + step, line)
        return remote(
            infos_ref.at[here],
            infos_ref.at[here],
            info_send.at[step - 1],
            info_recv.at[step - 1],
            peer * 2 + side,
        )

    log_forget, cum_row, gap_row = log_rows(forget_ref, input_ref)
    pl.semaphore_wait(barrier, greeted)
    total = jnp.sum(log_forget, axis=1, keepdims=True)
    best = jnp.max(gap_row, axis=1, keepdims=True)
    keep_row = jnp.exp(gap_row - best) * width ** (-0.5)
    weighted = k_ref[...].astype(jnp.float32).T * keep_row
    high, low = split_two(weighted)
    v_all = v_ref[...]
    state_ref[0:width, :] = jnp.dot(high, v_all, preferred_element_type=jnp.float32) + jnp.dot(
        low, v_all, preferred_element_type=jnp.float32
    )
    vector = jnp.dot(
        jnp.broadcast_to(keep_row, (8, seq_len)),
        k_ref[...].astype(jnp.float32),
        precision=HIGHEST,
        preferred_element_type=jnp.float32,
    )[0:1]
    lanes = jnp.zeros((1, width), jnp.float32)
    state_ref[width : width + EXTRA, :] = jnp.concatenate(
        [vector, lanes + total, lanes + total + best, jnp.zeros((EXTRA - 3, width), jnp.float32)],
        axis=0,
    )
    sends = []
    for step in range(1, count):
        peer = lax.rem(place + step, count)
        extra_copy = pltpu.make_async_remote_copy(
            src_ref=state_ref.at[pl.ds(width, EXTRA)],
            dst_ref=extra_ref.at[place],
            send_sem=extra_send_sems.at[step - 1],
            recv_sem=extra_recv_sems.at[step - 1],
            device_id={"sp": peer},
            device_id_type=pl.DeviceIdType.MESH,
        )
        piece_copy = pltpu.make_async_remote_copy(
            src_ref=state_ref.at[pl.ds(pl.multiple_of(peer * cut, cut), cut)],
            dst_ref=piece_ref.at[place],
            send_sem=send_sems.at[step - 1],
            recv_sem=recv_sems.at[step - 1],
            device_id={"sp": peer},
            device_id_type=pl.DeviceIdType.MESH,
        )
        extra_copy.start()
        piece_copy.start()
        sends += [extra_copy, piece_copy]
    extra_ref[place] = state_ref[width : width + EXTRA, :]
    piece_ref[place] = state_ref[pl.ds(pl.multiple_of(place * cut, cut), cut), :]


    eye_row, eye_col = col_mask(0, tokens, tokens)
    eye = jnp.where(eye_row == eye_col, 1.0, 0.0)
    for half in range(halves):
        span = slice(half * tokens, (half + 1) * tokens)
        ids = routes_ref[:, span].astype(jnp.float32)
        scores = scores_ref[:, span]
        zeros = jnp.zeros((8 - ids.shape[0], tokens), jnp.float32)
        columns = lax.dot_general(
            eye,
            jnp.concatenate([ids, zeros], axis=0),
            (((1,), (1,)), ((), ())),
            precision=HIGHEST,
            preferred_element_type=jnp.float32,
        )
        ranks = []
        for route in range(2):
            rank = jnp.zeros((1, tokens), jnp.float32)
            for other in range(2):
                same = (columns[:, other : other + 1] == ids[route : route + 1]) & (eye_row < eye_col)
                rank += jnp.sum(jnp.where(same, 1.0, 0.0), axis=0, keepdims=True)
            ranks.append(rank)
        infos_ref[here, half] = jnp.concatenate(
            [ids] + ranks + [scores / jnp.sum(scores, axis=0, keepdims=True), zeros[0:2]], axis=0
        )

    for step in range(1, line):
        info_copy(step).start()

    for first in range(0, seq_len, tile):
        span = first + tile
        row, col = col_mask(first, tile, span)
        causal = col <= row
        own = (col // BLOCK) == (row // BLOCK)
        gap = jnp.where(causal, gap_row[:, :span], -jnp.inf)
        top = jnp.max(gap, axis=1, keepdims=True)
        cum = jnp.sum(jnp.where(causal, log_forget[:, :span], 0.0), axis=1, keepdims=True)
        scores = lax.dot_general(
            q_ref[first:span, :],
            k_ref[0:span, :],
            (((1,), (1,)), ((), ())),
            preferred_element_type=jnp.float32,
        ) * width ** (-0.5)
        weights = scores * jnp.exp(gap - top)
        high = weights.astype(jnp.bfloat16)
        high_float = high.astype(jnp.float32)
        low_float = jnp.where(own, 0.0, weights - high_float)
        v = v_ref[0:span, :]
        num_ref[first:span, :] = jnp.dot(high, v, preferred_element_type=jnp.float32) + jnp.dot(
            low_float.astype(jnp.bfloat16), v, preferred_element_type=jnp.float32
        )
        den = jnp.sum(high_float + low_float, axis=1, keepdims=True)
        lane = lax.broadcasted_iota(jnp.int32, (tile, 128), 1)
        aux_ref[first:span, :] = jnp.where(lane == 0, den, jnp.where(lane == 1, top, cum))

    for copy in sends:
        copy.wait()

    running = jnp.zeros((cut, width), jnp.float32)
    vector = jnp.zeros((1, width), jnp.float32)
    far_max = jnp.full((1, width), FLOOR_LOG, jnp.float32)
    own_vector, own_max = vector, far_max
    for step in range(count):
        prefix_ref[step] = running
        own_vector = jnp.where(place == step, vector, own_vector)
        own_max = jnp.where(place == step, far_max, own_max)
        if step < count - 1:
            extra = extra_ref[step]
            new_max, step_total = extra[2:3], extra[1:2]
            joined = jnp.maximum(step_total + far_max, new_max)
            keep_old = jnp.exp(step_total + far_max - joined)
            keep_new = jnp.exp(new_max - joined)
            running = keep_old * running + keep_new * piece_ref[step]
            vector = keep_old * vector + keep_new * extra[0:1]
            far_max = joined
    backs = []
    for step in range(1, count):
        peer = lax.rem(place + step, count)
        back = pltpu.make_async_remote_copy(
            src_ref=prefix_ref.at[peer],
            dst_ref=mat_ref.at[pl.ds(pl.multiple_of(place * cut, cut), cut)],
            send_sem=back_send_sems.at[step - 1],
            recv_sem=back_recv_sems.at[step - 1],
            device_id={"sp": peer},
            device_id_type=pl.DeviceIdType.MESH,
        )
        back.start()
        backs.append(back)
    mat_ref[pl.ds(pl.multiple_of(place * cut, cut), cut), :] = prefix_ref[place]

    aux = aux_ref[...]
    den, top, cum = aux[:, 0:1], aux[:, 1:2], aux[:, 2:3]
    far = own_max[:, 0:1]
    joined = jnp.maximum(top, far)
    keep_own = jnp.exp(top - joined)
    keep_far = jnp.exp(far - joined)
    q_float = q_ref[...].astype(jnp.float32)
    far_den = jnp.sum(q_float * own_vector, axis=1, keepdims=True)
    denominator = keep_own * den + keep_far * far_den
    divisor = jnp.maximum(jnp.abs(denominator), jnp.exp(-(cum + joined)))
    for copy in backs:
        copy.wait()
    one, rest = split_two(mat_ref[...])
    two, three = split_two(mat_ref[...] - one.astype(jnp.float32))
    q = q_ref[...]
    far_num = (
        jnp.dot(q, one, preferred_element_type=jnp.float32)
        + jnp.dot(q, two, preferred_element_type=jnp.float32)
        + jnp.dot(q, three, preferred_element_type=jnp.float32)
    )
    numerator = keep_own * num_ref[...] + keep_far * far_num
    cell_ref[...] = (numerator / divisor).astype(cell_ref.dtype)

    share = seq_len // heads
    columns = pl.ds(pl.multiple_of(head * width, width), width)
    turns = []
    for step in range(1, heads):
        peer = lax.rem(head + step, heads)
        turn = pltpu.make_async_remote_copy(
            src_ref=cell_ref.at[pl.ds(pl.multiple_of(peer * share, share), share)],
            dst_ref=token_ref.at[:, columns],
            send_sem=turn_send_sems.at[step - 1],
            recv_sem=turn_recv_sems.at[step - 1],
            device_id={"tp": peer},
            device_id_type=pl.DeviceIdType.MESH,
        )
        turn.start()
        turns.append(turn)
    own_copy = pltpu.make_async_copy(
        cell_ref.at[pl.ds(pl.multiple_of(head * share, share), share)],
        token_ref.at[:, columns],
        own_sem,
    )
    own_copy.start()
    fetch(0, chunks)
    for load in loads[:3]:
        load.wait()
    own_copy.wait()
    for copy in turns:
        copy.wait()

    def row_copy(src, source, half, way):
        unit = source * halves + half
        return remote(
            src,
            held_ref.at[unit],
            row_send.at[way, unit],
            row_recv.at[unit],
            place + (4 * way - 2),
        )

    def cross_copy(unit):
        return remote(
            cross_ref.at[unit],
            crossed_ref.at[unit],
            cross_send.at[unit],
            cross_recv.at[unit],
            twin,
        )

    def answer_copy(unit):
        return remote(
            answer_ref.at[unit],
            back_ref.at[unit],
            answer_send.at[unit],
            answer_recv.at[unit],
            twin,
        )

    def sum_copy(target, half, way, piece):
        landing = ((target + way) * halves + half) * pieces + piece
        leaving = (target * halves + half) * pieces + piece
        return remote(
            part_ref.at[leaving],
            sum_ref.at[landing],
            sum_send.at[leaving],
            sum_recv.at[landing],
            place + (4 * way - 2),
        )

    def sum_wait(landing):
        remote(
            part_ref.at[0], sum_ref.at[landing], sum_send.at[0], sum_recv.at[landing], twin
        ).wait_recv()

    for half in range(halves):
        span = slice(half * tokens, (half + 1) * tokens)
        cell_float = token_ref[span, :].astype(jnp.float32)
        headed = (
            cell_float
            * lax.rsqrt(jnp.mean(cell_float * cell_float, axis=1, keepdims=True) + EPS)
            * head_gain_ref[...]
        )
        gated = (headed * jax.nn.sigmoid(out_gate_ref[span, :].astype(jnp.float32))).astype(
            jnp.bfloat16
        )
        mixed = resid_ref[span, :].astype(jnp.float32) + jnp.dot(
            gated, out_proj_ref[...], preferred_element_type=jnp.float32
        )
        own_ref[half] = mixed
        normed = (
            mixed
            * lax.rsqrt(jnp.mean(mixed * mixed, axis=1, keepdims=True) + EPS)
            * ffn_gain_ref[...]
        ).astype(jnp.bfloat16)
        rows_ref[half] = normed
        held_ref[here * halves + half] = normed
        if half == 0:
            for way in range(2):

                @pl.when((here < last) if way else (here > 0))
                def _():
                    row_copy(rows_ref.at[0], here, 0, way).start()

    def later_halves(way):
        for half in range(1, halves):
            row_copy(rows_ref.at[half], here, half, way).start()

    @pl.when(here == 0)
    def _():
        later_halves(1)

    @pl.when(here == last)
    def _():
        later_halves(0)

    for step in range(1, line):
        info_copy(step).wait()
    shorter = jnp.minimum(here, last - here)

    def in_stream(p, reach):
        first = p < reach
        turn = p - reach
        ahead = jnp.where(first, p + 1, reach - turn // (halves - 1))
        return ahead, jnp.where(first, 0, 1 + lax.rem(turn, halves - 1))

    def source_of(k):
        p = k - halves
        both = shorter * 2 * halves
        paired = p < both
        way = jnp.where(paired, lax.rem(p, 2), jnp.where(here < last - here, 1, 0))
        spot = jnp.where(paired, p // 2, p - shorter * halves)
        reach = jnp.where(way == 1, last - here, here)
        ahead, half = in_stream(spot, reach)
        is_own = k < halves
        final = spot == reach * halves - 1
        return (
            jnp.where(is_own, here, here + ahead * (2 * way - 1)),
            jnp.where(is_own, k, half),
            final,
        )

    def matches(source, half, weighted):
        info = infos_ref[source, half]
        rank = lax.broadcasted_iota(jnp.int32, (slots, tokens), 0).astype(jnp.float32)
        tables = []
        for expert in (place, twin):
            name = expert.astype(jnp.float32)
            table = jnp.zeros((slots, tokens), jnp.float32)
            for route in range(2):
                hit = jnp.where(info[route : route + 1] == name, info[2 + route : 3 + route], -1.0)
                value = info[4 + route : 5 + route] if weighted else 1.0
                table += jnp.where(hit == rank, value, 0.0)
            tables.append(table)
        return jnp.concatenate(tables, axis=0)

    first_way = jnp.where(last - here <= here, 0, 1)

    def relay(way, spot):
        reach = jnp.where(way == 1, last - here, here)

        @pl.when((spot >= 0) & (spot < reach * halves) & (here > 0) & (here < last))
        def _():
            ahead, half = in_stream(spot, reach)
            target = here + ahead * (2 * way - 1)
            for piece in range(pieces):
                unit = (target * halves + half) * pieces + piece
                landing = ((target + way) * halves + half) * pieces + piece
                sum_wait(landing)
                part_ref[unit] = (
                    part_ref[unit].astype(jnp.float32) + sum_ref[landing].astype(jnp.float32)
                ).astype(jnp.bfloat16)
                sum_copy(target, half, way, piece).start()

    def down(active, mat):
        return jnp.dot(active, mat, preferred_element_type=jnp.float32).astype(jnp.bfloat16)

    def activate(rows):
        gate = jnp.dot(rows, gate_ref[0], preferred_element_type=jnp.float32)
        up = jnp.dot(rows, up_ref[0], preferred_element_type=jnp.float32)
        return (jax.nn.silu(gate) * up).astype(jnp.bfloat16)

    inner_stop = (here > 0) & (here < last)
    lag = jnp.where(inner_stop, 1, 0)

    def row_wait(unit):
        remote(
            held_ref.at[unit], held_ref.at[unit], row_send.at[0, unit], row_recv.at[unit], twin
        ).wait_recv()

    def forward(k):
        source, half, final = source_of(k)
        unit = source * halves + half
        row_wait(unit)
        for way in range(2):

            @pl.when((source < here) if way else (source > here))
            def _():
                row_copy(held_ref.at[unit], source, half, way).start()

                @pl.when(final)
                def _():
                    later_halves(way)

    def forward_now(k):
        spot = k - halves
        paired = spot < shorter * 2 * halves
        leads = (spot >= 0) & (jnp.where(paired, lax.rem(spot, 2), 0) == 0)
        pl.when(inner_stop & leads)(lambda: forward(k))
        pl.when(inner_stop & leads & paired)(lambda: forward(k + 1))

    def step_body(k, carry):
        pl.when(k < units)(lambda: forward_now(k))

        @pl.when(k < units)
        def _():
            source, half, _ = source_of(k)
            unit = source * halves + half

            @pl.when((source != here) & ~inner_stop)
            def _():
                row_wait(unit)

            packed = jnp.dot(
                matches(source, half, False).astype(jnp.bfloat16),
                held_ref[unit],
                preferred_element_type=jnp.float32,
            ).astype(jnp.bfloat16)
            cross_ref[unit] = packed[slots:]
            cross_copy(unit).start()
            batch_ref[...] = packed[:slots]

        @pl.when(k == 0)
        def _():
            for load in loads[3:]:
                load.wait()

        @pl.when(k == 1)
        def _():
            pass_on(0, chunks)

        @pl.when(k < units)
        def _():
            source, half, _ = source_of(k)
            done_ref[source * halves + half, 0:slots, :] = down(
                activate(batch_ref[...]), down_ref[0]
            )

        @pl.when(k == 2)
        def _():
            hand_over(0, chunks)

        @pl.when(k == 1 + halves)
        def _():
            for chunk in range(chunks):
                weight_copy(2, chunk).wait_recv()
                weight_copy(3, chunk).wait_recv()

        def answer_twin():
            source, half, _ = source_of(k - lag)
            unit = source * halves + half
            cross_copy(unit).wait_recv()
            answer_ref[unit] = activate(crossed_ref[unit])
            answer_copy(unit).start()

        pl.when(inner_stop & (k >= lag) & (k < units + lag))(answer_twin)

        relay(first_way, k - units)
        relay(1 - first_way, k - units - 2)
        turn_now = k - 1 - lag

        @pl.when((turn_now >= halves) & (turn_now < units + halves))
        def _():
            source, half, _ = source_of(jnp.where(turn_now < units, turn_now, turn_now - units))
            unit = source * halves + half
            answer_copy(unit).wait_recv()
            done_ref[unit, slots : 2 * slots, :] = down(back_ref[unit], twin_down_ref[...])
            high, low = split_two(matches(source, half, True))
            answers = done_ref[unit]
            turned = (((0,), (0,)), ((), ()))
            part = lax.dot_general(
                high, answers, turned, preferred_element_type=jnp.float32
            ) + lax.dot_general(low, answers, turned, preferred_element_type=jnp.float32)

            @pl.when(source == here)
            def _():
                own_ref[half] = own_ref[half] + part

            @pl.when(source != here)
            def _():
                for piece in range(pieces):
                    part_ref[unit * pieces + piece] = part[
                        piece * grain : (piece + 1) * grain
                    ].astype(jnp.bfloat16)

            @pl.when((source < here) & (here == last))
            def _():
                for piece in range(pieces):
                    sum_copy(source, half, 0, piece).start()

            @pl.when((source > here) & (here == 0))
            def _():
                for piece in range(pieces):
                    sum_copy(source, half, 1, piece).start()

        pl.when(~inner_stop & (k < units))(answer_twin)

        return carry

    lax.fori_loop(0, units + 2 + halves, step_body, 0)

    for half in range(halves):
        for piece in range(pieces):
            rows = pl.ds(piece * grain, grain)
            for way in range(2):

                @pl.when((here > 0) if way else (here < last))
                def _():
                    landing = ((here + way) * halves + half) * pieces + piece
                    sum_wait(landing)
                    own_ref[half, rows] = own_ref[half, rows] + sum_ref[landing].astype(jnp.float32)

            out_ref[half, rows] = own_ref[half, rows].astype(out_ref.dtype)

    def drain(unit, carry):
        source = unit // halves
        half = lax.rem(unit, halves)
        cross_copy(unit).wait_send()
        answer_copy(unit).wait_send()

        @pl.when((source <= here) & (here < last))
        def _():
            row_copy(held_ref.at[unit], source, half, 1).wait_send()

        @pl.when((source >= here) & (here > 0))
        def _():
            row_copy(held_ref.at[unit], source, half, 0).wait_send()

        @pl.when(source != here)
        def _():
            for piece in range(pieces):
                sum_copy(source, half, 0, piece).wait_send()

        return carry

    lax.fori_loop(0, units, drain, 0)
    for chunk in range(chunks):
        for stage in range(4):
            weight_copy(stage, chunk).wait_send()


def run_layer(
    resid,
    query,
    keys,
    values,
    out_gate,
    forget_pre,
    input_pre,
    head_gain,
    out_proj,
    ffn_gain,
    routes,
    route_scores,
    w_gate,
    w_up,
    w_down,
    halves,
    slots,
):
    count, heads = lax.axis_size("sp"), lax.axis_size("tp")
    line = count // 2
    units = line * halves
    seq_len, width = query.shape
    cut = width // count
    share = seq_len // heads
    wide, inner = resid.shape[1], w_down.shape[1]
    tokens = share // halves
    pieces = 2
    grain = tokens // pieces
    tile = 4 * BLOCK if seq_len % (4 * BLOCK) == 0 else BLOCK
    vmem = pl.BlockSpec(memory_space=pltpu.VMEM)
    whole = pl.BlockSpec(memory_space=pl.ANY)
    dma = pltpu.SemaphoreType.DMA
    f32, bf16 = jnp.float32, jnp.bfloat16
    chunks = WEIGHT_PIECES
    out = pl.pallas_call(
        functools.partial(
            layer_kernel,
            count=count,
            heads=heads,
            line=line,
            halves=halves,
            slots=slots,
            pieces=pieces,
            tile=tile,
        ),
        out_shape=jax.ShapeDtypeStruct((halves, tokens, wide), bf16),
        in_specs=[vmem] * 9 + [whole] * 6,
        out_specs=vmem,
        scratch_shapes=[
            pltpu.VMEM((width + EXTRA, width), f32),
            pltpu.VMEM((count, cut, width), f32),
            pltpu.VMEM((count, EXTRA, width), f32),
            pltpu.VMEM((count, cut, width), f32),
            pltpu.VMEM((width, width), f32),
            pltpu.VMEM((seq_len, width), f32),
            pltpu.VMEM((seq_len, 128), f32),
            pltpu.VMEM((seq_len, width), bf16),
            pltpu.VMEM((share, heads * width), bf16),
            pltpu.VMEM(resid.shape, bf16),
            pltpu.VMEM(out_gate.shape, bf16),
            pltpu.VMEM(out_proj.shape, bf16),
            pltpu.VMEM(w_gate.shape, bf16),
            pltpu.VMEM(w_up.shape, bf16),
            pltpu.VMEM(w_down.shape, bf16),
            pltpu.VMEM(w_down.shape[1:], bf16),
            pltpu.VMEM((line, halves, 8, tokens), f32),
            pltpu.VMEM((halves, tokens, wide), bf16),
            pltpu.VMEM((units, tokens, wide), bf16),
            pltpu.VMEM((units, slots, wide), bf16),
            pltpu.VMEM((units, slots, wide), bf16),
            pltpu.VMEM((units, slots, inner), bf16),
            pltpu.VMEM((units, slots, inner), bf16),
            pltpu.VMEM((slots, wide), bf16),
            pltpu.VMEM((units, 2 * slots, wide), bf16),
            pltpu.VMEM((units * pieces, grain, wide), bf16),
            pltpu.VMEM((halves, tokens, wide), f32),
            pltpu.VMEM(((units + halves) * pieces, grain, wide), bf16),
            dma((6,)),
            dma(()),
            dma((count - 1,)),
            dma((count - 1,)),
            dma((count - 1,)),
            dma((count - 1,)),
            dma((count - 1,)),
            dma((count - 1,)),
            dma((heads - 1,)),
            dma((heads - 1,)),
            dma((line - 1,)),
            dma((line - 1,)),
            dma((2, units)),
            dma((units,)),
            dma((units,)),
            dma((units,)),
            dma((units,)),
            dma((units,)),
            dma((units * pieces,)),
            dma(((units + halves) * pieces,)),
            dma((4, chunks)),
            dma((4, chunks)),
        ],
        compiler_params=pltpu.CompilerParams(
            vmem_limit_bytes=LAYER_VMEM, collective_id=5, has_side_effects=True
        ),
        cost_estimate=pl.CostEstimate(flops=10**10, bytes_accessed=2**24, transcendentals=0),
        name="layer",
    )(
        query,
        keys,
        values,
        forget_pre,
        input_pre,
        head_gain[None, :],
        ffn_gain[None, :],
        routes.T,
        route_scores.T,
        resid,
        out_gate,
        out_proj,
        w_gate,
        w_up,
        w_down,
    )
    return out.reshape(share, wide)


def slot_select(expert_ids, expert_count, capacity):
    flat_ids = expert_ids.reshape(-1)
    one_hot = (flat_ids[:, None] == jnp.arange(expert_count, dtype=jnp.int32)[None, :]).astype(
        jnp.int32
    )
    slot_rank = jnp.sum((jnp.cumsum(one_hot, axis=0) - 1) * one_hot, axis=1)
    target = flat_ids * capacity + slot_rank
    return (
        jnp.arange(expert_count * capacity, dtype=jnp.int32)[:, None] == target[None, :]
    ).astype(jnp.bfloat16)


def exchange_kernel(send_ref, recv_ref, send_sems, recv_sems, own_sem, *, axis, count):
    place = lax.axis_index(axis)
    barrier = pltpu.get_barrier_semaphore()
    for step in range(1, count):
        peer = lax.rem(place + step, count)
        pl.semaphore_signal(
            barrier, inc=1, device_id={axis: peer}, device_id_type=pl.DeviceIdType.MESH
        )
    own = pltpu.make_async_copy(send_ref.at[place], recv_ref.at[place], own_sem)
    own.start()
    pl.semaphore_wait(barrier, count - 1)
    copies = []
    for step in range(1, count):
        peer = lax.rem(place + step, count)
        copy = pltpu.make_async_remote_copy(
            src_ref=send_ref.at[peer],
            dst_ref=recv_ref.at[place],
            send_sem=send_sems.at[step - 1],
            recv_sem=recv_sems.at[step - 1],
            device_id={axis: peer},
            device_id_type=pl.DeviceIdType.MESH,
        )
        copy.start()
        copies.append(copy)
    own.wait()
    for copy in copies:
        copy.wait()


def exchange(blocks, axis, collective_id):
    count = lax.axis_size(axis)
    grouped = blocks.reshape((count, -1) + blocks.shape[2:])
    out = pl.pallas_call(
        functools.partial(exchange_kernel, axis=axis, count=count),
        out_shape=jax.ShapeDtypeStruct(grouped.shape, grouped.dtype),
        in_specs=[pl.BlockSpec(memory_space=pl.ANY)],
        out_specs=pl.BlockSpec(memory_space=pl.ANY),
        scratch_shapes=[
            pltpu.SemaphoreType.DMA((count - 1,)),
            pltpu.SemaphoreType.DMA((count - 1,)),
            pltpu.SemaphoreType.DMA(()),
        ],
        compiler_params=pltpu.CompilerParams(collective_id=collective_id, has_side_effects=True),
        name="exchange",
    )(grouped)
    return out.reshape(blocks.shape)


def run_experts(arrived, w_gate, w_up, w_down, sources):
    local_count = w_gate.shape[0]
    grouped = arrived.reshape(sources, local_count, arrived.shape[1], arrived.shape[2])
    gate_pre = jnp.einsum("pesd,edf->pesf", grouped, w_gate, preferred_element_type=jnp.float32)
    up_pre = jnp.einsum("pesd,edf->pesf", grouped, w_up, preferred_element_type=jnp.float32)
    active = (jax.nn.silu(gate_pre) * up_pre).astype(jnp.bfloat16)
    result = jnp.einsum(
        "pesf,efd->pesd", active, w_down, preferred_element_type=jnp.float32
    ).astype(jnp.bfloat16)
    return result.reshape(arrived.shape)


def line_kernel(
    rows_ref,
    mix_ref,
    info_ref,
    gate_hbm,
    up_hbm,
    down_hbm,
    out_ref,
    gate_ref,
    up_ref,
    down_ref,
    infos_ref,
    held_ref,
    cross_ref,
    crossed_ref,
    answer_ref,
    done_ref,
    batch_ref,
    part_ref,
    own_ref,
    sum_ref,
    load_sems,
    info_send,
    info_recv,
    row_send,
    row_recv,
    cross_send,
    cross_recv,
    answer_send,
    answer_recv,
    sum_send,
    sum_recv,
    *,
    line,
    halves,
    slots,
    pieces,
):
    place = lax.axis_index("sp")
    here = place // 2
    side = lax.rem(place, 2)
    twin = place + 1 - 2 * side
    units = line * halves
    tokens = rows_ref.shape[1]
    grain = tokens // pieces
    last = line - 1

    def remote(src, dst, send, recv, peer):
        return pltpu.make_async_remote_copy(
            src_ref=src,
            dst_ref=dst,
            send_sem=send,
            recv_sem=recv,
            device_id={"sp": peer},
            device_id_type=pl.DeviceIdType.MESH,
        )

    loads = [
        pltpu.make_async_copy(src, dst, load_sems.at[i])
        for i, (src, dst) in enumerate(
            [(gate_hbm, gate_ref), (up_hbm, up_ref), (down_hbm, down_ref)]
        )
    ]
    for load in loads:
        load.start()

    barrier = pltpu.get_barrier_semaphore()
    for step in range(1, line):
        pl.semaphore_signal(
            barrier,
            inc=1,
            device_id={"sp": lax.rem(here + step, line) * 2 + side},
            device_id_type=pl.DeviceIdType.MESH,
        )
    pl.semaphore_signal(
        barrier, inc=1, device_id={"sp": twin}, device_id_type=pl.DeviceIdType.MESH
    )
    pl.semaphore_wait(barrier, line)

    def info_copy(step):
        peer = lax.rem(here + step, line)
        return remote(
            info_ref,
            infos_ref.at[here],
            info_send.at[step - 1],
            info_recv.at[step - 1],
            peer * 2 + side,
        )

    def row_copy(src, source, half, way):
        unit = source * halves + half
        return remote(
            src,
            held_ref.at[unit],
            row_send.at[way, unit],
            row_recv.at[unit],
            place + (4 * way - 2),
        )

    def cross_copy(unit):
        return remote(
            cross_ref.at[unit],
            crossed_ref.at[unit],
            cross_send.at[unit],
            cross_recv.at[unit],
            twin,
        )

    def answer_copy(unit):
        return remote(
            answer_ref.at[unit],
            done_ref.at[unit, pl.ds(slots, slots)],
            answer_send.at[unit],
            answer_recv.at[unit],
            twin,
        )

    def sum_copy(target, half, way, piece):
        landing = ((target + way) * halves + half) * pieces + piece
        leaving = (target * halves + half) * pieces + piece
        return remote(
            part_ref.at[leaving],
            sum_ref.at[landing],
            sum_send.at[leaving],
            sum_recv.at[landing],
            place + (4 * way - 2),
        )

    def sum_wait(landing):
        remote(
            part_ref.at[0], sum_ref.at[landing], sum_send.at[0], sum_recv.at[landing], twin
        ).wait_recv()

    for step in range(1, line):
        info_copy(step).start()
    for way in range(2):

        @pl.when((here < last) if way else (here > 0))
        def _():
            row_copy(rows_ref.at[0], here, 0, way).start()

    def later_halves(way):
        for half in range(1, halves):
            row_copy(rows_ref.at[half], here, half, way).start()

    @pl.when(here == 0)
    def _():
        later_halves(1)

    @pl.when(here == last)
    def _():
        later_halves(0)

    infos_ref[here] = info_ref[...]
    for half in range(halves):
        held_ref[here * halves + half] = rows_ref[half]
    batch_ref[...] = jnp.zeros_like(batch_ref)
    for step in range(1, line):
        info_copy(step).wait()

    shorter = jnp.minimum(here, last - here)

    def in_stream(p, reach):
        first = p < reach
        turn = p - reach
        ahead = jnp.where(first, p + 1, reach - turn // (halves - 1))
        return ahead, jnp.where(first, 0, 1 + lax.rem(turn, halves - 1))

    def source_of(k):
        p = k - halves
        both = shorter * 2 * halves
        paired = p < both
        way = jnp.where(paired, lax.rem(p, 2), jnp.where(here < last - here, 1, 0))
        spot = jnp.where(paired, p // 2, p - shorter * halves)
        reach = jnp.where(way == 1, last - here, here)
        ahead, half = in_stream(spot, reach)
        is_own = k < halves
        final = spot == reach * halves - 1
        return (
            jnp.where(is_own, here, here + ahead * (2 * way - 1)),
            jnp.where(is_own, k, half),
            final,
        )

    def matches(source, half, weighted):
        info = infos_ref[source, half]
        rank = lax.broadcasted_iota(jnp.int32, (slots, tokens), 0).astype(jnp.float32)
        tables = []
        for expert in (place, twin):
            name = expert.astype(jnp.float32)
            table = jnp.zeros((slots, tokens), jnp.float32)
            for route in range(2):
                hit = jnp.where(info[route : route + 1] == name, info[2 + route : 3 + route], -1.0)
                value = info[4 + route : 5 + route] if weighted else 1.0
                table += jnp.where(hit == rank, value, 0.0)
            tables.append(table)
        return jnp.concatenate(tables, axis=0)

    first_way = jnp.where(last - here <= here, 0, 1)

    def relay(way, spot):
        reach = jnp.where(way == 1, last - here, here)

        @pl.when((spot >= 0) & (spot < reach * halves) & (here > 0) & (here < last))
        def _():
            ahead, half = in_stream(spot, reach)
            target = here + ahead * (2 * way - 1)
            for piece in range(pieces):
                unit = (target * halves + half) * pieces + piece
                landing = ((target + way) * halves + half) * pieces + piece
                sum_wait(landing)
                part_ref[unit] = (
                    part_ref[unit].astype(jnp.float32) + sum_ref[landing].astype(jnp.float32)
                ).astype(jnp.bfloat16)
                sum_copy(target, half, way, piece).start()

    def step_body(k, carry):
        @pl.when(k < units)
        def _():
            source, half, final = source_of(k)
            unit = source * halves + half

            @pl.when(source != here)
            def _():
                remote(
                    held_ref.at[unit], held_ref.at[unit], row_send.at[0, unit], row_recv.at[unit], twin
                ).wait_recv()

            @pl.when((source < here) & (here < last))
            def _():
                row_copy(held_ref.at[unit], source, half, 1).start()

                @pl.when(final)
                def _():
                    later_halves(1)

            @pl.when((source > here) & (here > 0))
            def _():
                row_copy(held_ref.at[unit], source, half, 0).start()

                @pl.when(final)
                def _():
                    later_halves(0)

            packed = jnp.dot(
                matches(source, half, False).astype(jnp.bfloat16),
                held_ref[unit],
                preferred_element_type=jnp.float32,
            ).astype(jnp.bfloat16)
            cross_ref[unit] = packed[slots:]
            cross_copy(unit).start()
            batch_ref[0:slots, :] = packed[:slots]

        @pl.when(k == 0)
        def _():
            for load in loads:
                load.wait()

        relay(first_way, k - units)

        @pl.when((k > 0) & (k <= units))
        def _():
            source, half, _ = source_of(k - 1)
            unit = source * halves + half
            cross_copy(unit).wait_recv()
            batch_ref[slots : 2 * slots, :] = crossed_ref[unit]

        @pl.when(k <= units)
        def _():
            rows = batch_ref[...]
            gate = jnp.dot(rows, gate_ref[0], preferred_element_type=jnp.float32)
            up = jnp.dot(rows, up_ref[0], preferred_element_type=jnp.float32)
            active = (jax.nn.silu(gate) * up).astype(jnp.bfloat16)
            batch_ref[...] = jnp.dot(
                active, down_ref[0], preferred_element_type=jnp.float32
            ).astype(jnp.bfloat16)

        @pl.when(k < units)
        def _():
            source, half, _ = source_of(k)
            done_ref[source * halves + half, 0:slots, :] = batch_ref[0:slots, :]

        @pl.when((k > 0) & (k <= units))
        def _():
            source, half, _ = source_of(k - 1)
            unit = source * halves + half
            answer_ref[unit] = batch_ref[slots : 2 * slots, :]

            @pl.when(source != here)
            def _():
                answer_copy(unit).start()

        @pl.when(k == units)
        def _():
            for half in range(halves):
                answer_copy(here * halves + half).start()

        relay(1 - first_way, k - units - 2)

        @pl.when(k > 1 + halves)
        def _():
            source, half, _ = source_of(jnp.where(k > units + 1, k - units - 2, k - 2))
            unit = source * halves + half
            answer_copy(unit).wait_recv()
            high, low = split_two(matches(source, half, True))
            answers = done_ref[unit]
            turned = (((0,), (0,)), ((), ()))
            part = lax.dot_general(
                high, answers, turned, preferred_element_type=jnp.float32
            ) + lax.dot_general(low, answers, turned, preferred_element_type=jnp.float32)

            @pl.when(source == here)
            def _():
                own_ref[half] = part

            @pl.when(source != here)
            def _():
                for piece in range(pieces):
                    part_ref[unit * pieces + piece] = part[
                        piece * grain : (piece + 1) * grain
                    ].astype(jnp.bfloat16)

            @pl.when((source < here) & (here == last))
            def _():
                for piece in range(pieces):
                    sum_copy(source, half, 0, piece).start()

            @pl.when((source > here) & (here == 0))
            def _():
                for piece in range(pieces):
                    sum_copy(source, half, 1, piece).start()

        return carry

    lax.fori_loop(0, units + 2 + halves, step_body, 0)

    for half in range(halves):
        for piece in range(pieces):
            rows = pl.ds(piece * grain, grain)
            own_ref[half, rows] = own_ref[half, rows] + mix_ref[half, rows]
            for way in range(2):

                @pl.when((here > 0) if way else (here < last))
                def _():
                    landing = ((here + way) * halves + half) * pieces + piece
                    sum_wait(landing)
                    own_ref[half, rows] = own_ref[half, rows] + sum_ref[landing].astype(jnp.float32)

            out_ref[half, rows] = own_ref[half, rows].astype(out_ref.dtype)

    def drain(unit, carry):
        source = unit // halves
        half = lax.rem(unit, halves)
        cross_copy(unit).wait_send()
        answer_copy(unit).wait_send()

        @pl.when((source <= here) & (here < last))
        def _():
            row_copy(held_ref.at[unit], source, half, 1).wait_send()

        @pl.when((source >= here) & (here > 0))
        def _():
            row_copy(held_ref.at[unit], source, half, 0).wait_send()

        @pl.when(source != here)
        def _():
            for piece in range(pieces):
                sum_copy(source, half, 0, piece).wait_send()

        return carry

    lax.fori_loop(0, units, drain, 0)


def run_line(normed_rows, after_mix, info, w_gate, w_up, w_down, slots):
    count = lax.axis_size("sp")
    line, halves = count // 2, info.shape[0]
    units = line * halves
    row_count, width = normed_rows.shape
    tokens = row_count // halves
    pieces = 2
    grain = tokens // pieces
    vmem = pl.BlockSpec(memory_space=pltpu.VMEM)
    whole = pl.BlockSpec(memory_space=pl.ANY)
    dma = pltpu.SemaphoreType.DMA
    out = pl.pallas_call(
        functools.partial(line_kernel, line=line, halves=halves, slots=slots, pieces=pieces),
        out_shape=jax.ShapeDtypeStruct((halves, tokens, width), jnp.bfloat16),
        in_specs=[vmem, vmem, vmem, whole, whole, whole],
        out_specs=vmem,
        scratch_shapes=[
            pltpu.VMEM(w_gate.shape, jnp.bfloat16),
            pltpu.VMEM(w_up.shape, jnp.bfloat16),
            pltpu.VMEM(w_down.shape, jnp.bfloat16),
            pltpu.VMEM((line,) + info.shape, jnp.float32),
            pltpu.VMEM((units, tokens, width), jnp.bfloat16),
            pltpu.VMEM((units, slots, width), jnp.bfloat16),
            pltpu.VMEM((units, slots, width), jnp.bfloat16),
            pltpu.VMEM((units, slots, width), jnp.bfloat16),
            pltpu.VMEM((units, 2 * slots, width), jnp.bfloat16),
            pltpu.VMEM((2 * slots, width), jnp.bfloat16),
            pltpu.VMEM((units * pieces, grain, width), jnp.bfloat16),
            pltpu.VMEM((halves, tokens, width), jnp.float32),
            pltpu.VMEM(((units + halves) * pieces, grain, width), jnp.bfloat16),
            dma((3,)),
            dma((line - 1,)),
            dma((line - 1,)),
            dma((2, units)),
            dma((units,)),
            dma((units,)),
            dma((units,)),
            dma((units,)),
            dma((units,)),
            dma((units * pieces,)),
            dma(((units + halves) * pieces,)),
        ],
        compiler_params=pltpu.CompilerParams(
            vmem_limit_bytes=VMEM_LIMIT, collective_id=4, has_side_effects=True
        ),
        cost_estimate=pl.CostEstimate(flops=10**10, bytes_accessed=2**23, transcendentals=0),
        name="experts",
    )(
        normed_rows.reshape(halves, tokens, width),
        after_mix.reshape(halves, tokens, width),
        info,
        w_gate,
        w_up,
        w_down,
    )
    return out.reshape(row_count, width)


def route_info(routes, route_weight, halves):
    tokens = routes.shape[0] // halves
    ids = routes.reshape(halves, -1)
    order = jnp.arange(ids.shape[1], dtype=jnp.int32)
    same = (ids[:, :, None] == ids[:, None, :]) & (order[None, None, :] < order[None, :, None])
    rank = jnp.sum(same.astype(jnp.float32), axis=2)

    def turned(a):
        return a.astype(jnp.float32).reshape(halves, tokens, -1).transpose(0, 2, 1)

    return jnp.concatenate(
        [turned(routes), turned(rank), turned(route_weight), jnp.zeros((halves, 2, tokens), jnp.float32)],
        axis=1,
    )


def shards(
    resid,
    query,
    keys,
    values,
    out_gate,
    forget_pre,
    input_pre,
    head_gain,
    out_proj,
    ffn_gain,
    routes,
    route_scores,
    w_gate,
    w_up,
    w_down,
):
    head_width = query.shape[1]
    row_count, route_count = routes.shape
    sources = lax.axis_size("sp")
    local_experts = w_gate.shape[0]
    expert_count = local_experts * sources
    half_rows = row_count // 2
    capacity = max(2, 2 * half_rows * route_count // expert_count)
    dense = local_experts == 1 and sources % 2 == 0 and sources <= 8 and route_count == 2
    dense = dense and 2 * capacity >= half_rows and capacity % 16 == 0 and half_rows % 32 == 0
    if dense and lax.axis_size("tp") == 4 and head_width % (8 * sources) == 0:
        return run_layer(
            resid,
            query,
            keys,
            values,
            out_gate,
            forget_pre,
            input_pre,
            head_gain,
            out_proj,
            ffn_gain,
            routes,
            route_scores,
            w_gate,
            w_up,
            w_down,
            2,
            capacity,
        )
    route_weight = route_scores / jnp.sum(route_scores, axis=1, keepdims=True)
    token_rows = token_cell(query, keys, values, forget_pre, input_pre)
    cell_float = token_rows.astype(jnp.float32)
    headed = (
        cell_float
        * lax.rsqrt(jnp.mean(cell_float * cell_float, axis=1, keepdims=True) + EPS)
        * head_gain[None, :]
    )
    gated_out = (headed * jax.nn.sigmoid(out_gate.astype(jnp.float32))).astype(jnp.bfloat16)
    after_mix = resid.astype(jnp.float32) + jnp.dot(
        gated_out, out_proj, preferred_element_type=jnp.float32
    )
    normed_rows = (
        after_mix
        * lax.rsqrt(jnp.mean(after_mix * after_mix, axis=1, keepdims=True) + EPS)
        * ffn_gain[None, :]
    ).astype(jnp.bfloat16)
    if dense:
        info = route_info(routes, route_weight, 2)
        return run_line(normed_rows, after_mix, info, w_gate, w_up, w_down, capacity)
    selects = [
        slot_select(
            routes[half_idx * half_rows : (half_idx + 1) * half_rows], expert_count, capacity
        )
        for half_idx in range(2)
    ]

    def pack_rows(half_idx):
        selection = (
            selects[half_idx].reshape(expert_count * capacity, half_rows, route_count).sum(axis=2)
        )
        packed = jnp.dot(
            selection,
            normed_rows[half_idx * half_rows : (half_idx + 1) * half_rows],
            preferred_element_type=jnp.float32,
        )
        return packed.astype(jnp.bfloat16).reshape(expert_count, capacity, normed_rows.shape[1])

    send_rows = jnp.concatenate([pack_rows(0), pack_rows(1)], axis=1)
    finished = run_experts(
        exchange(send_rows, "sp", 1),
        w_gate,
        w_up,
        w_down,
        sources,
    )
    returned = exchange(finished, "sp", 2)
    answers = [returned[:, :capacity], returned[:, capacity:]]
    pieces = []
    for half_idx in range(2):
        gathered = lax.dot_general(
            selects[half_idx],
            answers[half_idx].reshape(expert_count * capacity, -1),
            (((0,), (0,)), ((), ())),
            preferred_element_type=jnp.float32,
        )
        weights_half = route_weight[half_idx * half_rows : (half_idx + 1) * half_rows]
        pieces.append(
            jnp.sum(gathered.reshape(half_rows, route_count, -1) * weights_half[:, :, None], axis=1)
        )
    return (after_mix + jnp.concatenate(pieces, axis=0)).astype(jnp.bfloat16)


def solution(mesh):
    placed = (
        P(("sp", "tp"), None),
        P("sp", "tp"),
        P("sp", "tp"),
        P("sp", "tp"),
        P(("sp", "tp"), None),
        P("tp", "sp"),
        P("tp", "sp"),
        P(),
        P(),
        P(),
        P(("sp", "tp"), None),
        P(("sp", "tp"), None),
        P("sp", None, None),
        P("sp", None, None),
        P("sp", None, None),
    )
    return jax.shard_map(
        shards, mesh=mesh, in_specs=placed, out_specs=P(("sp", "tp"), None), check_vma=False
    )
```
